32 devices in a mesh: sp: 4 (over z), tp: 4 (over y, x), dp: 2 (over core).
Axes of the slice: x: 2, y: 2, z: 4, core: 2. Of those that a mesh axis runs over, the one named last changes fastest.
Arguments:
- latent: bfloat16 [2048, 4, 2048], P(('sp', 'tp'), 'dp'), may hold values from -6 to 6
- context: bfloat16 [1024, 4, 2048], P('sp', 'dp'), may hold values from -6 to 6
- condition: bfloat16 [4, 2048], P('dp', 'sp'), may hold values from -6 to 6
- ctx_condition: bfloat16 [2048], P('sp'), may hold values from -6 to 6
- norm_gain: float32 [2048], replicated, may hold values from 0.1 to 1.9
- w_shift: bfloat16 [2048, 2048], P('sp', 'tp'), may hold values from -0.1875 to 0.1875
- w_scale: bfloat16 [2048, 2048], P('sp', 'tp'), may hold values from -0.1875 to 0.1875
- w_gate: bfloat16 [2048, 2048], P('sp', 'tp'), may hold values from -0.1875 to 0.1875
- w_query: bfloat16 [2048, 2048], P(None, 'tp'), may hold values from -0.125 to 0.125
- w_key: bfloat16 [2048, 512], P(None, 'tp'), may hold values from -6 to 6
- w_value: bfloat16 [2048, 512], P(None, 'tp'), may hold values from -0.125 to 0.125
- w_out: bfloat16 [2048, 2048], P('tp'), may hold values from -1 to 1
- sink: float32 [16], P('tp'), may hold values from 5 to 9
Outputs:
- mixed: bfloat16 [2048, 4, 2048], P(('sp', 'tp'), 'dp')
The draws below stay inside these ranges and needn't reach their ends.
All inputs are finite; a program needn't handle non-finite values.
Results may differ from the reference program's by a relative error of at most 0.015.
The reference program's roundings to bfloat16 on the way count: a program that leaves them out, or rounds other values in their place, can miss the bound.
Values may be sent and summed in bfloat16 or wider, within the bound.
A program may use at most 128 MiB of HBM per device.

```python
import jax
import jax.numpy as jnp
from jax import lax

D = 2048
HEADS = 16
KV_HEADS = 4
HEAD_DIM = 128
WINDOW = 128
GRID_W = 64
CTX = 1024
TOK_SP = 512
SEQ = 2048
SAMPLES = 4
N_SP = 4
N_TP = 4


def draw_w_key(key, part):
    matrix = jax.random.normal(key, (D, KV_HEADS * HEAD_DIM), jnp.float32) * D ** (-0.5)
    return jnp.clip(matrix, -6.0, 6.0).astype(jnp.bfloat16)


def block_levels(rng, shape, split, low, high):
    level = 1.0
    for dim, shards_of in split:
        draws = jax.random.uniform(jax.random.fold_in(jax.random.fold_in(rng, 6), dim), (shards_of,), jnp.float32, low / len(split), high / len(split))
        level = level * jnp.repeat(jnp.exp(draws), shape[dim] // shards_of).reshape((-1,) + (1,) * (len(shape) - 1 - dim))
    return level


def gaussian(key, dims, scale, reach, cuts=(), held_as=jnp.bfloat16):
    array = jax.random.normal(key, dims, jnp.float32) * scale
    if len(cuts) > 0:
        array = block_levels(key, dims, cuts, -0.22, 0.18) * array
    return jnp.clip(array, min=-reach, max=reach).astype(held_as)


def setup_inputs(seed: int = 0) -> dict:
    key_list = jax.random.split(jax.random.key(seed), 14)
    return {
        "latent": gaussian(key_list[0], (SEQ, SAMPLES, D), 1.0, 6.0, ((0, 16), (1, 2))),
        "context": gaussian(key_list[1], (CTX, SAMPLES, D), 1.0, 6.0, ((0, 4), (1, 2))),
        "condition": gaussian(key_list[2], (SAMPLES, D), 1.0, 6.0, ((0, 2), (1, 4))),
        "ctx_condition": gaussian(key_list[3], (D,), 1.0, 6.0, ((0, 4),)),
        "norm_gain": jnp.clip(1.0 + 0.18 * jax.random.normal(key_list[4], (D,), jnp.float32), 0.1, 1.9),
        "w_shift": gaussian(key_list[5], (D, D), (D // 2) ** -0.5, 0.1875, ((0, 4), (1, 4))),
        "w_scale": gaussian(key_list[6], (D, D), (D // 2) ** -0.5, 0.1875, ((0, 4), (1, 4))),
        "w_gate": gaussian(key_list[7], (D, D), (D // 2) ** -0.5, 0.1875, ((0, 4), (1, 4))),
        "w_query": gaussian(key_list[8], (D, HEADS * HEAD_DIM), D ** -0.5, 0.125, ((1, 4),)),
        "w_key": draw_w_key(jax.random.fold_in(key_list[13], 71), 0),
        "w_value": gaussian(key_list[10], (D, KV_HEADS * HEAD_DIM), D ** -0.5, 0.125, ((1, 4),)),
        "w_out": gaussian(key_list[11], (HEADS * HEAD_DIM, D), (HEAD_DIM // 4) ** -0.5, 1.0, ((0, 4),)),
        "sink": jnp.clip(5.0 + 4.0 * jax.random.uniform(key_list[12], (HEADS,), jnp.float32) ** block_levels(key_list[12], (HEADS,), ((0, 4),), -0.2, 0.2), 5.0, 9.0),
    }


EPSILON = 1e-06
NEGATIVE = -1e+30

def normed(values, gain):
    floats = values.astype(jnp.float32)
    return floats * lax.rsqrt(lax.optimization_barrier(jnp.mean(floats * floats, axis=-1, keepdims=True)) + EPSILON) * gain

def rotate(tensor, position):
    quarter = HEAD_DIM // 4
    freqs = 10000.0 ** (-jnp.arange(quarter, dtype=jnp.float32) / quarter)
    row_pos = (position // GRID_W).astype(jnp.float32)
    col_pos = (position % GRID_W).astype(jnp.float32)
    angle = jnp.stack([row_pos[:, None] * freqs, col_pos[:, None] * freqs], axis=1)
    cosine = jnp.cos(angle)[:, None, None]
    sine = jnp.sin(angle)[:, None, None]
    pieces = tensor.reshape(tensor.shape[:-1] + (2, 2, quarter))
    first = pieces[..., 0, :]
    second = pieces[..., 1, :]
    turned = jnp.stack([first * cosine - second * sine, second * cosine + first * sine], axis=-2)
    return turned.reshape(tensor.shape)

def attend_block(queries, keys, values, allowed, ctx_keys, ctx_values, sink_logit):
    q_rows, batch, heads_n, width = queries.shape
    kv_heads = keys.shape[2]
    grouped = queries.reshape(q_rows, batch, kv_heads, heads_n // kv_heads, width).astype(jnp.float32)
    factor = width ** (-0.5)
    local_scores = jnp.einsum('qbkgd,jbkd->bkgqj', grouped, keys.astype(jnp.float32)) * factor
    local_scores = jnp.where(allowed, local_scores, NEGATIVE)
    ctx_scores = jnp.einsum('qbkgd,jbkd->bkgqj', grouped, ctx_keys.astype(jnp.float32)) * factor
    sink_scores = sink_logit.astype(jnp.float32).reshape(kv_heads, heads_n // kv_heads)[None, :, :, None, None]
    top = jnp.maximum(jnp.maximum(lax.optimization_barrier(jnp.max(local_scores, axis=-1, keepdims=True)), lax.optimization_barrier(jnp.max(ctx_scores, axis=-1, keepdims=True))), sink_scores)
    local_exp = jnp.exp(local_scores - top)
    ctx_exp = jnp.exp(ctx_scores - top)
    total = lax.optimization_barrier(jnp.sum(local_exp, axis=-1, keepdims=True)) + lax.optimization_barrier(jnp.sum(ctx_exp, axis=-1, keepdims=True)) + jnp.exp(sink_scores - top)
    local_weights = (local_exp / total).astype(jnp.bfloat16)
    ctx_weights = (ctx_exp / total).astype(jnp.bfloat16)
    result = jnp.einsum('bkgqj,jbkd->qbkgd', local_weights.astype(jnp.float32), values.astype(jnp.float32))
    result = result + jnp.einsum('bkgqj,jbkd->qbkgd', ctx_weights.astype(jnp.float32), ctx_values.astype(jnp.float32))
    return result.astype(jnp.bfloat16).reshape(q_rows, batch, heads_n * width)

def reference(latent, context, condition, ctx_condition, norm_gain, w_shift, w_scale, w_gate, w_query, w_key, w_value, w_out, sink):
    act = jax.nn.silu(condition.astype(jnp.float32)).astype(jnp.bfloat16)
    ctx_act = jax.nn.silu(ctx_condition.astype(jnp.float32)).astype(jnp.bfloat16)
    both = jnp.concatenate([act, ctx_act[None]], axis=0)
    shift_all = jnp.dot(both, w_shift, preferred_element_type=jnp.float32)
    scale_all = jnp.dot(both, w_scale, preferred_element_type=jnp.float32)
    gate = jnp.dot(act, w_gate, preferred_element_type=jnp.float32)
    samples_n = latent.shape[1]
    hidden = (normed(latent, norm_gain) * (1.0 + scale_all[None, :samples_n]) + shift_all[None, :samples_n]).astype(jnp.bfloat16)
    ctx_hidden = (normed(context, norm_gain) * (1.0 + scale_all[samples_n]) + shift_all[samples_n]).astype(jnp.bfloat16)
    seq_len = latent.shape[0]
    position = jnp.arange(seq_len, dtype=jnp.int32)
    queries = jnp.dot(hidden, w_query, preferred_element_type=jnp.float32).reshape(seq_len, samples_n, HEADS, HEAD_DIM)
    queries = rotate(queries, position).astype(jnp.bfloat16)
    keys = jnp.dot(hidden, w_key, preferred_element_type=jnp.float32).reshape(seq_len, samples_n, KV_HEADS, HEAD_DIM)
    keys = rotate(keys, position).astype(jnp.bfloat16)
    values = jnp.dot(hidden, w_value, preferred_element_type=jnp.float32).astype(jnp.bfloat16).reshape(seq_len, samples_n, KV_HEADS, HEAD_DIM)
    ctx_keys = jnp.dot(ctx_hidden, w_key, preferred_element_type=jnp.float32).astype(jnp.bfloat16).reshape(CTX, samples_n, KV_HEADS, HEAD_DIM)
    ctx_values = jnp.dot(ctx_hidden, w_value, preferred_element_type=jnp.float32).astype(jnp.bfloat16).reshape(CTX, samples_n, KV_HEADS, HEAD_DIM)
    padding = ((WINDOW, WINDOW), (0, 0), (0, 0), (0, 0))
    keys_pad = jnp.pad(keys, padding)
    values_pad = jnp.pad(values, padding)
    span = TOK_SP + 2 * WINDOW

    def one_block(block):
        start = (block * TOK_SP).astype(jnp.int32)
        block_q = lax.dynamic_slice_in_dim(queries, start, TOK_SP, 0)
        block_k = lax.dynamic_slice_in_dim(keys_pad, start, span, 0)
        block_v = lax.dynamic_slice_in_dim(values_pad, start, span, 0)
        q_pos = start + jnp.arange(TOK_SP, dtype=jnp.int32)
        k_pos = start - WINDOW + jnp.arange(span, dtype=jnp.int32)
        allowed = (jnp.abs(k_pos[None, :] - q_pos[:, None]) <= WINDOW) & (k_pos >= 0)[None, :] & (k_pos < seq_len)[None, :]
        return attend_block(block_q, block_k, block_v, allowed, ctx_keys, ctx_values, sink)
    attn = lax.map(one_block, jnp.arange(N_SP, dtype=jnp.int32)).reshape(seq_len, samples_n, HEADS * HEAD_DIM)
    group_width = HEADS * HEAD_DIM // N_TP
    branch = jnp.zeros((seq_len, samples_n, D), jnp.float32)
    for group in range(N_TP):
        part = jnp.dot(attn[..., group * group_width:(group + 1) * group_width], w_out[group * group_width:(group + 1) * group_width], preferred_element_type=jnp.float32)
        branch = branch + part.astype(jnp.bfloat16).astype(jnp.float32)
    return (latent.astype(jnp.float32) + gate[None] * branch).astype(jnp.bfloat16)
```

```python
import functools
import math

import jax
import jax.numpy as jnp
import numpy as np
from jax import lax
from jax.experimental import pallas as pl
from jax.experimental.pallas import tpu as pltpu
from jax.sharding import PartitionSpec as P

HEAD_DIM = 128
WINDOW = 128
GRID_W = 64
EPSILON = 1e-06
NEGATIVE = -1e30
MESH = pl.DeviceIdType.MESH
F32 = jnp.float32
BF16 = jnp.bfloat16
LOG2E = math.log2(math.e)
CHUNK = 16
SENDS = ((3, 0), (3, 1), (1, 0), (2, 1), (2, 0), (1, 1), (0, 0), (0, 1))
TARGETS = (1, 2, 1, 2, 2, 1)


def kernel(
    n_sp,
    lat_hbm,
    ctx_hbm,
    cond_ref,
    cctx_ref,
    gain_ref,
    wsh_hbm,
    wsc_hbm,
    wga_hbm,
    wq_hbm,
    wk_hbm,
    wv_hbm,
    wo_hbm,
    sink_ref,
    row_cos,
    row_sin,
    col_cos,
    col_sin,
    out_ref,
    lat_raw,
    lat_all,
    ctx_v,
    wmod,
    wqkv,
    wo,
    act_s,
    mod_p,
    mod_all,
    mod_a,
    mod_b,
    mod_g,
    hbuf,
    qbuf,
    kvbuf,
    ckv,
    abuf,
    cos_ref,
    sin_ref,
    psend,
    rs,

    loc_sem,
    modp_s,
    modp_r,
    moda_s,
    moda_r,
    lat_s,
    lat_r,
    early_s,
    early_r,
    ctx_s,
    ctx_r,
    halo_s,
    halo_r,
    rs_s,
    rs_r,
):
    rows, samples, width = lat_hbm.shape
    n_tp = mod_all.shape[0]
    wid = wmod.shape[2]
    qw = wq_hbm.shape[1]
    kw = wk_hbm.shape[1]
    heads = qw // HEAD_DIM
    lc = ctx_hbm.shape[0]
    block = rows * n_tp
    sp = lax.axis_index("sp")
    tp = lax.axis_index("tp")
    tx, ty = tp % 2, tp // 2
    peer = {1: 2 * ty + 1 - tx, 2: 2 * (1 - ty) + tx, 3: 3 - tp}

    def sp_peer(o):
        return lax.rem(sp + o, n_sp)

    loads = [
        pltpu.make_async_copy(wsh_hbm, wmod.at[0], loc_sem.at[0]),
        pltpu.make_async_copy(wsc_hbm, wmod.at[1], loc_sem.at[1]),
        pltpu.make_async_copy(wga_hbm, wmod.at[2], loc_sem.at[2]),
        pltpu.make_async_copy(ctx_hbm, ctx_v, loc_sem.at[3]),
        pltpu.make_async_copy(wk_hbm, wqkv.at[:, pl.ds(qw, kw)], loc_sem.at[4]),
        pltpu.make_async_copy(wv_hbm, wqkv.at[:, pl.ds(qw + kw, kw)], loc_sem.at[5]),
        pltpu.make_async_copy(lat_hbm, lat_raw, loc_sem.at[6]),
        pltpu.make_async_copy(wq_hbm, wqkv.at[:, pl.ds(0, qw)], loc_sem.at[7]),
        pltpu.make_async_copy(wo_hbm, wo, loc_sem.at[8]),
    ]
    for i in (6, 0, 1, 2, 3, 4, 5, 7, 8):
        loads[i].start()

    barrier = pltpu.get_barrier_semaphore()
    for o in range(1, n_sp):
        pl.semaphore_signal(barrier, inc=1, device_id={"sp": sp_peer(o)}, device_id_type=MESH)
    for k in (1, 2, 3):
        pl.semaphore_signal(barrier, inc=1, device_id={"tp": peer[k]}, device_id_type=MESH)

    def apart(src, at):
        return jnp.swapaxes(src[pl.ds(at, CHUNK)], 0, 1)

    loads[6].wait()

    @pl.loop(0, rows // CHUNK)
    def _(c):
        at = pl.multiple_of(c * CHUNK, CHUNK)
        both = apart(lat_raw, at)
        for s in range(samples):
            lat_all[0, s, pl.ds(at, CHUNK), :] = both[s]

    pl.semaphore_wait(barrier, n_sp - 1 + n_tp - 1)

    def remote(src, dst, ssem, rsem, dev):
        return pltpu.make_async_remote_copy(
            src_ref=src, dst_ref=dst, send_sem=ssem, recv_sem=rsem, device_id=dev, device_id_type=MESH
        )

    def lat_copy(k, s, relay):
        if not relay:
            return remote(
                lat_all.at[0, s], lat_all.at[k, s], lat_s.at[k, s], lat_r.at[k, s], {"tp": peer[k]}
            )
        via, to = (1, 2) if s == 0 else (2, 1)
        return remote(
            lat_all.at[via, s], lat_all.at[3, s], lat_s.at[3, s], lat_r.at[3, s], {"tp": peer[to]}
        )

    half = rows // 2

    def lat_part(k, s, p):
        part = pl.ds(p * half, half)
        return remote(
            lat_all.at[0, s, part], lat_all.at[k, s, part], early_s.at[k, p], early_r.at[k, p], {"tp": peer[k]}
        )

    lat_part(1, 0, 0).start()
    lat_part(2, 1, 0).start()

    act_s[...] = jnp.zeros_like(act_s)
    cv = cond_ref[...].astype(F32)
    act_s[0:samples, :] = cv / (1.0 + jnp.exp(-cv))
    cc = cctx_ref[...].astype(F32).reshape(1, -1)
    act_s[samples : samples + 1, :] = cc / (1.0 + jnp.exp(-cc))
    both = act_s[...].astype(BF16)
    for m in range(3):
        loads[m].wait()
        mod_p[0, :, m * wid : (m + 1) * wid] = jnp.dot(both, wmod[m], preferred_element_type=F32)
    mod_copies = [
        remote(mod_p.at[0], mod_p.at[o], modp_s.at[o], modp_r.at[o], {"sp": sp_peer(o)})
        for o in range(1, n_sp)
    ]
    for copy in mod_copies:
        copy.start()

    grid_rows = block // GRID_W
    for by_row, by_col, table in ((row_cos, col_cos, cos_ref), (row_sin, col_sin, sin_ref)):
        left = lax.broadcasted_iota(jnp.int32, (GRID_W, HEAD_DIM), 1) < HEAD_DIM // 2
        for r in range(grid_rows):
            table[r * GRID_W : (r + 1) * GRID_W, :] = jnp.where(
                left, by_row[pl.ds(sp * grid_rows + r, 1), :], by_col[...]
            )

    for copy in mod_copies:
        copy.wait_recv()
    total = mod_p[0]
    for o in range(1, n_sp):
        total = total + mod_p[o]
    mod_all[tp] = total
    all_copies = [
        remote(mod_all.at[tp], mod_all.at[tp], moda_s.at[k], moda_r.at[k], {"tp": peer[k]})
        for k in (1, 2, 3)
    ]
    for copy in all_copies:
        copy.start()
    lat_part(1, 0, 1).start()
    lat_part(2, 1, 1).start()
    lat_copy(1, 1, False).start()
    lat_copy(2, 0, False).start()
    for k in (1, 2, 3):
        remote(
            mod_all.at[peer[k]], mod_all.at[peer[k]], moda_s.at[k], moda_r.at[k], {"tp": peer[k]}
        ).wait_recv()
    for t in range(n_tp):
        cols = slice(t * wid, (t + 1) * wid)
        mod_b[:, cols] = mod_all[t, :, 0:wid]
        mod_a[:, cols] = (1.0 + mod_all[t, :, wid : 2 * wid]) * gain_ref[:, cols]
        mod_g[:, cols] = mod_all[t, :, 2 * wid : 3 * wid]

    def modulate(values, mod_row):
        x = values.astype(F32)
        inv = lax.rsqrt(jnp.mean(x * x, axis=-1, keepdims=True) + EPSILON)
        return (x * inv * mod_a[mod_row : mod_row + 1, :] + mod_b[mod_row : mod_row + 1, :]).astype(BF16)

    def norm_rows(src, mod_row, base, count):
        @pl.loop(0, count // CHUNK, unroll=4)
        def _(c):
            at = pl.multiple_of(c * CHUNK, CHUNK)
            hbuf[pl.ds(base + at, CHUNK), :] = modulate(src[pl.ds(at, CHUNK), :], mod_row)

    for i in (3, 4, 5):
        loads[i].wait()
    ctx_at = pl.multiple_of(sp * lc, lc)

    @pl.loop(0, lc // CHUNK, unroll=2)
    def _(c):
        at = pl.multiple_of(c * CHUNK, CHUNK)
        both = apart(ctx_v, at)
        for s in range(samples):
            hbuf[pl.ds(s * lc + at, CHUNK), :] = modulate(both[s], samples)

    made = jnp.dot(hbuf[...], wqkv[:, qw : qw + 2 * kw], preferred_element_type=F32).astype(BF16)
    for s in range(samples):
        ckv[s, pl.ds(ctx_at, lc), :] = made[s * lc : (s + 1) * lc]

    mine = ckv.at[:, pl.ds(ctx_at, lc), :]
    ctx_copies = [
        remote(mine, mine, ctx_s.at[o], ctx_r.at[o], {"sp": sp_peer(o)}) for o in range(1, n_sp)
    ]
    for copy in ctx_copies:
        copy.start()

    for s in (0, 1):
        lat_part(1 + s, s, 0).wait_recv()
        lat_part(1 + s, s, 1).wait_recv()
        lat_copy(3, s, True).start()

    loads[7].wait()
    lane = lax.broadcasted_iota(jnp.int32, (rows, HEAD_DIM), 1)
    low = lane % (HEAD_DIM // 2) < HEAD_DIM // 4

    def turn(u, cos, sin):
        other = jnp.where(
            low, pltpu.roll(u, HEAD_DIM - HEAD_DIM // 4, 1), pltpu.roll(u, HEAD_DIM // 4, 1)
        )
        return u * cos + other * sin

    halo_up = remote(
        kvbuf.at[:, pl.ds(block, WINDOW), :],
        kvbuf.at[:, pl.ds(0, WINDOW), :],
        halo_s.at[0],
        halo_r.at[0],
        {"sp": sp_peer(1)},
    )
    halo_down = remote(
        kvbuf.at[:, pl.ds(WINDOW, WINDOW), :],
        kvbuf.at[:, pl.ds(WINDOW + block, WINDOW), :],
        halo_s.at[1],
        halo_r.at[1],
        {"sp": sp_peer(n_sp - 1)},
    )

    @pl.loop(0, n_tp)
    def _(k):
        @pl.when(k == 1)
        def _():
            lat_copy(1, 1, False).wait_recv()

        @pl.when(k == 2)
        def _():
            lat_copy(2, 0, False).wait_recv()

        @pl.when(k == 3)
        def _():
            lat_copy(3, 0, True).wait_recv()
            lat_copy(3, 1, True).wait_recv()

        kx, ky = k % 2, k // 2
        bx = tx + kx - 2 * tx * kx
        by = ty + ky - 2 * ty * ky
        b = 2 * by + bx
        for s in range(samples):
            norm_rows(lat_all.at[k, s], s, s * rows, rows)
        at = pl.multiple_of(b * rows, rows)
        cos = cos_ref[pl.ds(at, rows), :]
        sin = sin_ref[pl.ds(at, rows), :]
        for c in range(heads // 2 + 1):
            prod = jnp.dot(
                hbuf[0 : samples * rows, :], wqkv[:, c * 2 * HEAD_DIM : (c + 1) * 2 * HEAD_DIM], preferred_element_type=F32
            )
            for s in range(samples):
                part = prod[s * rows : (s + 1) * rows]
                first = turn(part[:, :HEAD_DIM], cos, sin).astype(BF16)
                if c < heads // 2:
                    second = turn(part[:, HEAD_DIM:], cos, sin).astype(BF16)
                    qbuf[s, b, 2 * c * rows : (2 * c + 1) * rows, :] = first
                    qbuf[s, b, (2 * c + 1) * rows : (2 * c + 2) * rows, :] = second
                else:
                    kvbuf[s, pl.ds(WINDOW + at, rows), 0:HEAD_DIM] = first
                    kvbuf[s, pl.ds(WINDOW + at, rows), HEAD_DIM:] = part[:, HEAD_DIM:].astype(BF16)

        @pl.when(b == 0)
        def _():
            halo_down.start()

        @pl.when(b == n_tp - 1)
        def _():
            halo_up.start()

    loads[8].wait()
    for o in range(1, n_sp):
        got = ckv.at[:, pl.ds(pl.multiple_of(sp_peer(n_sp - o) * lc, lc), lc), :]
        remote(got, got, ctx_s.at[o], ctx_r.at[o], {"sp": sp_peer(o)}).wait_recv()

    scale = HEAD_DIM ** (-0.5) * LOG2E
    seq = block * n_sp
    nums = (((1,), (1,)), ((), ()))

    def rs_copy(i):
        return remote(
            psend.at[i], rs.at[i], rs_s.at[i], rs_r.at[i], {"tp": peer[TARGETS[i]]}
        )

    def pick(i, which):
        value = SENDS[-1][which]
        for j in range(len(SENDS) - 1):
            value = jnp.where(i == j, SENDS[j][which], value)
        return value

    span = 3 * WINDOW
    pair = 2 * rows
    row_id = lax.broadcasted_iota(jnp.int32, (pair, 1), 0)

    @pl.loop(0, 8)
    def _(i):
        k = pick(i, 0)
        s = pick(i, 1)
        kx, ky = k % 2, k // 2
        b = 2 * (ty + ky - 2 * ty * ky) + tx + kx - 2 * tx * kx
        at = pl.multiple_of(b * rows, rows)
        fresh = (i == 0) | (i == 2) | (i == 3) | (i == 6)

        @pl.when(fresh & (b == 0))
        def _():
            halo_up.wait_recv()

        @pl.when(fresh & (b == n_tp - 1))
        def _():
            halo_down.wait_recv()

        kc = ckv[s, :, 0:HEAD_DIM]
        vc = ckv[s, :, HEAD_DIM:]
        kl = kvbuf[s, pl.ds(at, span), 0:HEAD_DIM]
        vl = kvbuf[s, pl.ds(at, span), HEAD_DIM:]
        key = lax.broadcasted_iota(jnp.int32, (pair, span), 1)
        query = lax.broadcasted_iota(jnp.int32, (pair, span), 0) % rows
        pos = key + (sp * block + b * rows - WINDOW)
        allowed = (key >= query) & (key <= query + 2 * WINDOW) & (pos >= 0) & (pos < seq)
        for c in range(heads // 2):
            q = qbuf[s, b, c * pair : (c + 1) * pair, :]
            sc = lax.dot_general(q, kc, nums, preferred_element_type=F32)
            sl = lax.dot_general(q, kl, nums, preferred_element_type=F32)
            sl = jnp.where(allowed, sl, NEGATIVE)
            sink2 = jnp.where(row_id < rows, sink_ref[0, 2 * c], sink_ref[0, 2 * c + 1]) * LOG2E
            top = jnp.maximum(
                jnp.max(sc, axis=-1, keepdims=True), jnp.max(sl, axis=-1, keepdims=True)
            )
            top = jnp.maximum(top * scale, sink2)
            ec = jnp.exp2(sc * scale - top)
            el = jnp.exp2(sl * scale - top)
            total = (
                jnp.sum(ec, axis=-1, keepdims=True)
                + jnp.sum(el, axis=-1, keepdims=True)
                + jnp.exp2(sink2 - top)
            )
            o = jnp.dot(ec.astype(BF16), vc, preferred_element_type=F32)
            o = o + jnp.dot(el.astype(BF16), vl, preferred_element_type=F32)
            o = (o / total).astype(BF16)
            abuf[:, 2 * c * HEAD_DIM : (2 * c + 1) * HEAD_DIM] = o[:rows]
            abuf[:, (2 * c + 1) * HEAD_DIM : (2 * c + 2) * HEAD_DIM] = o[rows:]
        for n in range(n_tp):
            cols = slice(n * wid, (n + 1) * wid)
            psend[i, :, cols] = jnp.dot(
                abuf[...], wo[:, cols], preferred_element_type=F32
            ).astype(BF16)

        for j in range(4):

            @pl.when(i == j)
            def _(j=j):
                rs_copy(j).start()

        for j in (4, 5):

            @pl.when(i == j)
            def _(j=j):
                rs_copy(j - 4).wait_recv()

                @pl.loop(0, rows // CHUNK)
                def _(r):
                    part = pl.ds(pl.multiple_of(r * CHUNK, CHUNK), CHUNK)
                    psend[j, part, :] = (
                        psend[j, part, :].astype(F32) + rs[j - 4, part, :].astype(F32)
                    ).astype(BF16)

                rs_copy(j).start()

    for s in range(2):
        rs_copy(2 + s).wait_recv()
        rs_copy(4 + s).wait_recv()

    @pl.loop(0, rows // CHUNK, unroll=2)
    def _(r):
        part = pl.ds(pl.multiple_of(r * CHUNK, CHUNK), CHUNK)
        both = []
        for s in range(samples):
            branch = (
                psend[6 + s, part, :].astype(F32)
                + rs[2 + s, part, :].astype(F32)
                + rs[4 + s, part, :].astype(F32)
            )
            both.append((lat_all[0, s, part, :].astype(F32) + mod_g[s : s + 1, :] * branch).astype(BF16))
        out_ref[part] = jnp.swapaxes(jnp.stack(both), 0, 1)

    for copy in mod_copies + all_copies + ctx_copies:
        copy.wait_send()
    for k, s in ((1, 1), (2, 0)):
        lat_copy(k, s, False).wait_send()
        lat_part(k, k - 1, 0).wait_send()
        lat_part(k, k - 1, 1).wait_send()
    for s in (0, 1):
        lat_copy(3, s, True).wait_send()
    halo_up.wait_send()
    halo_down.wait_send()
    for i in range(6):
        rs_copy(i).wait_send()


def local(
    n_sp,
    n_tp,
    latent,
    context,
    condition,
    ctx_condition,
    norm_gain,
    w_shift,
    w_scale,
    w_gate,
    w_query,
    w_key,
    w_value,
    w_out,
    sink,
):
    rows, samples, width = latent.shape
    lc = context.shape[0]
    wid = w_shift.shape[1]
    depth = w_shift.shape[0]
    qw, kw = w_query.shape[1], w_key.shape[1]
    heads = qw // HEAD_DIM
    block = rows * n_tp
    assert n_tp == 4 and samples == 2 and kw == HEAD_DIM and rows == WINDOW and block % GRID_W == 0 and heads % 2 == 0
    quarter = HEAD_DIM // 4
    lane = np.arange(HEAD_DIM)
    freqs = 10000.0 ** (-(lane % quarter).astype(np.float32) / quarter)
    sign = np.where(lane % (2 * quarter) < quarter, -1.0, 1.0)

    def table(count):
        angle = np.arange(count, dtype=np.float32)[:, None] * freqs[None, :].astype(np.float32)
        return jnp.asarray(np.cos(angle), F32), jnp.asarray(np.sin(angle) * sign[None, :], F32)

    row_table = table(n_sp * block // GRID_W)
    col_table = table(GRID_W)
    hbm = pl.BlockSpec(memory_space=pl.ANY)
    vmem = pl.BlockSpec(memory_space=pltpu.VMEM)
    smem = pl.BlockSpec(memory_space=pltpu.SMEM)
    dma = pltpu.SemaphoreType.DMA
    mixed = pl.pallas_call(
        functools.partial(kernel, n_sp),
        out_shape=jax.ShapeDtypeStruct((rows, samples, width), BF16),
        in_specs=[hbm, hbm, vmem, vmem, vmem, hbm, hbm, hbm, hbm, hbm, hbm, hbm, smem, vmem, vmem, vmem, vmem],
        out_specs=vmem,
        scratch_shapes=[
            pltpu.VMEM((rows, samples, width), BF16),
            pltpu.VMEM((n_tp, samples, rows, width), BF16),
            pltpu.VMEM((lc, samples, width), BF16),
            pltpu.VMEM((3, depth, wid), BF16),
            pltpu.VMEM((width, qw + 2 * kw), BF16),
            pltpu.VMEM((qw, width), BF16),
            pltpu.VMEM((8, depth), F32),
            pltpu.VMEM((n_sp, 8, 3 * wid), F32),
            pltpu.VMEM((n_tp, 8, 3 * wid), F32),
            pltpu.VMEM((8, width), F32),
            pltpu.VMEM((8, width), F32),
            pltpu.VMEM((8, width), F32),
            pltpu.VMEM((samples * max(rows, lc), width), BF16),
            pltpu.VMEM((samples, n_tp, heads * rows, HEAD_DIM), BF16),
            pltpu.VMEM((samples, block + 2 * WINDOW, 2 * kw), BF16),
            pltpu.VMEM((samples, lc * n_sp, 2 * kw), BF16),
            pltpu.VMEM((rows, qw), BF16),
            pltpu.VMEM((block, HEAD_DIM), F32),
            pltpu.VMEM((block, HEAD_DIM), F32),
            pltpu.VMEM((8, rows, width), BF16),
            pltpu.VMEM((6, rows, width), BF16),
            dma((9,)),
            dma((n_sp,)),
            dma((n_sp,)),
            dma((n_tp,)),
            dma((n_tp,)),
            dma((n_tp, 2)),
            dma((n_tp, 2)),
            dma((n_tp, 2)),
            dma((n_tp, 2)),
            dma((n_sp,)),
            dma((n_sp,)),
            dma((2,)),
            dma((2,)),
            dma((6,)),
            dma((6,)),
        ],
        compiler_params=pltpu.CompilerParams(
            collective_id=0, has_side_effects=True, vmem_limit_bytes=60 * 1024 * 1024
        ),
        name="step",
    )(
        latent,
        context,
        condition,
        ctx_condition,
        norm_gain[None],
        w_shift,
        w_scale,
        w_gate,
        w_query,
        w_key,
        w_value,
        w_out,
        sink[None],
        *row_table,
        *col_table,
    )
    return mixed


def solution(mesh):
    return jax.shard_map(
        functools.partial(local, mesh.shape["sp"], mesh.shape["tp"]),
        mesh=mesh,
        in_specs=(
            P(("sp", "tp"), "dp", None),
            P("sp", "dp", None),
            P("dp", "sp"),
            P("sp"),
            P(),
            P("sp", "tp"),
            P("sp", "tp"),
            P("sp", "tp"),
            P(None, "tp"),
            P(None, "tp"),
            P(None, "tp"),
            P("tp", None),
            P("tp"),
        ),
        out_specs=P(("sp", "tp"), "dp", None),
        check_vma=False,
    )
```

```python
import functools
import math

import jax
import jax.numpy as jnp
import numpy as np
from jax import lax
from jax.experimental import pallas as pl
from jax.experimental.pallas import tpu as pltpu
from jax.sharding import PartitionSpec as P

HEAD_DIM = 128
WINDOW = 128
GRID_W = 64
EPSILON = 1e-06
NEGATIVE = -1e30
MESH = pl.DeviceIdType.MESH
F32 = jnp.float32
BF16 = jnp.bfloat16
LOG2E = math.log2(math.e)
CHUNK = 16


def kernel(
    n_sp,
    lat_hbm,
    ctx_hbm,
    cond_ref,
    cctx_ref,
    gain_ref,
    wsh_hbm,
    wsc_hbm,
    wga_hbm,
    wq_hbm,
    wk_hbm,
    wv_hbm,
    wo_hbm,
    sink_ref,
    row_cos,
    row_sin,
    col_cos,
    col_sin,
    out_ref,
    lat_raw,
    lat_all,
    ctx_v,
    wmod,
    wqkv,
    wo_all,
    act_s,
    mod_p,
    mod_all,
    mod_a,
    mod_b,
    mod_g,
    hbuf,
    qbuf,
    kvbuf,
    ckv,
    attn,
    acc,
    cos_ref,
    sin_ref,
    loc_sem,
    modp_s,
    modp_r,
    moda_s,
    moda_r,
    lat_s,
    lat_r,
    relay_s,
    relay_r,
    ctx_s,
    ctx_r,
    halo_s,
    halo_r,
    attn_s,
    attn_r,
    wo_s,
    wo_r,
    wod_s,
    wod_r,
    woz_s,
    woz_r,
    woc_s,
    woc_r,
    woe_s,
    woe_r,
):
    rows, samples, width = lat_hbm.shape
    n_tp = mod_all.shape[0]
    wid = wmod.shape[2]
    qw = wq_hbm.shape[1]
    kw = wk_hbm.shape[1]
    heads = qw // HEAD_DIM
    lc = ctx_hbm.shape[0]
    block = rows * n_tp
    sp = lax.axis_index("sp")
    tp = lax.axis_index("tp")
    dp = lax.axis_index("dp")
    tx, ty = tp % 2, tp // 2
    peer = {1: 2 * ty + 1 - tx, 2: 2 * (1 - ty) + tx, 3: 3 - tp}

    def sp_peer(o):
        return lax.rem(sp + o, n_sp)

    loads = [
        pltpu.make_async_copy(wsh_hbm, wmod.at[0], loc_sem.at[0]),
        pltpu.make_async_copy(wsc_hbm, wmod.at[1], loc_sem.at[1]),
        pltpu.make_async_copy(wga_hbm, wmod.at[2], loc_sem.at[2]),
        pltpu.make_async_copy(ctx_hbm, ctx_v, loc_sem.at[3]),
        pltpu.make_async_copy(wk_hbm, wqkv.at[:, pl.ds(qw, kw)], loc_sem.at[4]),
        pltpu.make_async_copy(wv_hbm, wqkv.at[:, pl.ds(qw + kw, kw)], loc_sem.at[5]),
        pltpu.make_async_copy(lat_hbm, lat_raw, loc_sem.at[6]),
        pltpu.make_async_copy(wq_hbm, wqkv.at[:, pl.ds(0, qw)], loc_sem.at[7]),
        pltpu.make_async_copy(wo_hbm, wo_all.at[0], loc_sem.at[8]),
    ]
    for i in (6, 0, 1, 2, 3, 4, 5, 7, 8):
        loads[i].start()

    barrier = pltpu.get_barrier_semaphore()
    for o in range(1, n_sp):
        pl.semaphore_signal(barrier, inc=1, device_id={"sp": sp_peer(o)}, device_id_type=MESH)
    for k in (1, 2, 3):
        pl.semaphore_signal(barrier, inc=1, device_id={"tp": peer[k]}, device_id_type=MESH)

    pl.semaphore_signal(barrier, inc=1, device_id={"dp": 1 - dp}, device_id_type=MESH)

    def apart(src, at):
        return jnp.swapaxes(src[pl.ds(at, CHUNK)], 0, 1)

    loads[6].wait()

    @pl.loop(0, rows // CHUNK)
    def _(c):
        at = pl.multiple_of(c * CHUNK, CHUNK)
        both = apart(lat_raw, at)
        for s in range(samples):
            lat_all[0, s, pl.ds(at, CHUNK), :] = both[s]

    pl.semaphore_wait(barrier, n_sp - 1 + n_tp)

    def remote(src, dst, ssem, rsem, dev):
        return pltpu.make_async_remote_copy(
            src_ref=src, dst_ref=dst, send_sem=ssem, recv_sem=rsem, device_id=dev, device_id_type=MESH
        )

    half = rows // 2

    def direct(k, s, p):
        part = pl.ds(p * half, half)
        return remote(
            lat_all.at[0, s, part], lat_all.at[k, s, part], lat_s.at[k, s, p], lat_r.at[k, s, p], {"tp": peer[k]}
        )

    def relay(s, p):
        part = pl.ds(p * half, half)
        return remote(
            lat_all.at[1 + p, s, part], lat_all.at[3, s, part], relay_s.at[s, p], relay_r.at[s, p], {"tp": peer[2 - p]}
        )

    zh = sp % 2
    quarter = qw // 4
    mine_q = 2 * zh + dp
    pair_q = 2 * (1 - zh) + dp

    def wo_rows(index, count=quarter, skip=0):
        return pl.ds(pl.multiple_of(index * quarter + skip, count), count)

    def wo_direct(k):
        part = wo_rows(mine_q)
        return remote(wo_hbm.at[part], wo_all.at[k, part], wo_s.at[k], wo_r.at[k], {"tp": peer[k]})

    def wo_relay(p):
        part = wo_rows(mine_q, quarter // 2, p * (quarter // 2))
        return remote(
            wo_all.at[1 + p, part], wo_all.at[3, part], wod_s.at[p], wod_r.at[p], {"tp": peer[2 - p]}
        )

    def wo_pair(k, index):
        part = wo_all.at[k, wo_rows(index)]
        return remote(part, part, woz_s.at[k], woz_r.at[k], {"sp": sp + 1 - 2 * zh})

    def wo_core(k, index):
        part = wo_all.at[k, wo_rows(index)]
        return remote(part, part, woc_s.at[k], woc_r.at[k], {"dp": 1 - dp})

    def wo_last(k, index):
        part = wo_all.at[k, wo_rows(index)]
        return remote(part, part, woe_s.at[k], woe_r.at[k], {"dp": 1 - dp})

    direct(1, 0, 0).start()
    direct(2, 0, 1).start()

    act_s[...] = jnp.zeros_like(act_s)
    cv = cond_ref[...].astype(F32)
    act_s[0:samples, :] = cv / (1.0 + jnp.exp(-cv))
    cc = cctx_ref[...].astype(F32).reshape(1, -1)
    act_s[samples : samples + 1, :] = cc / (1.0 + jnp.exp(-cc))
    both = act_s[...].astype(BF16)
    for m in range(3):
        loads[m].wait()
        mod_p[0, :, m * wid : (m + 1) * wid] = jnp.dot(both, wmod[m], preferred_element_type=F32)
    mod_copies = [
        remote(mod_p.at[0], mod_p.at[o], modp_s.at[o], modp_r.at[o], {"sp": sp_peer(o)})
        for o in range(1, n_sp)
    ]
    for copy in mod_copies:
        copy.start()

    grid_rows = block // GRID_W
    for by_row, by_col, table in ((row_cos, col_cos, cos_ref), (row_sin, col_sin, sin_ref)):
        left = lax.broadcasted_iota(jnp.int32, (GRID_W, HEAD_DIM), 1) < HEAD_DIM // 2
        for r in range(grid_rows):
            table[r * GRID_W : (r + 1) * GRID_W, :] = jnp.where(
                left, by_row[pl.ds(sp * grid_rows + r, 1), :], by_col[...]
            )

    for copy in mod_copies:
        copy.wait_recv()
    total = mod_p[0]
    for o in range(1, n_sp):
        total = total + mod_p[o]
    mod_all[tp] = total
    all_copies = [
        remote(mod_all.at[tp], mod_all.at[tp], moda_s.at[k], moda_r.at[k], {"tp": peer[k]})
        for k in (1, 2, 3)
    ]
    for copy in all_copies:
        copy.start()
    direct(1, 0, 1).start()
    direct(2, 0, 0).start()
    direct(1, 0, 0).wait_recv()
    direct(2, 0, 1).wait_recv()
    relay(0, 0).start()
    relay(0, 1).start()
    wo_direct(1).start()
    wo_direct(2).start()
    direct(1, 1, 0).start()
    direct(2, 1, 1).start()
    direct(1, 1, 1).start()
    direct(2, 1, 0).start()
    for k in (1, 2, 3):
        remote(
            mod_all.at[peer[k]], mod_all.at[peer[k]], moda_s.at[k], moda_r.at[k], {"tp": peer[k]}
        ).wait_recv()
    for t in range(n_tp):
        cols = slice(t * wid, (t + 1) * wid)
        mod_b[:, cols] = mod_all[t, :, 0:wid]
        mod_a[:, cols] = (1.0 + mod_all[t, :, wid : 2 * wid]) * gain_ref[:, cols]
        mod_g[:, cols] = mod_all[t, :, 2 * wid : 3 * wid]

    def modulate(values, mod_row):
        x = values.astype(F32)
        inv = lax.rsqrt(jnp.mean(x * x, axis=-1, keepdims=True) + EPSILON)
        row = pl.ds(mod_row, 1)
        return (x * inv * mod_a[row, :] + mod_b[row, :]).astype(BF16)

    def norm_rows(src, mod_row, base, count):
        @pl.loop(0, count // CHUNK, unroll=4)
        def _(c):
            at = pl.multiple_of(c * CHUNK, CHUNK)
            hbuf[pl.ds(base + at, CHUNK), :] = modulate(src[pl.ds(at, CHUNK), :], mod_row)

    for i in (3, 4, 5):
        loads[i].wait()
    ctx_at = pl.multiple_of(sp * lc, lc)

    @pl.loop(0, lc // CHUNK, unroll=2)
    def _(c):
        at = pl.multiple_of(c * CHUNK, CHUNK)
        both = apart(ctx_v, at)
        for s in range(samples):
            hbuf[pl.ds(s * lc + at, CHUNK), :] = modulate(both[s], samples)

    made = jnp.dot(hbuf[...], wqkv[:, qw : qw + 2 * kw], preferred_element_type=F32).astype(BF16)
    for s in range(samples):
        ckv[s, pl.ds(ctx_at, lc), :] = made[s * lc : (s + 1) * lc]

    mine = ckv.at[:, pl.ds(ctx_at, lc), :]
    ctx_copies = [
        remote(mine, mine, ctx_s.at[o], ctx_r.at[o], {"sp": sp_peer(o)}) for o in range(1, n_sp)
    ]
    for copy in ctx_copies:
        copy.start()

    loads[7].wait()
    lane = lax.broadcasted_iota(jnp.int32, (rows, HEAD_DIM), 1)
    low = lane % (HEAD_DIM // 2) < HEAD_DIM // 4

    def turn(u, cos, sin):
        other = jnp.where(
            low, pltpu.roll(u, HEAD_DIM - HEAD_DIM // 4, 1), pltpu.roll(u, HEAD_DIM // 4, 1)
        )
        return u * cos + other * sin

    def halo_up(s):
        return remote(
            kvbuf.at[s, pl.ds(block, WINDOW), :],
            kvbuf.at[s, pl.ds(0, WINDOW), :],
            halo_s.at[0, s],
            halo_r.at[0, s],
            {"sp": lax.min(sp + 1, n_sp - 1)},
        )

    def halo_down(s):
        return remote(
            kvbuf.at[s, pl.ds(WINDOW, WINDOW), :],
            kvbuf.at[s, pl.ds(WINDOW + block, WINDOW), :],
            halo_s.at[1, s],
            halo_r.at[1, s],
            {"sp": lax.max(sp - 1, 0)},
        )

    not_first, not_last = sp > 0, sp < n_sp - 1

    @pl.when(sp == 0)
    def _():
        kvbuf[:, 0:WINDOW, :] = jnp.zeros((samples, WINDOW, 2 * kw), BF16)

    @pl.when(sp == n_sp - 1)
    def _():
        kvbuf[:, WINDOW + block :, :] = jnp.zeros((samples, WINDOW, 2 * kw), BF16)

    acc[...] = jnp.zeros_like(acc)

    def attn_copy(k, s, dest):
        return remote(attn.at[n_tp + k, s], attn.at[k, s], attn_s.at[k, s], attn_r.at[k, s], {"tp": dest})

    def project(s):
        @pl.loop(0, n_tp // 2)
        def _(j):
            @pl.when(j == 0)
            def _():
                direct(1, s, 1).wait_recv()

            @pl.when(j == 1)
            def _():
                direct(2, s, 0).wait_recv()
                relay(s, 0).wait_recv()
                relay(s, 1).wait_recv()

            by = ty + j - 2 * ty * j
            spots = []
            for e in range(2):
                norm_rows(lat_all.at[2 * j + e, s], s, e * rows, rows)
                b = 2 * by + (1 - tx if e else tx)
                at = pl.multiple_of(b * rows, rows)
                spots.append((b, at, cos_ref[pl.ds(at, rows), :], sin_ref[pl.ds(at, rows), :]))
            for c in range(heads // 2 + 1):
                prod = jnp.dot(
                    hbuf[0 : 2 * rows, :],
                    wqkv[:, c * 2 * HEAD_DIM : (c + 1) * 2 * HEAD_DIM],
                    preferred_element_type=F32,
                )
                for e, (b, at, cos, sin) in enumerate(spots):
                    part = prod[e * rows : (e + 1) * rows]
                    first = turn(part[:, :HEAD_DIM], cos, sin).astype(BF16)
                    if c < heads // 2:
                        second = turn(part[:, HEAD_DIM:], cos, sin).astype(BF16)
                        qbuf[s, b, 2 * c * rows : (2 * c + 1) * rows, :] = first
                        qbuf[s, b, (2 * c + 1) * rows : (2 * c + 2) * rows, :] = second
                    else:
                        kvbuf[s, pl.ds(WINDOW + at, rows), 0:HEAD_DIM] = first
                        kvbuf[s, pl.ds(WINDOW + at, rows), HEAD_DIM:] = part[:, HEAD_DIM:].astype(BF16)

        @pl.when(not_last)
        def _():
            halo_up(s).start()

        @pl.when(not_first)
        def _():
            halo_down(s).start()

    scale = HEAD_DIM ** (-0.5) * LOG2E
    seq = block * n_sp
    nums = (((1,), (1,)), ((), ()))

    span = 3 * WINDOW
    pair = 2 * rows
    row_id = lax.broadcasted_iota(jnp.int32, (pair, 1), 0)

    def attend(i, s):
        b = jnp.where(i < 2, i + 1, (i - 2) * (n_tp - 1))
        bx, by = b % 2, b // 2
        k = 2 * (by + ty - 2 * by * ty) + bx + tx - 2 * bx * tx
        at = pl.multiple_of(b * rows, rows)
        slot = jnp.where(k == 0, 0, n_tp + k)

        @pl.when((b == 0) & not_first)
        def _():
            halo_up(s).wait_recv()

        @pl.when((b == n_tp - 1) & not_last)
        def _():
            halo_down(s).wait_recv()

        kc = ckv[s, :, 0:HEAD_DIM]
        vc = ckv[s, :, HEAD_DIM:]
        kl = kvbuf[s, pl.ds(at, span), 0:HEAD_DIM]
        vl = kvbuf[s, pl.ds(at, span), HEAD_DIM:]
        key = lax.broadcasted_iota(jnp.int32, (pair, span), 1)
        query = lax.broadcasted_iota(jnp.int32, (pair, span), 0) % rows
        pos = key + (sp * block + b * rows - WINDOW)
        allowed = (key >= query) & (key <= query + 2 * WINDOW) & (pos >= 0) & (pos < seq)
        for c in range(heads // 2):
            q = qbuf[s, b, c * pair : (c + 1) * pair, :]
            sc = lax.dot_general(q, kc, nums, preferred_element_type=F32)
            sl = lax.dot_general(q, kl, nums, preferred_element_type=F32)
            sl = jnp.where(allowed, sl, NEGATIVE)
            sink2 = jnp.where(row_id < rows, sink_ref[0, 2 * c], sink_ref[0, 2 * c + 1]) * LOG2E
            top = jnp.maximum(
                jnp.max(sc, axis=-1, keepdims=True), jnp.max(sl, axis=-1, keepdims=True)
            )
            top = jnp.maximum(top * scale, sink2)
            ec = jnp.exp2(sc * scale - top)
            el = jnp.exp2(sl * scale - top)
            total = (
                jnp.sum(ec, axis=-1, keepdims=True)
                + jnp.sum(el, axis=-1, keepdims=True)
                + jnp.exp2(sink2 - top)
            )
            o = jnp.dot(ec.astype(BF16), vc, preferred_element_type=F32)
            o = o + jnp.dot(el.astype(BF16), vl, preferred_element_type=F32)
            o = (o / total).astype(BF16)
            attn[slot, s, :, 2 * c * HEAD_DIM : (2 * c + 1) * HEAD_DIM] = o[:rows]
            attn[slot, s, :, (2 * c + 1) * HEAD_DIM : (2 * c + 2) * HEAD_DIM] = o[rows:]

        @pl.when((s == 1) & (k > 0))
        def _():
            attn_copy(k, s, b).start()

        @pl.when((s == 1) & (i == 1))
        def _():
            for p in range(2):
                wo_relay(p).wait_recv()
            wo_pair(3, mine_q).start()
            wo_core(3, mine_q).start()

    @pl.loop(0, samples)
    def _(s):
        project(s)

        @pl.when(s == 0)
        def _():
            for o in range(1, n_sp):
                got = ckv.at[:, pl.ds(pl.multiple_of(sp_peer(n_sp - o) * lc, lc), lc), :]
                remote(got, got, ctx_s.at[o], ctx_r.at[o], {"sp": sp_peer(o)}).wait_recv()
            for k in (1, 2):
                wo_direct(k).wait_recv()
                wo_pair(k, mine_q).start()
                wo_core(k, mine_q).start()

        @pl.loop(0, n_tp)
        def _(i):
            attend(i, s)

        @pl.when(s == 0)
        def _():
            direct(1, 1, 0).wait_recv()
            direct(2, 1, 1).wait_recv()
            for p in range(2):
                relay(1, p).start()
            for p in range(2):
                wo_relay(p).start()
            for k in (3, 2, 1):
                attn_copy(k, 0, peer[k]).start()

    loads[8].wait()

    def hand_over(k):
        wo_pair(k, pair_q).wait_recv()
        wo_last(k, pair_q).start()

    def project_out(k):
        if k > 0:
            wo_core(k, mine_q + 1 - 2 * dp).wait_recv()
            wo_last(k, pair_q + 1 - 2 * dp).wait_recv()
            for s in range(samples):
                attn_copy(k, s, peer[k]).wait_recv()

        @pl.loop(0, n_tp)
        def _(n):
            cols = pl.ds(pl.multiple_of(n * wid, wid), wid)
            part = jnp.dot(
                attn[k].reshape(samples * rows, qw), wo_all[k, :, cols], preferred_element_type=F32
            )
            acc[:, cols] = acc[:, cols] + part.astype(BF16).astype(F32)

    hand_over(1)
    hand_over(2)
    project_out(0)
    project_out(1)
    project_out(2)
    hand_over(3)
    project_out(3)

    @pl.loop(0, rows // CHUNK, unroll=2)
    def _(r):
        part = pl.ds(pl.multiple_of(r * CHUNK, CHUNK), CHUNK)
        both = []
        for s in range(samples):
            branch = acc[pl.ds(pl.multiple_of(s * rows + r * CHUNK, CHUNK), CHUNK), :]
            both.append((lat_all[0, s, part, :].astype(F32) + mod_g[s : s + 1, :] * branch).astype(BF16))
        out_ref[part] = jnp.swapaxes(jnp.stack(both), 0, 1)

    for copy in mod_copies + all_copies + ctx_copies:
        copy.wait_send()
    for s in range(samples):
        for p in range(2):
            direct(1, s, p).wait_send()
            direct(2, s, p).wait_send()
            relay(s, p).wait_send()
        for k in (1, 2, 3):
            attn_copy(k, s, peer[k]).wait_send()

        @pl.when(not_last)
        def _(s=s):
            halo_up(s).wait_send()

        @pl.when(not_first)
        def _(s=s):
            halo_down(s).wait_send()

    for p in range(2):
        wo_direct(1 + p).wait_send()
        wo_relay(p).wait_send()
    for k in (1, 2, 3):
        wo_pair(k, mine_q).wait_send()
        wo_core(k, mine_q).wait_send()
        wo_last(k, pair_q).wait_send()


def local(
    n_sp,
    n_tp,
    latent,
    context,
    condition,
    ctx_condition,
    norm_gain,
    w_shift,
    w_scale,
    w_gate,
    w_query,
    w_key,
    w_value,
    w_out,
    sink,
):
    rows, samples, width = latent.shape
    lc = context.shape[0]
    wid = w_shift.shape[1]
    depth = w_shift.shape[0]
    qw, kw = w_query.shape[1], w_key.shape[1]
    heads = qw // HEAD_DIM
    block = rows * n_tp
    assert n_tp == 4 and n_sp % 2 == 0 and qw % 64 == 0 and samples == 2 and kw == HEAD_DIM and rows == WINDOW and block % GRID_W == 0 and heads % 2 == 0
    quarter = HEAD_DIM // 4
    lane = np.arange(HEAD_DIM)
    freqs = 10000.0 ** (-(lane % quarter).astype(np.float32) / quarter)
    sign = np.where(lane % (2 * quarter) < quarter, -1.0, 1.0)

    def table(count):
        angle = np.arange(count, dtype=np.float32)[:, None] * freqs[None, :].astype(np.float32)
        return jnp.asarray(np.cos(angle), F32), jnp.asarray(np.sin(angle) * sign[None, :], F32)

    row_table = table(n_sp * block // GRID_W)
    col_table = table(GRID_W)
    hbm = pl.BlockSpec(memory_space=pl.ANY)
    vmem = pl.BlockSpec(memory_space=pltpu.VMEM)
    smem = pl.BlockSpec(memory_space=pltpu.SMEM)
    dma = pltpu.SemaphoreType.DMA
    mixed = pl.pallas_call(
        functools.partial(kernel, n_sp),
        out_shape=jax.ShapeDtypeStruct((rows, samples, width), BF16),
        in_specs=[hbm, hbm, vmem, vmem, vmem, hbm, hbm, hbm, hbm, hbm, hbm, hbm, smem, vmem, vmem, vmem, vmem],
        out_specs=vmem,
        scratch_shapes=[
            pltpu.VMEM((rows, samples, width), BF16),
            pltpu.VMEM((n_tp, samples, rows, width), BF16),
            pltpu.VMEM((lc, samples, width), BF16),
            pltpu.VMEM((3, depth, wid), BF16),
            pltpu.VMEM((width, qw + 2 * kw), BF16),
            pltpu.VMEM((n_tp, qw, width), BF16),
            pltpu.VMEM((8, depth), F32),
            pltpu.VMEM((n_sp, 8, 3 * wid), F32),
            pltpu.VMEM((n_tp, 8, 3 * wid), F32),
            pltpu.VMEM((8, width), F32),
            pltpu.VMEM((8, width), F32),
            pltpu.VMEM((8, width), F32),
            pltpu.VMEM((samples * max(rows, lc), width), BF16),
            pltpu.VMEM((samples, n_tp, heads * rows, HEAD_DIM), BF16),
            pltpu.VMEM((samples, block + 2 * WINDOW, 2 * kw), BF16),
            pltpu.VMEM((samples, lc * n_sp, 2 * kw), BF16),
            pltpu.VMEM((2 * n_tp, samples, rows, qw), BF16),
            pltpu.VMEM((samples * rows, width), F32),
            pltpu.VMEM((block, HEAD_DIM), F32),
            pltpu.VMEM((block, HEAD_DIM), F32),
            dma((9,)),
            dma((n_sp,)),
            dma((n_sp,)),
            dma((n_tp,)),
            dma((n_tp,)),
            dma((n_tp, samples, 2)),
            dma((n_tp, samples, 2)),
            dma((samples, 2)),
            dma((samples, 2)),
            dma((n_sp,)),
            dma((n_sp,)),
            dma((2, samples)),
            dma((2, samples)),
            dma((n_tp, samples)),
            dma((n_tp, samples)),
            dma((n_tp,)),
            dma((n_tp,)),
            dma((2,)),
            dma((2,)),
            dma((n_tp,)),
            dma((n_tp,)),
            dma((n_tp,)),
            dma((n_tp,)),
            dma((n_tp,)),
            dma((n_tp,)),
        ],
        compiler_params=pltpu.CompilerParams(
            collective_id=0, has_side_effects=True, vmem_limit_bytes=60 * 1024 * 1024
        ),
        name="step",
    )(
        latent,
        context,
        condition,
        ctx_condition,
        norm_gain[None],
        w_shift,
        w_scale,
        w_gate,
        w_query,
        w_key,
        w_value,
        w_out,
        sink[None],
        *row_table,
        *col_table,
    )
    return mixed


def solution(mesh):
    return jax.shard_map(
        functools.partial(local, mesh.shape["sp"], mesh.shape["tp"]),
        mesh=mesh,
        in_specs=(
            P(("sp", "tp"), "dp", None),
            P("sp", "dp", None),
            P("dp", "sp"),
            P("sp"),
            P(),
            P("sp", "tp"),
            P("sp", "tp"),
            P("sp", "tp"),
            P(None, "tp"),
            P(None, "tp"),
            P(None, "tp"),
            P("tp", None),
            P("tp"),
        ),
        out_specs=P(("sp", "tp"), "dp", None),
        check_vma=False,
    )
```

```python
import functools
import math

import jax
import jax.numpy as jnp
import numpy as np
from jax import lax
from jax.experimental import pallas as pl
from jax.experimental.pallas import tpu as pltpu
from jax.sharding import PartitionSpec as P

HEAD_DIM = 128
WINDOW = 128
GRID_W = 64
EPSILON = 1e-06
NEGATIVE = -1e30
MESH = pl.DeviceIdType.MESH
F32 = jnp.float32
BF16 = jnp.bfloat16
LOG2E = math.log2(math.e)
CHUNK = 16


def kernel(
    n_sp,
    lat_hbm,
    ctx_hbm,
    cond_ref,
    cctx_ref,
    gain_ref,
    wsh_hbm,
    wsc_hbm,
    wga_hbm,
    wq_hbm,
    wk_hbm,
    wv_hbm,
    wo_hbm,
    sink_ref,
    row_cos,
    row_sin,
    col_cos,
    col_sin,
    out_hbm,
    mixed,
    lat_raw,
    lat_all,
    ctx_v,
    wmod,
    wqkv,
    wo_all,
    act_s,
    mod_p,
    mod_all,
    mod_a,
    mod_b,
    mod_g,
    hbuf,
    qbuf,
    kvbuf,
    ckv,
    attn,
    acc,
    cos_ref,
    sin_ref,
    loc_sem,
    modp_s,
    modp_r,
    moda_s,
    moda_r,
    lat_s,
    lat_r,
    relay_s,
    relay_r,
    ctx_s,
    ctx_r,
    halo_s,
    halo_r,
    attn_s,
    attn_r,
    wo_s,
    wo_r,
    wod_s,
    wod_r,
    woz_s,
    woz_r,
    woc_s,
    woc_r,
    woe_s,
    woe_r,
    out_sem,
):
    rows, samples, width = lat_hbm.shape
    n_tp = mod_all.shape[0]
    wid = wmod.shape[2]
    qw = wq_hbm.shape[1]
    kw = wk_hbm.shape[1]
    heads = qw // HEAD_DIM
    lc = ctx_hbm.shape[0]
    block = rows * n_tp
    sp = lax.axis_index("sp")
    tp = lax.axis_index("tp")
    dp = lax.axis_index("dp")
    tx, ty = tp % 2, tp // 2
    peer = {1: 2 * ty + 1 - tx, 2: 2 * (1 - ty) + tx, 3: 3 - tp}

    def sp_peer(o):
        return lax.rem(sp + o, n_sp)

    loads = [
        pltpu.make_async_copy(wsh_hbm, wmod.at[0], loc_sem.at[0]),
        pltpu.make_async_copy(wsc_hbm, wmod.at[1], loc_sem.at[1]),
        pltpu.make_async_copy(wga_hbm, wmod.at[2], loc_sem.at[2]),
        pltpu.make_async_copy(ctx_hbm, ctx_v, loc_sem.at[3]),
        pltpu.make_async_copy(wk_hbm, wqkv.at[:, pl.ds(qw, kw)], loc_sem.at[4]),
        pltpu.make_async_copy(wv_hbm, wqkv.at[:, pl.ds(qw + kw, kw)], loc_sem.at[5]),
        pltpu.make_async_copy(lat_hbm, lat_raw, loc_sem.at[6]),
        pltpu.make_async_copy(wq_hbm, wqkv.at[:, pl.ds(0, qw)], loc_sem.at[7]),
        pltpu.make_async_copy(wo_hbm, wo_all.at[0], loc_sem.at[8]),
    ]
    for i in (0, 1, 2, 6, 3, 4, 5, 7, 8):
        loads[i].start()

    barrier = pltpu.get_barrier_semaphore()
    for o in range(1, n_sp):
        pl.semaphore_signal(barrier, inc=1, device_id={"sp": sp_peer(o)}, device_id_type=MESH)
    for k in (1, 2, 3):
        pl.semaphore_signal(barrier, inc=1, device_id={"tp": peer[k]}, device_id_type=MESH)

    pl.semaphore_signal(barrier, inc=1, device_id={"dp": 1 - dp}, device_id_type=MESH)

    def apart(src, at):
        return jnp.swapaxes(src[pl.ds(at, CHUNK)], 0, 1)

    pl.semaphore_wait(barrier, n_sp - 1 + n_tp)

    def remote(src, dst, ssem, rsem, dev):
        return pltpu.make_async_remote_copy(
            src_ref=src, dst_ref=dst, send_sem=ssem, recv_sem=rsem, device_id=dev, device_id_type=MESH
        )

    half = rows // 2

    def direct(k, s, p):
        part = pl.ds(p * half, half)
        return remote(
            lat_all.at[0, s, part], lat_all.at[k, s, part], lat_s.at[k, s, p], lat_r.at[k, s, p], {"tp": peer[k]}
        )

    def relay(s, p):
        part = pl.ds(p * half, half)
        return remote(
            lat_all.at[1 + p, s, part], lat_all.at[3, s, part], relay_s.at[s, p], relay_r.at[s, p], {"tp": peer[2 - p]}
        )

    zh = sp % 2
    quarter = qw // 4
    mine_q = 2 * zh + dp
    pair_q = 2 * (1 - zh) + dp

    def wo_rows(index, count=quarter, skip=0):
        return pl.ds(pl.multiple_of(index * quarter + skip, count), count)

    def wo_half(index, p):
        return wo_rows(index, quarter // 2, p * (quarter // 2))

    def wo_direct(k, p):
        part = wo_half(mine_q, p)
        return remote(wo_hbm.at[part], wo_all.at[k, part], wo_s.at[k, p], wo_r.at[k, p], {"tp": peer[k]})

    def wo_relay(p):
        part = wo_half(mine_q, p)
        return remote(
            wo_all.at[1 + p, part], wo_all.at[3, part], wod_s.at[p], wod_r.at[p], {"tp": peer[2 - p]}
        )

    def wo_pair(k, p, index):
        part = wo_all.at[k, wo_half(index, p)]
        return remote(part, part, woz_s.at[k, p], woz_r.at[k, p], {"sp": sp + 1 - 2 * zh})

    def wo_core(k, p, index):
        part = wo_all.at[k, wo_half(index, p)]
        return remote(part, part, woc_s.at[k, p], woc_r.at[k, p], {"dp": 1 - dp})

    def wo_share(k, p):
        wo_pair(k, p, mine_q).start()
        wo_core(k, p, mine_q).start()

    def wo_last(k, index):
        part = wo_all.at[k, wo_rows(index)]
        return remote(part, part, woe_s.at[k], woe_r.at[k], {"dp": 1 - dp})

    wo_direct(1, 0).start()
    wo_direct(2, 1).start()

    act_s[...] = jnp.zeros_like(act_s)
    cv = cond_ref[...].astype(F32)
    act_s[0:samples, :] = cv / (1.0 + jnp.exp(-cv))
    cc = cctx_ref[...].astype(F32).reshape(1, -1)
    act_s[samples : samples + 1, :] = cc / (1.0 + jnp.exp(-cc))
    both = act_s[...].astype(BF16)
    for m in range(3):
        loads[m].wait()
        mod_p[0, :, m * wid : (m + 1) * wid] = jnp.dot(both, wmod[m], preferred_element_type=F32)[0:4]
    mod_copies = [
        remote(mod_p.at[0], mod_p.at[o], modp_s.at[o], modp_r.at[o], {"sp": sp_peer(o)})
        for o in range(1, n_sp)
    ]
    for copy in mod_copies:
        copy.start()

    loads[6].wait()

    @pl.loop(0, rows // CHUNK)
    def _(c):
        at = pl.multiple_of(c * CHUNK, CHUNK)
        both = apart(lat_raw, at)
        for s in range(samples):
            lat_all[0, s, pl.ds(at, CHUNK), :] = both[s]

    grid_rows = block // GRID_W
    for by_row, by_col, table in ((row_cos, col_cos, cos_ref), (row_sin, col_sin, sin_ref)):
        left = lax.broadcasted_iota(jnp.int32, (GRID_W, HEAD_DIM), 1) < HEAD_DIM // 2
        for r in range(grid_rows):
            table[r * GRID_W : (r + 1) * GRID_W, :] = jnp.where(
                left, by_row[pl.ds(sp * grid_rows + r, 1), :], by_col[...]
            )

    for copy in mod_copies:
        copy.wait_recv()
    total = mod_p[0]
    for o in range(1, n_sp):
        total = total + mod_p[o]
    mod_all[tp] = total
    all_copies = [
        remote(mod_all.at[tp], mod_all.at[tp], moda_s.at[k], moda_r.at[k], {"tp": peer[k]})
        for k in (1, 2, 3)
    ]
    for copy in all_copies:
        copy.start()
    wo_direct(1, 1).start()
    wo_direct(2, 0).start()
    direct(1, 0, 0).start()
    direct(2, 0, 1).start()
    direct(1, 0, 1).start()
    direct(2, 0, 0).start()
    wo_direct(1, 0).wait_recv()
    wo_direct(2, 1).wait_recv()
    wo_share(1, 0)
    wo_share(2, 1)
    for k in (1, 2, 3):
        remote(
            mod_all.at[peer[k]], mod_all.at[peer[k]], moda_s.at[k], moda_r.at[k], {"tp": peer[k]}
        ).wait_recv()
    for t in range(n_tp):
        cols = slice(t * wid, (t + 1) * wid)
        mod_b[:, cols] = mod_all[t, :, 0:wid]
        mod_a[:, cols] = (1.0 + mod_all[t, :, wid : 2 * wid]) * gain_ref[:, cols]
        mod_g[:, cols] = mod_all[t, :, 2 * wid : 3 * wid]

    def modulate(values, mod_row):
        x = values.astype(F32)
        inv = lax.rsqrt(jnp.mean(x * x, axis=-1, keepdims=True) + EPSILON)
        row = pl.ds(mod_row, 1)
        return (x * inv * mod_a[row, :] + mod_b[row, :]).astype(BF16)

    def norm_rows(src, mod_row, base, count):
        @pl.loop(0, count // CHUNK, unroll=4)
        def _(c):
            at = pl.multiple_of(c * CHUNK, CHUNK)
            hbuf[pl.ds(base + at, CHUNK), :] = modulate(src[pl.ds(at, CHUNK), :], mod_row)

    for i in (3, 4, 5):
        loads[i].wait()
    ctx_at = pl.multiple_of(sp * lc, lc)

    @pl.loop(0, lc // CHUNK, unroll=2)
    def _(c):
        at = pl.multiple_of(c * CHUNK, CHUNK)
        both = apart(ctx_v, at)
        for s in range(samples):
            hbuf[pl.ds(s * lc + at, CHUNK), :] = modulate(both[s], samples)

    made = jnp.dot(hbuf[...], wqkv[:, qw : qw + 2 * kw], preferred_element_type=F32).astype(BF16)
    for s in range(samples):
        ckv[s, pl.ds(ctx_at, lc), :] = made[s * lc : (s + 1) * lc]

    mine = ckv.at[:, pl.ds(ctx_at, lc), :]
    ctx_copies = [
        remote(mine, mine, ctx_s.at[o], ctx_r.at[o], {"sp": sp_peer(o)}) for o in range(1, n_sp)
    ]
    for copy in ctx_copies:
        copy.start()

    wo_direct(1, 1).wait_recv()
    wo_direct(2, 0).wait_recv()
    direct(1, 0, 0).wait_recv()
    direct(2, 0, 1).wait_recv()
    for p in range(2):
        relay(0, p).start()
    for p in range(2):
        wo_relay(p).start()
    direct(1, 1, 0).start()
    direct(2, 1, 1).start()
    direct(1, 1, 1).start()
    direct(2, 1, 0).start()

    loads[7].wait()
    lane = lax.broadcasted_iota(jnp.int32, (rows, HEAD_DIM), 1)
    low = lane % (HEAD_DIM // 2) < HEAD_DIM // 4

    def turn(u, cos, sin):
        other = jnp.where(
            low, pltpu.roll(u, HEAD_DIM - HEAD_DIM // 4, 1), pltpu.roll(u, HEAD_DIM // 4, 1)
        )
        return u * cos + other * sin

    def halo_up(s):
        return remote(
            kvbuf.at[s, pl.ds(block, WINDOW), :],
            kvbuf.at[s, pl.ds(0, WINDOW), :],
            halo_s.at[0, s],
            halo_r.at[0, s],
            {"sp": lax.min(sp + 1, n_sp - 1)},
        )

    def halo_down(s):
        return remote(
            kvbuf.at[s, pl.ds(WINDOW, WINDOW), :],
            kvbuf.at[s, pl.ds(WINDOW + block, WINDOW), :],
            halo_s.at[1, s],
            halo_r.at[1, s],
            {"sp": lax.max(sp - 1, 0)},
        )

    not_first, not_last = sp > 0, sp < n_sp - 1

    @pl.when(sp == 0)
    def _():
        kvbuf[:, 0:WINDOW, :] = jnp.zeros((samples, WINDOW, 2 * kw), BF16)

    @pl.when(sp == n_sp - 1)
    def _():
        kvbuf[:, WINDOW + block :, :] = jnp.zeros((samples, WINDOW, 2 * kw), BF16)

    acc[...] = jnp.zeros_like(acc)

    def attn_copy(k, s, dest):
        return remote(attn.at[n_tp + k, s], attn.at[k, s], attn_s.at[k, s], attn_r.at[k, s], {"tp": dest})

    def project(s):
        @pl.loop(0, n_tp // 2)
        def _(j):
            @pl.when(j == 0)
            def _():
                direct(1, s, 1).wait_recv()

            @pl.when(j == 1)
            def _():
                direct(2, s, 0).wait_recv()
                relay(s, 0).wait_recv()
                relay(s, 1).wait_recv()

            by = ty + j - 2 * ty * j
            spots = []
            for e in range(2):
                norm_rows(lat_all.at[2 * j + e, s], s, e * rows, rows)
                b = 2 * by + (1 - tx if e else tx)
                at = pl.multiple_of(b * rows, rows)
                spots.append((b, at, cos_ref[pl.ds(at, rows), :], sin_ref[pl.ds(at, rows), :]))
            for c in range(heads // 2 + 1):
                prod = jnp.dot(
                    hbuf[0 : 2 * rows, :],
                    wqkv[:, c * 2 * HEAD_DIM : (c + 1) * 2 * HEAD_DIM],
                    preferred_element_type=F32,
                )
                for e, (b, at, cos, sin) in enumerate(spots):
                    part = prod[e * rows : (e + 1) * rows]
                    first = turn(part[:, :HEAD_DIM], cos, sin).astype(BF16)
                    if c < heads // 2:
                        second = turn(part[:, HEAD_DIM:], cos, sin).astype(BF16)
                        qbuf[s, b, 2 * c * rows : (2 * c + 1) * rows, :] = first
                        qbuf[s, b, (2 * c + 1) * rows : (2 * c + 2) * rows, :] = second
                    else:
                        kvbuf[s, pl.ds(WINDOW + at, rows), 0:HEAD_DIM] = first
                        kvbuf[s, pl.ds(WINDOW + at, rows), HEAD_DIM:] = part[:, HEAD_DIM:].astype(BF16)

            @pl.when(not_last & (by == 1))
            def _():
                halo_up(s).start()

            @pl.when(not_first & (by == 0))
            def _():
                halo_down(s).start()

    scale = HEAD_DIM ** (-0.5) * LOG2E
    seq = block * n_sp
    nums = (((1,), (1,)), ((), ()))

    span = 3 * WINDOW
    pair = 2 * rows
    row_id = lax.broadcasted_iota(jnp.int32, (pair, 1), 0)

    def attend(i, s):
        k = n_tp - 1 - i
        kx, ky = k % 2, k // 2
        b = 2 * (ty + ky - 2 * ty * ky) + tx + kx - 2 * tx * kx
        at = pl.multiple_of(b * rows, rows)
        slot = jnp.where(k == 0, 0, n_tp + k)

        @pl.when((b == 0) & not_first)
        def _():
            halo_up(s).wait_recv()

        @pl.when((b == n_tp - 1) & not_last)
        def _():
            halo_down(s).wait_recv()

        kc = ckv[s, :, 0:HEAD_DIM]
        vc = ckv[s, :, HEAD_DIM:]
        kl = kvbuf[s, pl.ds(at, span), 0:HEAD_DIM]
        vl = kvbuf[s, pl.ds(at, span), HEAD_DIM:]
        key = lax.broadcasted_iota(jnp.int32, (pair, span), 1)
        query = lax.broadcasted_iota(jnp.int32, (pair, span), 0) % rows
        pos = key + (sp * block + b * rows - WINDOW)
        allowed = (key >= query) & (key <= query + 2 * WINDOW) & (pos >= 0) & (pos < seq)
        for c in range(heads // 2):
            q = qbuf[s, b, c * pair : (c + 1) * pair, :]
            sc = lax.dot_general(q, kc, nums, preferred_element_type=F32)
            sl = lax.dot_general(q, kl, nums, preferred_element_type=F32)
            sl = jnp.where(allowed, sl, NEGATIVE)
            sink2 = jnp.where(row_id < rows, sink_ref[0, 2 * c], sink_ref[0, 2 * c + 1]) * LOG2E
            top = jnp.maximum(
                jnp.max(sc, axis=-1, keepdims=True), jnp.max(sl, axis=-1, keepdims=True)
            )
            top = jnp.maximum(top * scale, sink2)
            ec = jnp.exp2(sc * scale - top)
            el = jnp.exp2(sl * scale - top)
            total = (
                jnp.sum(ec, axis=-1, keepdims=True)
                + jnp.sum(el, axis=-1, keepdims=True)
                + jnp.exp2(sink2 - top)
            )
            o = jnp.dot(ec.astype(BF16), vc, preferred_element_type=F32)
            o = o + jnp.dot(el.astype(BF16), vl, preferred_element_type=F32)
            o = (o / total).astype(BF16)
            attn[slot, s, :, 2 * c * HEAD_DIM : (2 * c + 1) * HEAD_DIM] = o[:rows]
            attn[slot, s, :, (2 * c + 1) * HEAD_DIM : (2 * c + 2) * HEAD_DIM] = o[rows:]

        @pl.when((s == 1) & (k > 0))
        def _():
            attn_copy(k, s, b).start()

    @pl.loop(0, samples)
    def _(s):
        project(s)

        @pl.when(s == 0)
        def _():
            wo_share(1, 1)
            wo_share(2, 0)
            for o in range(1, n_sp):
                got = ckv.at[:, pl.ds(pl.multiple_of(sp_peer(n_sp - o) * lc, lc), lc), :]
                remote(got, got, ctx_s.at[o], ctx_r.at[o], {"sp": sp_peer(o)}).wait_recv()
            wo_relay(0).wait_recv()
            wo_share(3, 0)

        @pl.when(s == 1)
        def _():
            wo_relay(1).wait_recv()
            wo_share(3, 1)

        @pl.loop(0, n_tp)
        def _(i):
            attend(i, s)

        @pl.when(s == 0)
        def _():
            direct(1, 1, 0).wait_recv()
            direct(2, 1, 1).wait_recv()
            for p in range(2):
                relay(1, p).start()
            for k in (3, 2, 1):
                attn_copy(k, 0, peer[k]).start()

    loads[8].wait()

    def hand_over(k):
        for p in range(2):
            wo_pair(k, p, pair_q).wait_recv()
        wo_last(k, pair_q).start()

    def project_out(k):
        if k > 0:
            for p in range(2):
                wo_core(k, p, mine_q + 1 - 2 * dp).wait_recv()
            wo_last(k, pair_q + 1 - 2 * dp).wait_recv()
            for s in range(samples):
                attn_copy(k, s, peer[k]).wait_recv()

        @pl.loop(0, n_tp)
        def _(n):
            cols = pl.ds(pl.multiple_of(n * wid, wid), wid)
            part = jnp.dot(
                attn[k].reshape(samples * rows, qw), wo_all[k, :, cols], preferred_element_type=F32
            )
            total = acc[:, cols] + part.astype(BF16).astype(F32)
            if k != 1:
                acc[:, cols] = total
            else:
                both = []
                for s in range(samples):
                    branch = total[s * rows : (s + 1) * rows]
                    both.append(
                        (lat_all[0, s, :, cols].astype(F32) + mod_g[s : s + 1, cols] * branch).astype(BF16)
                    )
                mixed[:, :, cols] = jnp.swapaxes(jnp.stack(both), 0, 1)
                out_copy(n).start()

    def out_copy(n):
        cols = pl.ds(pl.multiple_of(n * wid, wid), wid)
        return pltpu.make_async_copy(mixed.at[:, :, cols], out_hbm.at[:, :, cols], out_sem.at[n])

    hand_over(1)
    hand_over(2)
    project_out(0)
    hand_over(3)
    project_out(3)
    project_out(2)
    project_out(1)

    for copy in mod_copies + all_copies + ctx_copies:
        copy.wait_send()
    for s in range(samples):
        for p in range(2):
            direct(1, s, p).wait_send()
            direct(2, s, p).wait_send()
            relay(s, p).wait_send()
        for k in (1, 2, 3):
            attn_copy(k, s, peer[k]).wait_send()

        @pl.when(not_last)
        def _(s=s):
            halo_up(s).wait_send()

        @pl.when(not_first)
        def _(s=s):
            halo_down(s).wait_send()

    for p in range(2):
        wo_direct(1, p).wait_send()
        wo_direct(2, p).wait_send()
        wo_relay(p).wait_send()
        for k in (1, 2, 3):
            wo_pair(k, p, mine_q).wait_send()
            wo_core(k, p, mine_q).wait_send()
    for k in (1, 2, 3):
        wo_last(k, pair_q).wait_send()
    for n in range(n_tp):
        out_copy(n).wait()


def local(
    n_sp,
    n_tp,
    latent,
    context,
    condition,
    ctx_condition,
    norm_gain,
    w_shift,
    w_scale,
    w_gate,
    w_query,
    w_key,
    w_value,
    w_out,
    sink,
):
    rows, samples, width = latent.shape
    lc = context.shape[0]
    wid = w_shift.shape[1]
    depth = w_shift.shape[0]
    qw, kw = w_query.shape[1], w_key.shape[1]
    heads = qw // HEAD_DIM
    block = rows * n_tp
    assert n_tp == 4 and n_sp % 2 == 0 and qw % 64 == 0 and samples == 2 and kw == HEAD_DIM and rows == WINDOW and block % GRID_W == 0 and heads % 2 == 0
    quarter = HEAD_DIM // 4
    lane = np.arange(HEAD_DIM)
    freqs = 10000.0 ** (-(lane % quarter).astype(np.float32) / quarter)
    sign = np.where(lane % (2 * quarter) < quarter, -1.0, 1.0)

    def table(count):
        angle = np.arange(count, dtype=np.float32)[:, None] * freqs[None, :].astype(np.float32)
        return jnp.asarray(np.cos(angle), F32), jnp.asarray(np.sin(angle) * sign[None, :], F32)

    row_table = table(n_sp * block // GRID_W)
    col_table = table(GRID_W)
    hbm = pl.BlockSpec(memory_space=pl.ANY)
    vmem = pl.BlockSpec(memory_space=pltpu.VMEM)
    smem = pl.BlockSpec(memory_space=pltpu.SMEM)
    dma = pltpu.SemaphoreType.DMA
    mixed = pl.pallas_call(
        functools.partial(kernel, n_sp),
        out_shape=jax.ShapeDtypeStruct((rows, samples, width), BF16),
        in_specs=[hbm, hbm, vmem, vmem, vmem, hbm, hbm, hbm, hbm, hbm, hbm, hbm, smem, vmem, vmem, vmem, vmem],
        out_specs=hbm,
        scratch_shapes=[
            pltpu.VMEM((rows, samples, width), BF16),
            pltpu.VMEM((rows, samples, width), BF16),
            pltpu.VMEM((n_tp, samples, rows, width), BF16),
            pltpu.VMEM((lc, samples, width), BF16),
            pltpu.VMEM((3, depth, wid), BF16),
            pltpu.VMEM((width, qw + 2 * kw), BF16),
            pltpu.VMEM((n_tp, qw, width), BF16),
            pltpu.VMEM((8, depth), F32),
            pltpu.VMEM((n_sp, 4, 3 * wid), F32),
            pltpu.VMEM((n_tp, 4, 3 * wid), F32),
            pltpu.VMEM((4, width), F32),
            pltpu.VMEM((4, width), F32),
            pltpu.VMEM((4, width), F32),
            pltpu.VMEM((samples * max(rows, lc), width), BF16),
            pltpu.VMEM((samples, n_tp, heads * rows, HEAD_DIM), BF16),
            pltpu.VMEM((samples, block + 2 * WINDOW, 2 * kw), BF16),
            pltpu.VMEM((samples, lc * n_sp, 2 * kw), BF16),
            pltpu.VMEM((2 * n_tp, samples, rows, qw), BF16),
            pltpu.VMEM((samples * rows, width), F32),
            pltpu.VMEM((block, HEAD_DIM), F32),
            pltpu.VMEM((block, HEAD_DIM), F32),
            dma((9,)),
            dma((n_sp,)),
            dma((n_sp,)),
            dma((n_tp,)),
            dma((n_tp,)),
            dma((n_tp, samples, 2)),
            dma((n_tp, samples, 2)),
            dma((samples, 2)),
            dma((samples, 2)),
            dma((n_sp,)),
            dma((n_sp,)),
            dma((2, samples)),
            dma((2, samples)),
            dma((n_tp, samples)),
            dma((n_tp, samples)),
            dma((n_tp, 2)),
            dma((n_tp, 2)),
            dma((2,)),
            dma((2,)),
            dma((n_tp, 2)),
            dma((n_tp, 2)),
            dma((n_tp, 2)),
            dma((n_tp, 2)),
            dma((n_tp,)),
            dma((n_tp,)),
            dma((n_tp,)),
        ],
        compiler_params=pltpu.CompilerParams(
            collective_id=0, has_side_effects=True, vmem_limit_bytes=60 * 1024 * 1024
        ),
        name="step",
    )(
        latent,
        context,
        condition,
        ctx_condition,
        norm_gain[None],
        w_shift,
        w_scale,
        w_gate,
        w_query,
        w_key,
        w_value,
        w_out,
        sink[None],
        *row_table,
        *col_table,
    )
    pieces = 4
    piece = rows // pieces

    def hand_out(src, dst, held, sems):
        def copy(i, out):
            part = pl.ds(i * piece, piece)
            if out:
                return pltpu.make_async_copy(held.at[part], dst.at[part], sems.at[1, i])
            return pltpu.make_async_copy(src.at[part], held.at[part], sems.at[0, i])

        for i in range(pieces):
            copy(i, False).start()
        for i in range(pieces):
            copy(i, False).wait()
            copy(i, True).start()
        for i in range(pieces):
            copy(i, True).wait()

    return pl.pallas_call(
        hand_out,
        out_shape=jax.ShapeDtypeStruct(mixed.shape, BF16),
        in_specs=[hbm],
        out_specs=hbm,
        scratch_shapes=[pltpu.VMEM((rows, samples, width), BF16), dma((2, pieces))],
        name="hand_out",
    )(mixed)


def solution(mesh):
    return jax.shard_map(
        functools.partial(local, mesh.shape["sp"], mesh.shape["tp"]),
        mesh=mesh,
        in_specs=(
            P(("sp", "tp"), "dp", None),
            P("sp", "dp", None),
            P("dp", "sp"),
            P("sp"),
            P(),
            P("sp", "tp"),
            P("sp", "tp"),
            P("sp", "tp"),
            P(None, "tp"),
            P(None, "tp"),
            P(None, "tp"),
            P("tp", None),
            P("tp"),
        ),
        out_specs=P(("sp", "tp"), "dp", None),
        check_vma=False,
    )
```

```python
import functools
import math

import jax
import jax.numpy as jnp
import numpy as np
from jax import lax
from jax.experimental import pallas as pl
from jax.experimental.pallas import tpu as pltpu
from jax.sharding import PartitionSpec as P

HEAD_DIM = 128
WINDOW = 128
GRID_W = 64
EPSILON = 1e-06
NEGATIVE = -1e30
MESH = pl.DeviceIdType.MESH
F32 = jnp.float32
BF16 = jnp.bfloat16
LOG2E = math.log2(math.e)
CHUNK = 16
OUT_PIECES = 2


def kernel(
    n_sp,
    lat_hbm,
    ctx_hbm,
    cond_ref,
    cctx_ref,
    gain_ref,
    wsh_hbm,
    wsc_hbm,
    wga_hbm,
    wq_hbm,
    wk_hbm,
    wv_hbm,
    wo_hbm,
    sink_ref,
    row_cos,
    row_sin,
    col_cos,
    col_sin,
    out_hbm,
    mixed,
    lat_raw,
    lat_all,
    ctx_v,
    wmod,
    wqkv,
    wo_all,
    act_s,
    mod_p,
    mod_all,
    mod_a,
    mod_b,
    mod_g,
    hbuf,
    qbuf,
    kvbuf,
    ckv,
    attn,
    acc,
    cos_ref,
    sin_ref,
    loc_sem,
    modp_s,
    modp_r,
    moda_s,
    moda_r,
    lat_s,
    lat_r,
    relay_s,
    relay_r,
    ctx_s,
    ctx_r,
    halo_s,
    halo_r,
    attn_s,
    attn_r,
    wo_s,
    wo_r,
    wod_s,
    wod_r,
    woz_s,
    woz_r,
    woc_s,
    woc_r,
    woe_s,
    woe_r,
    out_sem,
):
    rows, samples, width = lat_hbm.shape
    n_tp = mod_all.shape[0]
    wid = wmod.shape[2]
    qw = wq_hbm.shape[1]
    kw = wk_hbm.shape[1]
    heads = qw // HEAD_DIM
    lc = ctx_hbm.shape[0]
    block = rows * n_tp
    sp = lax.axis_index("sp")
    tp = lax.axis_index("tp")
    dp = lax.axis_index("dp")
    tx, ty = tp % 2, tp // 2
    peer = {1: 2 * ty + 1 - tx, 2: 2 * (1 - ty) + tx, 3: 3 - tp}

    def sp_peer(o):
        return lax.rem(sp + o, n_sp)

    loads = [
        pltpu.make_async_copy(wsh_hbm, wmod.at[0], loc_sem.at[0]),
        pltpu.make_async_copy(wsc_hbm, wmod.at[1], loc_sem.at[1]),
        pltpu.make_async_copy(wga_hbm, wmod.at[2], loc_sem.at[2]),
        pltpu.make_async_copy(ctx_hbm, ctx_v, loc_sem.at[3]),
        pltpu.make_async_copy(wk_hbm, wqkv.at[:, pl.ds(qw, kw)], loc_sem.at[4]),
        pltpu.make_async_copy(wv_hbm, wqkv.at[:, pl.ds(qw + kw, kw)], loc_sem.at[5]),
        pltpu.make_async_copy(lat_hbm, lat_raw, loc_sem.at[6]),
        pltpu.make_async_copy(wq_hbm, wqkv.at[:, pl.ds(0, qw)], loc_sem.at[7]),
        pltpu.make_async_copy(wo_hbm, wo_all.at[0], loc_sem.at[8]),
    ]
    for i in (8, 0, 1, 2, 6, 3, 4, 5, 7):
        loads[i].start()

    barrier = pltpu.get_barrier_semaphore()
    for o in range(1, n_sp):
        pl.semaphore_signal(barrier, inc=1, device_id={"sp": sp_peer(o)}, device_id_type=MESH)
    for k in (1, 2, 3):
        pl.semaphore_signal(barrier, inc=1, device_id={"tp": peer[k]}, device_id_type=MESH)

    pl.semaphore_signal(barrier, inc=1, device_id={"dp": 1 - dp}, device_id_type=MESH)

    def apart(src, at):
        return jnp.swapaxes(src[pl.ds(at, CHUNK)], 0, 1)

    pl.semaphore_wait(barrier, n_sp - 1 + n_tp)

    def remote(src, dst, ssem, rsem, dev):
        return pltpu.make_async_remote_copy(
            src_ref=src, dst_ref=dst, send_sem=ssem, recv_sem=rsem, device_id=dev, device_id_type=MESH
        )

    half = rows // 2

    def direct(k, s, p):
        part = pl.ds(p * half, half)
        return remote(
            lat_all.at[0, s, part], lat_all.at[k, s, part], lat_s.at[k, s, p], lat_r.at[k, s, p], {"tp": peer[k]}
        )

    def relay(s, p):
        part = pl.ds(p * half, half)
        return remote(
            lat_all.at[1 + p, s, part], lat_all.at[3, s, part], relay_s.at[s, p], relay_r.at[s, p], {"tp": peer[2 - p]}
        )

    zh = sp % 2
    quarter = qw // 4
    mine_q = 2 * zh + dp
    pair_q = 2 * (1 - zh) + dp

    def wo_rows(index, count=quarter, skip=0):
        return pl.ds(pl.multiple_of(index * quarter + skip, count), count)

    def wo_half(index, p):
        return wo_rows(index, quarter // 2, p * (quarter // 2))

    def wo_direct(k, p):
        part = wo_half(mine_q, p)
        return remote(wo_all.at[0, part], wo_all.at[k, part], wo_s.at[k, p], wo_r.at[k, p], {"tp": peer[k]})

    def wo_relay(p):
        part = wo_half(mine_q, p)
        return remote(
            wo_all.at[1 + p, part], wo_all.at[3, part], wod_s.at[p], wod_r.at[p], {"tp": peer[2 - p]}
        )

    def wo_pair(k, p, index):
        part = wo_all.at[k, wo_half(index, p)]
        return remote(part, part, woz_s.at[k, p], woz_r.at[k, p], {"sp": sp + 1 - 2 * zh})

    def wo_core(k, p, index):
        part = wo_all.at[k, wo_half(index, p)]
        return remote(part, part, woc_s.at[k, p], woc_r.at[k, p], {"dp": 1 - dp})

    def wo_share(k, p):
        wo_pair(k, p, mine_q).start()
        wo_core(k, p, mine_q).start()

    def wo_last(k, index):
        part = wo_all.at[k, wo_rows(index)]
        return remote(part, part, woe_s.at[k], woe_r.at[k], {"dp": 1 - dp})

    loads[8].wait()
    wo_direct(1, 0).start()
    wo_direct(2, 1).start()

    act_s[...] = jnp.zeros_like(act_s)
    cv = cond_ref[...].astype(F32)
    act_s[0:samples, :] = cv / (1.0 + jnp.exp(-cv))
    cc = cctx_ref[...].astype(F32).reshape(1, -1)
    act_s[samples : samples + 1, :] = cc / (1.0 + jnp.exp(-cc))
    both = act_s[...].astype(BF16)
    for m in range(3):
        loads[m].wait()
        mod_p[0, :, m * wid : (m + 1) * wid] = jnp.dot(both, wmod[m], preferred_element_type=F32)[0:4]
    mod_copies = [
        remote(mod_p.at[0], mod_p.at[o], modp_s.at[o], modp_r.at[o], {"sp": sp_peer(o)})
        for o in range(1, n_sp)
    ]
    for copy in mod_copies:
        copy.start()

    loads[6].wait()

    @pl.loop(0, rows // CHUNK)
    def _(c):
        at = pl.multiple_of(c * CHUNK, CHUNK)
        both = apart(lat_raw, at)
        for s in range(samples):
            lat_all[0, s, pl.ds(at, CHUNK), :] = both[s]

    grid_rows = block // GRID_W
    for by_row, by_col, table in ((row_cos, col_cos, cos_ref), (row_sin, col_sin, sin_ref)):
        left = lax.broadcasted_iota(jnp.int32, (GRID_W, HEAD_DIM), 1) < HEAD_DIM // 2
        for r in range(grid_rows):
            table[r * GRID_W : (r + 1) * GRID_W, :] = jnp.where(
                left, by_row[pl.ds(sp * grid_rows + r, 1), :], by_col[...]
            )

    for copy in mod_copies:
        copy.wait_recv()
    total = mod_p[0]
    for o in range(1, n_sp):
        total = total + mod_p[o]
    mod_all[tp] = total
    all_copies = [
        remote(mod_all.at[tp], mod_all.at[tp], moda_s.at[k], moda_r.at[k], {"tp": peer[k]})
        for k in (1, 2, 3)
    ]
    for copy in all_copies:
        copy.start()
    wo_direct(1, 1).start()
    wo_direct(2, 0).start()
    direct(1, 0, 0).start()
    direct(2, 0, 1).start()
    direct(1, 0, 1).start()
    direct(2, 0, 0).start()
    wo_direct(1, 0).wait_recv()
    wo_direct(2, 1).wait_recv()
    wo_share(1, 0)
    wo_share(2, 1)
    for k in (1, 2, 3):
        remote(
            mod_all.at[peer[k]], mod_all.at[peer[k]], moda_s.at[k], moda_r.at[k], {"tp": peer[k]}
        ).wait_recv()
    for t in range(n_tp):
        cols = slice(t * wid, (t + 1) * wid)
        mod_b[:, cols] = mod_all[t, :, 0:wid]
        mod_a[:, cols] = (1.0 + mod_all[t, :, wid : 2 * wid]) * gain_ref[:, cols]
        mod_g[:, cols] = mod_all[t, :, 2 * wid : 3 * wid]

    def modulate(values, mod_row):
        x = values.astype(F32)
        inv = lax.rsqrt(jnp.mean(x * x, axis=-1, keepdims=True) + EPSILON)
        row = pl.ds(mod_row, 1)
        return (x * inv * mod_a[row, :] + mod_b[row, :]).astype(BF16)

    def norm_rows(src, mod_row, base, count):
        @pl.loop(0, count // CHUNK, unroll=4)
        def _(c):
            at = pl.multiple_of(c * CHUNK, CHUNK)
            hbuf[pl.ds(base + at, CHUNK), :] = modulate(src[pl.ds(at, CHUNK), :], mod_row)

    for i in (3, 4, 5):
        loads[i].wait()
    ctx_at = pl.multiple_of(sp * lc, lc)

    @pl.loop(0, lc // CHUNK, unroll=2)
    def _(c):
        at = pl.multiple_of(c * CHUNK, CHUNK)
        both = apart(ctx_v, at)
        for s in range(samples):
            hbuf[pl.ds(s * lc + at, CHUNK), :] = modulate(both[s], samples)

    made = jnp.dot(hbuf[...], wqkv[:, qw : qw + 2 * kw], preferred_element_type=F32).astype(BF16)
    for s in range(samples):
        ckv[s, pl.ds(ctx_at, lc), :] = made[s * lc : (s + 1) * lc]

    mine = ckv.at[:, pl.ds(ctx_at, lc), :]
    ctx_copies = [
        remote(mine, mine, ctx_s.at[o], ctx_r.at[o], {"sp": sp_peer(o)}) for o in range(1, n_sp)
    ]
    for copy in ctx_copies:
        copy.start()

    wo_direct(1, 1).wait_recv()
    wo_direct(2, 0).wait_recv()
    direct(1, 0, 0).wait_recv()
    direct(2, 0, 1).wait_recv()
    for p in range(2):
        relay(0, p).start()
    for p in range(2):
        wo_relay(p).start()
    direct(1, 1, 0).start()
    direct(2, 1, 1).start()
    direct(1, 1, 1).start()
    direct(2, 1, 0).start()

    loads[7].wait()
    lane = lax.broadcasted_iota(jnp.int32, (rows, HEAD_DIM), 1)
    low = lane % (HEAD_DIM // 2) < HEAD_DIM // 4

    def turn(u, cos, sin):
        other = jnp.where(
            low, pltpu.roll(u, HEAD_DIM - HEAD_DIM // 4, 1), pltpu.roll(u, HEAD_DIM // 4, 1)
        )
        return u * cos + other * sin

    def halo_up(s):
        return remote(
            kvbuf.at[s, pl.ds(block, WINDOW), :],
            kvbuf.at[s, pl.ds(0, WINDOW), :],
            halo_s.at[0, s],
            halo_r.at[0, s],
            {"sp": lax.min(sp + 1, n_sp - 1)},
        )

    def halo_down(s):
        return remote(
            kvbuf.at[s, pl.ds(WINDOW, WINDOW), :],
            kvbuf.at[s, pl.ds(WINDOW + block, WINDOW), :],
            halo_s.at[1, s],
            halo_r.at[1, s],
            {"sp": lax.max(sp - 1, 0)},
        )

    not_first, not_last = sp > 0, sp < n_sp - 1

    @pl.when(sp == 0)
    def _():
        kvbuf[:, 0:WINDOW, :] = jnp.zeros((samples, WINDOW, 2 * kw), BF16)

    @pl.when(sp == n_sp - 1)
    def _():
        kvbuf[:, WINDOW + block :, :] = jnp.zeros((samples, WINDOW, 2 * kw), BF16)

    acc[...] = jnp.zeros_like(acc)

    def attn_copy(k, s, dest):
        return remote(attn.at[n_tp + k, s], attn.at[k, s], attn_s.at[k, s], attn_r.at[k, s], {"tp": dest})

    def project(blocks):
        spots = []
        for e, (k, s) in enumerate(blocks):
            norm_rows(lat_all.at[k, s], s, e * rows, rows)
            kx, ky = k % 2, k // 2
            b = 2 * (ty + ky - 2 * ty * ky) + tx + kx - 2 * tx * kx
            at = pl.multiple_of(b * rows, rows)
            spots.append((s, b, at, cos_ref[pl.ds(at, rows), :], sin_ref[pl.ds(at, rows), :]))
        for c in range(heads // 2 + 1):
            prod = jnp.dot(
                hbuf[0 : len(blocks) * rows, :],
                wqkv[:, c * 2 * HEAD_DIM : (c + 1) * 2 * HEAD_DIM],
                preferred_element_type=F32,
            )
            for e, (s, b, at, cos, sin) in enumerate(spots):
                part = prod[e * rows : (e + 1) * rows]
                first = turn(part[:, :HEAD_DIM], cos, sin).astype(BF16)
                if c < heads // 2:
                    second = turn(part[:, HEAD_DIM:], cos, sin).astype(BF16)
                    qbuf[s, b, 2 * c * rows : (2 * c + 1) * rows, :] = first
                    qbuf[s, b, (2 * c + 1) * rows : (2 * c + 2) * rows, :] = second
                else:
                    kvbuf[s, pl.ds(WINDOW + at, rows), 0:HEAD_DIM] = first
                    kvbuf[s, pl.ds(WINDOW + at, rows), HEAD_DIM:] = part[:, HEAD_DIM:].astype(BF16)

    def send_edges(s, bottom, top):
        @pl.when(not_last & top)
        def _():
            halo_up(s).start()

        @pl.when(not_first & bottom)
        def _():
            halo_down(s).start()

    at_first, at_last = tp == 0, tp == n_tp - 1
    inner = (tp > 0) & (tp < n_tp - 1)
    project([(0, s) for s in range(samples)])
    for s in range(samples):
        send_edges(s, at_first, at_last)

    scale = HEAD_DIM ** (-0.5) * LOG2E
    seq = block * n_sp
    nums = (((1,), (1,)), ((), ()))

    span = 3 * WINDOW
    pair = 2 * rows
    row_id = lax.broadcasted_iota(jnp.int32, (pair, 1), 0)

    def hand_over(k):
        for p in range(2):
            wo_pair(k, p, pair_q).wait_recv()
        wo_last(k, pair_q).start()

    def attend(i, s):
        k = jnp.where(i == 0, 1, jnp.where(i < n_tp - 1, n_tp - i, 0))
        kx, ky = k % 2, k // 2
        b = 2 * (ty + ky - 2 * ty * ky) + tx + kx - 2 * tx * kx
        at = pl.multiple_of(b * rows, rows)
        slot = jnp.where(k == 0, 0, n_tp + k)

        @pl.when((b == 0) & not_first)
        def _():
            halo_up(s).wait_recv()

        @pl.when((b == n_tp - 1) & not_last)
        def _():
            halo_down(s).wait_recv()

        kc = ckv[s, :, 0:HEAD_DIM]
        vc = ckv[s, :, HEAD_DIM:]
        kl = kvbuf[s, pl.ds(at, span), 0:HEAD_DIM]
        vl = kvbuf[s, pl.ds(at, span), HEAD_DIM:]
        key = lax.broadcasted_iota(jnp.int32, (pair, span), 1)
        query = lax.broadcasted_iota(jnp.int32, (pair, span), 0) % rows
        pos = key + (sp * block + b * rows - WINDOW)
        allowed = (key >= query) & (key <= query + 2 * WINDOW) & (pos >= 0) & (pos < seq)
        for c in range(heads // 2):
            q = qbuf[s, b, c * pair : (c + 1) * pair, :]
            sc = lax.dot_general(q, kc, nums, preferred_element_type=F32)
            sl = lax.dot_general(q, kl, nums, preferred_element_type=F32)
            sl = jnp.where(allowed, sl, NEGATIVE)
            sink2 = jnp.where(row_id < rows, sink_ref[0, 2 * c], sink_ref[0, 2 * c + 1]) * LOG2E
            top = jnp.maximum(
                jnp.max(sc, axis=-1, keepdims=True), jnp.max(sl, axis=-1, keepdims=True)
            )
            top = jnp.maximum(top * scale, sink2)
            ec = jnp.exp2(sc * scale - top)
            el = jnp.exp2(sl * scale - top)
            total = (
                jnp.sum(ec, axis=-1, keepdims=True)
                + jnp.sum(el, axis=-1, keepdims=True)
                + jnp.exp2(sink2 - top)
            )
            o = jnp.dot(ec.astype(BF16), vc, preferred_element_type=F32)
            o = o + jnp.dot(el.astype(BF16), vl, preferred_element_type=F32)
            o = (o / total).astype(BF16)
            attn[slot, s, :, 2 * c * HEAD_DIM : (2 * c + 1) * HEAD_DIM] = o[:rows]
            attn[slot, s, :, (2 * c + 1) * HEAD_DIM : (2 * c + 2) * HEAD_DIM] = o[rows:]

        @pl.when((s == 1) & (k > 0))
        def _():
            attn_copy(k, s, b).start()

    @pl.loop(0, samples)
    def _(s):
        direct(1, s, 1).wait_recv()
        direct(2, s, 0).wait_recv()
        project([(1, s), (2, s)])
        send_edges(s, inner, inner)

        @pl.loop(0, n_tp)
        def _(i):
            @pl.when(i == s)
            def _():
                relay(s, 0).wait_recv()
                relay(s, 1).wait_recv()
                project([(3, s)])
                send_edges(s, at_last, at_first)

                @pl.when(s == 0)
                def _():
                    wo_share(1, 1)
                    wo_share(2, 0)
                    for o in range(1, n_sp):
                        got = ckv.at[:, pl.ds(pl.multiple_of(sp_peer(n_sp - o) * lc, lc), lc), :]
                        remote(got, got, ctx_s.at[o], ctx_r.at[o], {"sp": sp_peer(o)}).wait_recv()
                    wo_relay(0).wait_recv()
                    wo_share(3, 0)

                @pl.when(s == 1)
                def _():
                    wo_relay(1).wait_recv()
                    wo_share(3, 1)
                    hand_over(1)
                    hand_over(2)

            attend(i, s)

        @pl.when(s == 0)
        def _():
            direct(1, 1, 0).wait_recv()
            direct(2, 1, 1).wait_recv()
            for p in range(2):
                relay(1, p).start()
            for k in (3, 2, 1):
                attn_copy(k, 0, peer[k]).start()

    def project_out(k):
        if k > 0:
            for p in range(2):
                wo_core(k, p, mine_q + 1 - 2 * dp).wait_recv()
            wo_last(k, pair_q + 1 - 2 * dp).wait_recv()
            for s in range(samples):
                attn_copy(k, s, peer[k]).wait_recv()

        @pl.loop(0, OUT_PIECES)
        def _(n):
            cols = out_cols(n)
            part = jnp.dot(
                attn[k].reshape(samples * rows, qw), wo_all[k, :, cols], preferred_element_type=F32
            )
            total = acc[:, cols] + part.astype(BF16).astype(F32)
            if k < n_tp - 1:
                acc[:, cols] = total
            else:
                both = []
                for s in range(samples):
                    branch = total[s * rows : (s + 1) * rows]
                    both.append(
                        (lat_all[0, s, :, cols].astype(F32) + mod_g[s : s + 1, cols] * branch).astype(BF16)
                    )
                mixed[:, :, cols] = jnp.swapaxes(jnp.stack(both), 0, 1)
                out_copy(n).start()

    def out_cols(n):
        span = width // OUT_PIECES
        return pl.ds(pl.multiple_of(n * span, span), span)

    def out_copy(n):
        cols = out_cols(n)
        return pltpu.make_async_copy(mixed.at[:, :, cols], out_hbm.at[:, :, cols], out_sem.at[n])

    hand_over(3)
    for k in range(n_tp):
        project_out(k)

    for copy in mod_copies + all_copies + ctx_copies:
        copy.wait_send()
    for s in range(samples):
        for p in range(2):
            direct(1, s, p).wait_send()
            direct(2, s, p).wait_send()
            relay(s, p).wait_send()
        for k in (1, 2, 3):
            attn_copy(k, s, peer[k]).wait_send()

        @pl.when(not_last)
        def _(s=s):
            halo_up(s).wait_send()

        @pl.when(not_first)
        def _(s=s):
            halo_down(s).wait_send()

    for p in range(2):
        wo_direct(1, p).wait_send()
        wo_direct(2, p).wait_send()
        wo_relay(p).wait_send()
        for k in (1, 2, 3):
            wo_pair(k, p, mine_q).wait_send()
            wo_core(k, p, mine_q).wait_send()
    for k in (1, 2, 3):
        wo_last(k, pair_q).wait_send()
    for n in range(OUT_PIECES):
        out_copy(n).wait()


def local(
    n_sp,
    n_tp,
    latent,
    context,
    condition,
    ctx_condition,
    norm_gain,
    w_shift,
    w_scale,
    w_gate,
    w_query,
    w_key,
    w_value,
    w_out,
    sink,
):
    rows, samples, width = latent.shape
    lc = context.shape[0]
    wid = w_shift.shape[1]
    depth = w_shift.shape[0]
    qw, kw = w_query.shape[1], w_key.shape[1]
    heads = qw // HEAD_DIM
    block = rows * n_tp
    assert n_tp == 4 and n_sp % 2 == 0 and qw % 64 == 0 and samples == 2 and kw == HEAD_DIM and rows == WINDOW and block % GRID_W == 0 and heads % 2 == 0
    quarter = HEAD_DIM // 4
    lane = np.arange(HEAD_DIM)
    freqs = 10000.0 ** (-(lane % quarter).astype(np.float32) / quarter)
    sign = np.where(lane % (2 * quarter) < quarter, -1.0, 1.0)

    def table(count):
        angle = np.arange(count, dtype=np.float32)[:, None] * freqs[None, :].astype(np.float32)
        return jnp.asarray(np.cos(angle), F32), jnp.asarray(np.sin(angle) * sign[None, :], F32)

    row_table = table(n_sp * block // GRID_W)
    col_table = table(GRID_W)
    hbm = pl.BlockSpec(memory_space=pl.ANY)
    vmem = pl.BlockSpec(memory_space=pltpu.VMEM)
    smem = pl.BlockSpec(memory_space=pltpu.SMEM)
    dma = pltpu.SemaphoreType.DMA
    mixed = pl.pallas_call(
        functools.partial(kernel, n_sp),
        out_shape=jax.ShapeDtypeStruct((rows, samples, width), BF16),
        in_specs=[hbm, hbm, vmem, vmem, vmem, hbm, hbm, hbm, hbm, hbm, hbm, hbm, smem, vmem, vmem, vmem, vmem],
        out_specs=hbm,
        scratch_shapes=[
            pltpu.VMEM((rows, samples, width), BF16),
            pltpu.VMEM((rows, samples, width), BF16),
            pltpu.VMEM((n_tp, samples, rows, width), BF16),
            pltpu.VMEM((lc, samples, width), BF16),
            pltpu.VMEM((3, depth, wid), BF16),
            pltpu.VMEM((width, qw + 2 * kw), BF16),
            pltpu.VMEM((n_tp, qw, width), BF16),
            pltpu.VMEM((8, depth), F32),
            pltpu.VMEM((n_sp, 4, 3 * wid), F32),
            pltpu.VMEM((n_tp, 4, 3 * wid), F32),
            pltpu.VMEM((4, width), F32),
            pltpu.VMEM((4, width), F32),
            pltpu.VMEM((4, width), F32),
            pltpu.VMEM((samples * max(rows, lc), width), BF16),
            pltpu.VMEM((samples, n_tp, heads * rows, HEAD_DIM), BF16),
            pltpu.VMEM((samples, block + 2 * WINDOW, 2 * kw), BF16),
            pltpu.VMEM((samples, lc * n_sp, 2 * kw), BF16),
            pltpu.VMEM((2 * n_tp, samples, rows, qw), BF16),
            pltpu.VMEM((samples * rows, width), F32),
            pltpu.VMEM((block, HEAD_DIM), F32),
            pltpu.VMEM((block, HEAD_DIM), F32),
            dma((9,)),
            dma((n_sp,)),
            dma((n_sp,)),
            dma((n_tp,)),
            dma((n_tp,)),
            dma((n_tp, samples, 2)),
            dma((n_tp, samples, 2)),
            dma((samples, 2)),
            dma((samples, 2)),
            dma((n_sp,)),
            dma((n_sp,)),
            dma((2, samples)),
            dma((2, samples)),
            dma((n_tp, samples)),
            dma((n_tp, samples)),
            dma((n_tp, 2)),
            dma((n_tp, 2)),
            dma((2,)),
            dma((2,)),
            dma((n_tp, 2)),
            dma((n_tp, 2)),
            dma((n_tp, 2)),
            dma((n_tp, 2)),
            dma((n_tp,)),
            dma((n_tp,)),
            dma((OUT_PIECES,)),
        ],
        compiler_params=pltpu.CompilerParams(
            collective_id=0, has_side_effects=True, vmem_limit_bytes=60 * 1024 * 1024
        ),
        name="step",
    )(
        latent,
        context,
        condition,
        ctx_condition,
        norm_gain[None],
        w_shift,
        w_scale,
        w_gate,
        w_query,
        w_key,
        w_value,
        w_out,
        sink[None],
        *row_table,
        *col_table,
    )
    pieces = 4
    piece = rows // pieces

    def hand_out(src, dst, held, sems):
        def copy(i, out):
            part = pl.ds(i * piece, piece)
            if out:
                return pltpu.make_async_copy(held.at[part], dst.at[part], sems.at[1, i])
            return pltpu.make_async_copy(src.at[part], held.at[part], sems.at[0, i])

        for i in range(pieces):
            copy(i, False).start()
        for i in range(pieces):
            copy(i, False).wait()
            copy(i, True).start()
        for i in range(pieces):
            copy(i, True).wait()

    return pl.pallas_call(
        hand_out,
        out_shape=jax.ShapeDtypeStruct(mixed.shape, BF16),
        in_specs=[hbm],
        out_specs=hbm,
        scratch_shapes=[pltpu.VMEM((rows, samples, width), BF16), dma((2, pieces))],
        name="hand_out",
    )(mixed)


def solution(mesh):
    return jax.shard_map(
        functools.partial(local, mesh.shape["sp"], mesh.shape["tp"]),
        mesh=mesh,
        in_specs=(
            P(("sp", "tp"), "dp", None),
            P("sp", "dp", None),
            P("dp", "sp"),
            P("sp"),
            P(),
            P("sp", "tp"),
            P("sp", "tp"),
            P("sp", "tp"),
            P(None, "tp"),
            P(None, "tp"),
            P(None, "tp"),
            P("tp", None),
            P("tp"),
        ),
        out_specs=P(("sp", "tp"), "dp", None),
        check_vma=False,
    )
```

```python
import functools
import math

import jax
import jax.numpy as jnp
import numpy as np
from jax import lax
from jax.experimental import pallas as pl
from jax.experimental.pallas import tpu as pltpu
from jax.sharding import PartitionSpec as P

HEAD_DIM = 128
WINDOW = 128
GRID_W = 64
EPSILON = 1e-06
NEGATIVE = -1e30
MESH = pl.DeviceIdType.MESH
F32 = jnp.float32
BF16 = jnp.bfloat16
LOG2E = math.log2(math.e)
CHUNK = 16
OUT_PIECES = 2


def kernel(
    n_sp,
    lat_hbm,
    ctx_hbm,
    cond_ref,
    cctx_ref,
    gain_ref,
    wsh_hbm,
    wsc_hbm,
    wga_hbm,
    wq_hbm,
    wk_hbm,
    wv_hbm,
    wo_hbm,
    sink_ref,
    row_cos,
    row_sin,
    col_cos,
    col_sin,
    mixed,
    lat_raw,
    lat_all,
    ctx_v,
    wmod,
    wqkv,
    wo_all,
    act_s,
    mod_p,
    mod_all,
    mod_a,
    mod_b,
    mod_g,
    hbuf,
    qbuf,
    kvbuf,
    ckv,
    attn,
    acc,
    cos_ref,
    sin_ref,
    loc_sem,
    modp_s,
    modp_r,
    moda_s,
    moda_r,
    lat_s,
    lat_r,
    relay_s,
    relay_r,
    ctx_s,
    ctx_r,
    halo_s,
    halo_r,
    attn_s,
    attn_r,
    wo_s,
    wo_r,
    wod_s,
    wod_r,
    woz_s,
    woz_r,
    woc_s,
    woc_r,
    woe_s,
    woe_r,
):
    rows, samples, width = lat_hbm.shape
    n_tp = mod_all.shape[0]
    wid = wmod.shape[2]
    qw = wq_hbm.shape[1]
    kw = wk_hbm.shape[1]
    heads = qw // HEAD_DIM
    lc = ctx_hbm.shape[0]
    block = rows * n_tp
    sp = lax.axis_index("sp")
    tp = lax.axis_index("tp")
    dp = lax.axis_index("dp")
    tx, ty = tp % 2, tp // 2
    peer = {1: 2 * ty + 1 - tx, 2: 2 * (1 - ty) + tx, 3: 3 - tp}

    def sp_peer(o):
        return lax.rem(sp + o, n_sp)

    loads = [
        pltpu.make_async_copy(wsh_hbm, wmod.at[0], loc_sem.at[0]),
        pltpu.make_async_copy(wsc_hbm, wmod.at[1], loc_sem.at[1]),
        pltpu.make_async_copy(wga_hbm, wmod.at[2], loc_sem.at[2]),
        pltpu.make_async_copy(ctx_hbm, ctx_v, loc_sem.at[3]),
        pltpu.make_async_copy(wk_hbm, wqkv.at[:, pl.ds(qw, kw)], loc_sem.at[4]),
        pltpu.make_async_copy(wv_hbm, wqkv.at[:, pl.ds(qw + kw, kw)], loc_sem.at[5]),
        pltpu.make_async_copy(lat_hbm, lat_raw, loc_sem.at[6]),
        pltpu.make_async_copy(wq_hbm, wqkv.at[:, pl.ds(0, qw)], loc_sem.at[7]),
        pltpu.make_async_copy(wo_hbm, wo_all.at[0], loc_sem.at[8]),
    ]
    for i in (8, 0, 1, 2, 6, 3, 4, 5, 7):
        loads[i].start()

    barrier = pltpu.get_barrier_semaphore()
    for o in range(1, n_sp):
        pl.semaphore_signal(barrier, inc=1, device_id={"sp": sp_peer(o)}, device_id_type=MESH)
    for k in (1, 2, 3):
        pl.semaphore_signal(barrier, inc=1, device_id={"tp": peer[k]}, device_id_type=MESH)

    pl.semaphore_signal(barrier, inc=1, device_id={"dp": 1 - dp}, device_id_type=MESH)

    def apart(src, at):
        return jnp.swapaxes(src[pl.ds(at, CHUNK)], 0, 1)

    pl.semaphore_wait(barrier, n_sp - 1 + n_tp)

    def remote(src, dst, ssem, rsem, dev):
        return pltpu.make_async_remote_copy(
            src_ref=src, dst_ref=dst, send_sem=ssem, recv_sem=rsem, device_id=dev, device_id_type=MESH
        )

    half = rows // 2

    def direct(k, s, p):
        part = pl.ds(p * half, half)
        return remote(
            lat_all.at[0, s, part], lat_all.at[k, s, part], lat_s.at[k, s, p], lat_r.at[k, s, p], {"tp": peer[k]}
        )

    def relay(s, p):
        part = pl.ds(p * half, half)
        return remote(
            lat_all.at[1 + p, s, part], lat_all.at[3, s, part], relay_s.at[s, p], relay_r.at[s, p], {"tp": peer[2 - p]}
        )

    zh = sp % 2
    quarter = qw // 4
    mine_q = 2 * zh + dp
    pair_q = 2 * (1 - zh) + dp

    def wo_rows(index, count=quarter, skip=0):
        return pl.ds(pl.multiple_of(index * quarter + skip, count), count)

    def wo_half(index, p):
        return wo_rows(index, quarter // 2, p * (quarter // 2))

    def wo_direct(k, p):
        part = wo_half(mine_q, p)
        return remote(wo_all.at[0, part], wo_all.at[k, part], wo_s.at[k, p], wo_r.at[k, p], {"tp": peer[k]})

    def wo_relay(p):
        part = wo_half(mine_q, p)
        return remote(
            wo_all.at[1 + p, part], wo_all.at[3, part], wod_s.at[p], wod_r.at[p], {"tp": peer[2 - p]}
        )

    def wo_pair(k, p, index):
        part = wo_all.at[k, wo_half(index, p)]
        return remote(part, part, woz_s.at[k, p], woz_r.at[k, p], {"sp": sp + 1 - 2 * zh})

    def wo_core(k, p, index):
        part = wo_all.at[k, wo_half(index, p)]
        return remote(part, part, woc_s.at[k, p], woc_r.at[k, p], {"dp": 1 - dp})

    def wo_share(k, p):
        wo_pair(k, p, mine_q).start()
        wo_core(k, p, mine_q).start()

    def wo_last(k, index):
        part = wo_all.at[k, wo_rows(index)]
        return remote(part, part, woe_s.at[k], woe_r.at[k], {"dp": 1 - dp})

    loads[8].wait()
    wo_direct(1, 0).start()
    wo_direct(2, 1).start()

    act_s[...] = jnp.zeros_like(act_s)
    cv = cond_ref[...].astype(F32)
    act_s[0:samples, :] = cv / (1.0 + jnp.exp(-cv))
    cc = cctx_ref[...].astype(F32).reshape(1, -1)
    act_s[samples : samples + 1, :] = cc / (1.0 + jnp.exp(-cc))
    both = act_s[...].astype(BF16)
    for m in range(3):
        loads[m].wait()
        mod_p[0, :, m * wid : (m + 1) * wid] = jnp.dot(both, wmod[m], preferred_element_type=F32)[0:4]
    mod_copies = [
        remote(mod_p.at[0], mod_p.at[o], modp_s.at[o], modp_r.at[o], {"sp": sp_peer(o)})
        for o in range(1, n_sp)
    ]
    for copy in mod_copies:
        copy.start()

    loads[6].wait()

    @pl.loop(0, rows // CHUNK)
    def _(c):
        at = pl.multiple_of(c * CHUNK, CHUNK)
        both = apart(lat_raw, at)
        for s in range(samples):
            lat_all[0, s, pl.ds(at, CHUNK), :] = both[s]

    grid_rows = block // GRID_W
    for by_row, by_col, table in ((row_cos, col_cos, cos_ref), (row_sin, col_sin, sin_ref)):
        left = lax.broadcasted_iota(jnp.int32, (GRID_W, HEAD_DIM), 1) < HEAD_DIM // 2
        for r in range(grid_rows):
            table[r * GRID_W : (r + 1) * GRID_W, :] = jnp.where(
                left, by_row[pl.ds(sp * grid_rows + r, 1), :], by_col[...]
            )

    for copy in mod_copies:
        copy.wait_recv()
    total = mod_p[0]
    for o in range(1, n_sp):
        total = total + mod_p[o]
    mod_all[tp] = total
    all_copies = [
        remote(mod_all.at[tp], mod_all.at[tp], moda_s.at[k], moda_r.at[k], {"tp": peer[k]})
        for k in (1, 2, 3)
    ]
    for copy in all_copies:
        copy.start()
    wo_direct(1, 1).start()
    wo_direct(2, 0).start()
    direct(1, 0, 0).start()
    direct(2, 0, 1).start()
    direct(1, 0, 1).start()
    direct(2, 0, 0).start()
    wo_direct(1, 0).wait_recv()
    wo_direct(2, 1).wait_recv()
    wo_share(1, 0)
    wo_share(2, 1)
    for k in (1, 2, 3):
        remote(
            mod_all.at[peer[k]], mod_all.at[peer[k]], moda_s.at[k], moda_r.at[k], {"tp": peer[k]}
        ).wait_recv()
    for t in range(n_tp):
        cols = slice(t * wid, (t + 1) * wid)
        mod_b[:, cols] = mod_all[t, :, 0:wid]
        mod_a[:, cols] = (1.0 + mod_all[t, :, wid : 2 * wid]) * gain_ref[:, cols]
        mod_g[:, cols] = mod_all[t, :, 2 * wid : 3 * wid]

    def modulate(values, mod_row):
        x = values.astype(F32)
        inv = lax.rsqrt(jnp.mean(x * x, axis=-1, keepdims=True) + EPSILON)
        row = pl.ds(mod_row, 1)
        return (x * inv * mod_a[row, :] + mod_b[row, :]).astype(BF16)

    def norm_rows(src, mod_row, base, count):
        @pl.loop(0, count // CHUNK, unroll=4)
        def _(c):
            at = pl.multiple_of(c * CHUNK, CHUNK)
            hbuf[pl.ds(base + at, CHUNK), :] = modulate(src[pl.ds(at, CHUNK), :], mod_row)

    for i in (3, 4, 5):
        loads[i].wait()
    ctx_at = pl.multiple_of(sp * lc, lc)

    @pl.loop(0, lc // CHUNK, unroll=2)
    def _(c):
        at = pl.multiple_of(c * CHUNK, CHUNK)
        both = apart(ctx_v, at)
        for s in range(samples):
            hbuf[pl.ds(s * lc + at, CHUNK), :] = modulate(both[s], samples)

    made = jnp.dot(hbuf[...], wqkv[:, qw : qw + 2 * kw], preferred_element_type=F32).astype(BF16)
    for s in range(samples):
        ckv[s, pl.ds(ctx_at, lc), :] = made[s * lc : (s + 1) * lc]

    mine = ckv.at[:, pl.ds(ctx_at, lc), :]
    ctx_copies = [
        remote(mine, mine, ctx_s.at[o], ctx_r.at[o], {"sp": sp_peer(o)}) for o in range(1, n_sp)
    ]
    for copy in ctx_copies:
        copy.start()

    wo_direct(1, 1).wait_recv()
    wo_direct(2, 0).wait_recv()
    direct(1, 0, 0).wait_recv()
    direct(2, 0, 1).wait_recv()
    for p in range(2):
        relay(0, p).start()
    for p in range(2):
        wo_relay(p).start()
    direct(1, 1, 0).start()
    direct(2, 1, 1).start()
    direct(1, 1, 1).start()
    direct(2, 1, 0).start()

    loads[7].wait()
    lane = lax.broadcasted_iota(jnp.int32, (rows, HEAD_DIM), 1)
    low = lane % (HEAD_DIM // 2) < HEAD_DIM // 4

    def turn(u, cos, sin):
        other = jnp.where(
            low, pltpu.roll(u, HEAD_DIM - HEAD_DIM // 4, 1), pltpu.roll(u, HEAD_DIM // 4, 1)
        )
        return u * cos + other * sin

    def halo_up(s):
        return remote(
            kvbuf.at[s, pl.ds(block, WINDOW), :],
            kvbuf.at[s, pl.ds(0, WINDOW), :],
            halo_s.at[0, s],
            halo_r.at[0, s],
            {"sp": lax.min(sp + 1, n_sp - 1)},
        )

    def halo_down(s):
        return remote(
            kvbuf.at[s, pl.ds(WINDOW, WINDOW), :],
            kvbuf.at[s, pl.ds(WINDOW + block, WINDOW), :],
            halo_s.at[1, s],
            halo_r.at[1, s],
            {"sp": lax.max(sp - 1, 0)},
        )

    not_first, not_last = sp > 0, sp < n_sp - 1

    @pl.when(sp == 0)
    def _():
        kvbuf[:, 0:WINDOW, :] = jnp.zeros((samples, WINDOW, 2 * kw), BF16)

    @pl.when(sp == n_sp - 1)
    def _():
        kvbuf[:, WINDOW + block :, :] = jnp.zeros((samples, WINDOW, 2 * kw), BF16)

    acc[...] = jnp.zeros_like(acc)

    def attn_copy(k, s, dest):
        return remote(attn.at[n_tp + k, s], attn.at[k, s], attn_s.at[k, s], attn_r.at[k, s], {"tp": dest})

    def project(blocks):
        spots = []
        for e, (k, s) in enumerate(blocks):
            norm_rows(lat_all.at[k, s], s, e * rows, rows)
            kx, ky = k % 2, k // 2
            b = 2 * (ty + ky - 2 * ty * ky) + tx + kx - 2 * tx * kx
            at = pl.multiple_of(b * rows, rows)
            spots.append((s, b, at, cos_ref[pl.ds(at, rows), :], sin_ref[pl.ds(at, rows), :]))
        for c in range(heads // 2 + 1):
            prod = jnp.dot(
                hbuf[0 : len(blocks) * rows, :],
                wqkv[:, c * 2 * HEAD_DIM : (c + 1) * 2 * HEAD_DIM],
                preferred_element_type=F32,
            )
            for e, (s, b, at, cos, sin) in enumerate(spots):
                part = prod[e * rows : (e + 1) * rows]
                first = turn(part[:, :HEAD_DIM], cos, sin).astype(BF16)
                if c < heads // 2:
                    second = turn(part[:, HEAD_DIM:], cos, sin).astype(BF16)
                    qbuf[s, b, 2 * c * rows : (2 * c + 1) * rows, :] = first
                    qbuf[s, b, (2 * c + 1) * rows : (2 * c + 2) * rows, :] = second
                else:
                    kvbuf[s, pl.ds(WINDOW + at, rows), 0:HEAD_DIM] = first
                    kvbuf[s, pl.ds(WINDOW + at, rows), HEAD_DIM:] = part[:, HEAD_DIM:].astype(BF16)

    def send_edges(s, bottom, top):
        @pl.when(not_last & top)
        def _():
            halo_up(s).start()

        @pl.when(not_first & bottom)
        def _():
            halo_down(s).start()

    at_first, at_last = tp == 0, tp == n_tp - 1
    inner = (tp > 0) & (tp < n_tp - 1)
    project([(0, s) for s in range(samples)])
    for s in range(samples):
        send_edges(s, at_first, at_last)

    scale = HEAD_DIM ** (-0.5) * LOG2E
    seq = block * n_sp
    nums = (((1,), (1,)), ((), ()))

    span = 3 * WINDOW
    pair = 2 * rows
    row_id = lax.broadcasted_iota(jnp.int32, (pair, 1), 0)

    def hand_over(k):
        for p in range(2):
            wo_pair(k, p, pair_q).wait_recv()
        wo_last(k, pair_q).start()

    def attend(i, s):
        k = jnp.where(i == 0, 1, jnp.where(i < n_tp - 1, n_tp - i, 0))
        kx, ky = k % 2, k // 2
        b = 2 * (ty + ky - 2 * ty * ky) + tx + kx - 2 * tx * kx
        at = pl.multiple_of(b * rows, rows)
        slot = jnp.where(k == 0, 0, n_tp + k)

        @pl.when((b == 0) & not_first)
        def _():
            halo_up(s).wait_recv()

        @pl.when((b == n_tp - 1) & not_last)
        def _():
            halo_down(s).wait_recv()

        kc = ckv[s, :, 0:HEAD_DIM]
        vc = ckv[s, :, HEAD_DIM:]
        kl = kvbuf[s, pl.ds(at, span), 0:HEAD_DIM]
        vl = kvbuf[s, pl.ds(at, span), HEAD_DIM:]
        key = lax.broadcasted_iota(jnp.int32, (pair, span), 1)
        query = lax.broadcasted_iota(jnp.int32, (pair, span), 0) % rows
        pos = key + (sp * block + b * rows - WINDOW)
        allowed = (key >= query) & (key <= query + 2 * WINDOW) & (pos >= 0) & (pos < seq)
        for c in range(heads // 2):
            q = qbuf[s, b, c * pair : (c + 1) * pair, :]
            sc = lax.dot_general(q, kc, nums, preferred_element_type=F32)
            sl = lax.dot_general(q, kl, nums, preferred_element_type=F32)
            sl = jnp.where(allowed, sl, NEGATIVE)
            sink2 = jnp.where(row_id < rows, sink_ref[0, 2 * c], sink_ref[0, 2 * c + 1]) * LOG2E
            top = jnp.maximum(
                jnp.max(sc, axis=-1, keepdims=True), jnp.max(sl, axis=-1, keepdims=True)
            )
            top = jnp.maximum(top * scale, sink2)
            ec = jnp.exp2(sc * scale - top)
            el = jnp.exp2(sl * scale - top)
            total = (
                jnp.sum(ec, axis=-1, keepdims=True)
                + jnp.sum(el, axis=-1, keepdims=True)
                + jnp.exp2(sink2 - top)
            )
            o = jnp.dot(ec.astype(BF16), vc, preferred_element_type=F32)
            o = o + jnp.dot(el.astype(BF16), vl, preferred_element_type=F32)
            o = (o / total).astype(BF16)
            attn[slot, s, :, 2 * c * HEAD_DIM : (2 * c + 1) * HEAD_DIM] = o[:rows]
            attn[slot, s, :, (2 * c + 1) * HEAD_DIM : (2 * c + 2) * HEAD_DIM] = o[rows:]

        @pl.when((s == 1) & (k > 0))
        def _():
            attn_copy(k, s, b).start()

    @pl.loop(0, samples)
    def _(s):
        direct(1, s, 1).wait_recv()
        direct(2, s, 0).wait_recv()
        project([(1, s), (2, s)])
        send_edges(s, inner, inner)

        @pl.loop(0, n_tp)
        def _(i):
            @pl.when(i == s)
            def _():
                relay(s, 0).wait_recv()
                relay(s, 1).wait_recv()
                project([(3, s)])
                send_edges(s, at_last, at_first)

                @pl.when(s == 0)
                def _():
                    wo_share(1, 1)
                    wo_share(2, 0)
                    for o in range(1, n_sp):
                        got = ckv.at[:, pl.ds(pl.multiple_of(sp_peer(n_sp - o) * lc, lc), lc), :]
                        remote(got, got, ctx_s.at[o], ctx_r.at[o], {"sp": sp_peer(o)}).wait_recv()
                    wo_relay(0).wait_recv()
                    wo_share(3, 0)

                @pl.when(s == 1)
                def _():
                    wo_relay(1).wait_recv()
                    wo_share(3, 1)
                    hand_over(1)
                    hand_over(2)

            attend(i, s)

        @pl.when(s == 0)
        def _():
            direct(1, 1, 0).wait_recv()
            direct(2, 1, 1).wait_recv()
            for p in range(2):
                relay(1, p).start()
            for k in (3, 2, 1):
                attn_copy(k, 0, peer[k]).start()

    def project_out(k):
        if k > 0:
            for p in range(2):
                wo_core(k, p, mine_q + 1 - 2 * dp).wait_recv()
            wo_last(k, pair_q + 1 - 2 * dp).wait_recv()
            for s in range(samples):
                attn_copy(k, s, peer[k]).wait_recv()

        @pl.loop(0, OUT_PIECES)
        def _(n):
            cols = out_cols(n)
            part = jnp.dot(
                attn[k].reshape(samples * rows, qw), wo_all[k, :, cols], preferred_element_type=F32
            )
            total = acc[:, cols] + part.astype(BF16).astype(F32)
            if k < n_tp - 1:
                acc[:, cols] = total
            else:
                both = []
                for s in range(samples):
                    branch = total[s * rows : (s + 1) * rows]
                    both.append(
                        (lat_all[0, s, :, cols].astype(F32) + mod_g[s : s + 1, cols] * branch).astype(BF16)
                    )
                mixed[:, :, cols] = jnp.swapaxes(jnp.stack(both), 0, 1)

    def out_cols(n):
        span = width // OUT_PIECES
        return pl.ds(pl.multiple_of(n * span, span), span)

    hand_over(3)
    for k in range(n_tp):
        project_out(k)

    for copy in mod_copies + all_copies + ctx_copies:
        copy.wait_send()
    for s in range(samples):
        for p in range(2):
            direct(1, s, p).wait_send()
            direct(2, s, p).wait_send()
            relay(s, p).wait_send()
        for k in (1, 2, 3):
            attn_copy(k, s, peer[k]).wait_send()

        @pl.when(not_last)
        def _(s=s):
            halo_up(s).wait_send()

        @pl.when(not_first)
        def _(s=s):
            halo_down(s).wait_send()

    for p in range(2):
        wo_direct(1, p).wait_send()
        wo_direct(2, p).wait_send()
        wo_relay(p).wait_send()
        for k in (1, 2, 3):
            wo_pair(k, p, mine_q).wait_send()
            wo_core(k, p, mine_q).wait_send()
    for k in (1, 2, 3):
        wo_last(k, pair_q).wait_send()


def local(
    n_sp,
    n_tp,
    latent,
    context,
    condition,
    ctx_condition,
    norm_gain,
    w_shift,
    w_scale,
    w_gate,
    w_query,
    w_key,
    w_value,
    w_out,
    sink,
):
    rows, samples, width = latent.shape
    lc = context.shape[0]
    wid = w_shift.shape[1]
    depth = w_shift.shape[0]
    qw, kw = w_query.shape[1], w_key.shape[1]
    heads = qw // HEAD_DIM
    block = rows * n_tp
    assert n_tp == 4 and n_sp % 2 == 0 and qw % 64 == 0 and samples == 2 and kw == HEAD_DIM and rows == WINDOW and block % GRID_W == 0 and heads % 2 == 0
    quarter = HEAD_DIM // 4
    lane = np.arange(HEAD_DIM)
    freqs = 10000.0 ** (-(lane % quarter).astype(np.float32) / quarter)
    sign = np.where(lane % (2 * quarter) < quarter, -1.0, 1.0)

    def table(count):
        angle = np.arange(count, dtype=np.float32)[:, None] * freqs[None, :].astype(np.float32)
        return jnp.asarray(np.cos(angle), F32), jnp.asarray(np.sin(angle) * sign[None, :], F32)

    row_table = table(n_sp * block // GRID_W)
    col_table = table(GRID_W)
    hbm = pl.BlockSpec(memory_space=pltpu.HBM)
    vmem = pl.BlockSpec(memory_space=pltpu.VMEM)
    smem = pl.BlockSpec(memory_space=pltpu.SMEM)
    dma = pltpu.SemaphoreType.DMA
    mixed = pl.pallas_call(
        functools.partial(kernel, n_sp),
        out_shape=pltpu.VMEM((rows, samples, width), BF16),
        in_specs=[hbm, hbm, vmem, vmem, vmem, hbm, hbm, hbm, hbm, hbm, hbm, hbm, smem, vmem, vmem, vmem, vmem],
        out_specs=vmem,
        scratch_shapes=[
            pltpu.VMEM((rows, samples, width), BF16),
            pltpu.VMEM((n_tp, samples, rows, width), BF16),
            pltpu.VMEM((lc, samples, width), BF16),
            pltpu.VMEM((3, depth, wid), BF16),
            pltpu.VMEM((width, qw + 2 * kw), BF16),
            pltpu.VMEM((n_tp, qw, width), BF16),
            pltpu.VMEM((8, depth), F32),
            pltpu.VMEM((n_sp, 4, 3 * wid), F32),
            pltpu.VMEM((n_tp, 4, 3 * wid), F32),
            pltpu.VMEM((4, width), F32),
            pltpu.VMEM((4, width), F32),
            pltpu.VMEM((4, width), F32),
            pltpu.VMEM((samples * max(rows, lc), width), BF16),
            pltpu.VMEM((samples, n_tp, heads * rows, HEAD_DIM), BF16),
            pltpu.VMEM((samples, block + 2 * WINDOW, 2 * kw), BF16),
            pltpu.VMEM((samples, lc * n_sp, 2 * kw), BF16),
            pltpu.VMEM((2 * n_tp, samples, rows, qw), BF16),
            pltpu.VMEM((samples * rows, width), F32),
            pltpu.VMEM((block, HEAD_DIM), F32),
            pltpu.VMEM((block, HEAD_DIM), F32),
            dma((9,)),
            dma((n_sp,)),
            dma((n_sp,)),
            dma((n_tp,)),
            dma((n_tp,)),
            dma((n_tp, samples, 2)),
            dma((n_tp, samples, 2)),
            dma((samples, 2)),
            dma((samples, 2)),
            dma((n_sp,)),
            dma((n_sp,)),
            dma((2, samples)),
            dma((2, samples)),
            dma((n_tp, samples)),
            dma((n_tp, samples)),
            dma((n_tp, 2)),
            dma((n_tp, 2)),
            dma((2,)),
            dma((2,)),
            dma((n_tp, 2)),
            dma((n_tp, 2)),
            dma((n_tp, 2)),
            dma((n_tp, 2)),
            dma((n_tp,)),
            dma((n_tp,)),
        ],
        compiler_params=pltpu.CompilerParams(
            collective_id=0, has_side_effects=True, vmem_limit_bytes=60 * 1024 * 1024
        ),
        name="step",
    )(
        latent,
        context,
        condition,
        ctx_condition,
        norm_gain[None],
        w_shift,
        w_scale,
        w_gate,
        w_query,
        w_key,
        w_value,
        w_out,
        sink[None],
        *row_table,
        *col_table,
    )
    return mixed


def solution(mesh):
    return jax.shard_map(
        functools.partial(local, mesh.shape["sp"], mesh.shape["tp"]),
        mesh=mesh,
        in_specs=(
            P(("sp", "tp"), "dp", None),
            P("sp", "dp", None),
            P("dp", "sp"),
            P("sp"),
            P(),
            P("sp", "tp"),
            P("sp", "tp"),
            P("sp", "tp"),
            P(None, "tp"),
            P(None, "tp"),
            P(None, "tp"),
            P("tp", None),
            P("tp"),
        ),
        out_specs=P(("sp", "tp"), "dp", None),
        check_vma=False,
    )
```

```python
import functools
import math

import jax
import jax.numpy as jnp
import numpy as np
from jax import lax
from jax.experimental import pallas as pl
from jax.experimental.pallas import tpu as pltpu
from jax.sharding import PartitionSpec as P

HEAD_DIM = 128
WINDOW = 128
GRID_W = 64
EPSILON = 1e-06
NEGATIVE = -1e30
MESH = pl.DeviceIdType.MESH
F32 = jnp.float32
BF16 = jnp.bfloat16
LOG2E = math.log2(math.e)
CHUNK = 16
OUT_PIECES = 2


def kernel(
    n_sp,
    lat_hbm,
    ctx_hbm,
    cond_ref,
    cctx_ref,
    gain_ref,
    wsh_hbm,
    wsc_hbm,
    wga_hbm,
    wq_hbm,
    wk_hbm,
    wv_hbm,
    wo_hbm,
    sink_ref,
    row_cos,
    row_sin,
    col_cos,
    col_sin,
    mixed,
    lat_raw,
    lat_all,
    ctx_v,
    wmod,
    wqkv,
    wo_all,
    act_s,
    mod_p,
    mod_all,
    mod_a,
    mod_b,
    mod_g,
    hbuf,
    qbuf,
    kvbuf,
    ckv,
    attn,
    acc,
    cos_ref,
    sin_ref,
    loc_sem,
    modp_s,
    modp_r,
    moda_s,
    moda_r,
    lat_s,
    lat_r,
    relay_s,
    relay_r,
    ctx_s,
    ctx_r,
    halo_s,
    halo_r,
    attn_s,
    attn_r,
    wo_s,
    wo_r,
    wod_s,
    wod_r,
    woz_s,
    woz_r,
    woc_s,
    woc_r,
    woe_s,
    woe_r,
):
    rows, samples, width = lat_hbm.shape
    n_tp = mod_all.shape[0]
    wid = wmod.shape[2]
    qw = wq_hbm.shape[1]
    kw = wk_hbm.shape[1]
    heads = qw // HEAD_DIM
    lc = ctx_hbm.shape[0]
    block = rows * n_tp
    sp = lax.axis_index("sp")
    tp = lax.axis_index("tp")
    dp = lax.axis_index("dp")
    tx, ty = tp % 2, tp // 2
    peer = {1: 2 * ty + 1 - tx, 2: 2 * (1 - ty) + tx, 3: 3 - tp}

    def sp_peer(o):
        return lax.rem(sp + o, n_sp)

    loads = [
        pltpu.make_async_copy(wsh_hbm, wmod.at[0], loc_sem.at[0]),
        pltpu.make_async_copy(wsc_hbm, wmod.at[1], loc_sem.at[1]),
        pltpu.make_async_copy(wga_hbm, wmod.at[2], loc_sem.at[2]),
        pltpu.make_async_copy(ctx_hbm, ctx_v, loc_sem.at[3]),
        pltpu.make_async_copy(wk_hbm, wqkv.at[:, pl.ds(qw, kw)], loc_sem.at[4]),
        pltpu.make_async_copy(wv_hbm, wqkv.at[:, pl.ds(qw + kw, kw)], loc_sem.at[5]),
        pltpu.make_async_copy(lat_hbm, lat_raw, loc_sem.at[6]),
        pltpu.make_async_copy(wq_hbm, wqkv.at[:, pl.ds(0, qw)], loc_sem.at[7]),
        pltpu.make_async_copy(wo_hbm, wo_all.at[0], loc_sem.at[8]),
    ]
    for i in (8, 0, 1, 2, 6, 3, 4, 5, 7):
        loads[i].start()

    barrier = pltpu.get_barrier_semaphore()
    for o in range(1, n_sp):
        pl.semaphore_signal(barrier, inc=1, device_id={"sp": sp_peer(o)}, device_id_type=MESH)
    for k in (1, 2, 3):
        pl.semaphore_signal(barrier, inc=1, device_id={"tp": peer[k]}, device_id_type=MESH)

    pl.semaphore_signal(barrier, inc=1, device_id={"dp": 1 - dp}, device_id_type=MESH)

    def apart(src, at):
        return jnp.swapaxes(src[pl.ds(at, CHUNK)], 0, 1)

    pl.semaphore_wait(barrier, n_sp - 1 + n_tp)

    def remote(src, dst, ssem, rsem, dev):
        return pltpu.make_async_remote_copy(
            src_ref=src, dst_ref=dst, send_sem=ssem, recv_sem=rsem, device_id=dev, device_id_type=MESH
        )

    half = rows // 2

    def direct(k, s, p):
        part = pl.ds(p * half, half)
        return remote(
            lat_all.at[0, s, part], lat_all.at[k, s, part], lat_s.at[k - 1, s, p], lat_r.at[k - 1, s, p], {"tp": peer[k]}
        )

    def relay(s, p):
        part = pl.ds(p * half, half)
        return remote(
            lat_all.at[1 + p, s, part], lat_all.at[3, s, part], relay_s.at[s, p], relay_r.at[s, p], {"tp": peer[2 - p]}
        )

    zh = sp % 2
    quarter = qw // 4
    mine_q = 2 * zh + dp
    pair_q = 2 * (1 - zh) + dp

    def wo_rows(index, count=quarter, skip=0):
        return pl.ds(pl.multiple_of(index * quarter + skip, count), count)

    def wo_half(index, p):
        return wo_rows(index, quarter // 2, p * (quarter // 2))

    def wo_direct(k, p):
        part = wo_half(mine_q, p)
        return remote(wo_all.at[0, part], wo_all.at[k, part], wo_s.at[k - 1, p], wo_r.at[k - 1, p], {"tp": peer[k]})

    def wo_relay(p):
        part = wo_half(mine_q, p)
        return remote(
            wo_all.at[1 + p, part], wo_all.at[3, part], wod_s.at[p], wod_r.at[p], {"tp": peer[2 - p]}
        )

    def wo_pair(k, p, index):
        part = wo_all.at[k, wo_rows(index) if p is None else wo_half(index, p)]
        return remote(part, part, woz_s.at[k - 1], woz_r.at[k - 1], {"sp": sp + 1 - 2 * zh})

    def wo_core(k, p, index):
        part = wo_all.at[k, wo_rows(index) if p is None else wo_half(index, p)]
        return remote(part, part, woc_s.at[k - 1], woc_r.at[k - 1], {"dp": 1 - dp})

    def wo_share(k, p):
        wo_pair(k, p, mine_q).start()
        wo_core(k, p, mine_q).start()

    def wo_last(k, index):
        part = wo_all.at[k, wo_rows(index)]
        return remote(part, part, woe_s.at[k - 1], woe_r.at[k - 1], {"dp": 1 - dp})

    loads[8].wait()
    wo_direct(1, 0).start()
    wo_direct(2, 1).start()

    act_s[...] = jnp.zeros_like(act_s)
    cv = cond_ref[...].astype(F32)
    act_s[0:samples, :] = cv / (1.0 + jnp.exp(-cv))
    cc = cctx_ref[...].astype(F32).reshape(1, -1)
    act_s[samples : samples + 1, :] = cc / (1.0 + jnp.exp(-cc))
    both = act_s[...].astype(BF16)
    for m in range(3):
        loads[m].wait()
        mod_p[0, :, m * wid : (m + 1) * wid] = jnp.dot(both, wmod[m], preferred_element_type=F32)[0:4]
    mod_copies = [
        remote(mod_p.at[0], mod_p.at[o], modp_s.at[o - 1], modp_r.at[o - 1], {"sp": sp_peer(o)})
        for o in range(1, n_sp)
    ]
    for copy in mod_copies:
        copy.start()

    loads[6].wait()

    @pl.loop(0, rows // CHUNK)
    def _(c):
        at = pl.multiple_of(c * CHUNK, CHUNK)
        both = apart(lat_raw, at)
        for s in range(samples):
            lat_all[0, s, pl.ds(at, CHUNK), :] = both[s]

    grid_rows = block // GRID_W
    for by_row, by_col, table in ((row_cos, col_cos, cos_ref), (row_sin, col_sin, sin_ref)):
        left = lax.broadcasted_iota(jnp.int32, (GRID_W, HEAD_DIM), 1) < HEAD_DIM // 2
        for r in range(grid_rows):
            table[r * GRID_W : (r + 1) * GRID_W, :] = jnp.where(
                left, by_row[pl.ds(sp * grid_rows + r, 1), :], by_col[...]
            )

    for copy in mod_copies:
        copy.wait_recv()
    total = mod_p[0]
    for o in range(1, n_sp):
        total = total + mod_p[o]
    mod_all[tp] = total
    all_copies = [
        remote(mod_all.at[tp], mod_all.at[tp], moda_s.at[k - 1], moda_r.at[k - 1], {"tp": peer[k]})
        for k in (1, 2, 3)
    ]
    for copy in all_copies:
        copy.start()
    wo_direct(1, 1).start()
    wo_direct(2, 0).start()
    direct(1, 0, 0).start()
    direct(2, 0, 1).start()
    direct(1, 0, 1).start()
    direct(2, 0, 0).start()
    wo_direct(1, 0).wait_recv()
    wo_direct(2, 1).wait_recv()
    wo_share(1, 0)
    wo_share(2, 1)
    for k in (1, 2, 3):
        remote(
            mod_all.at[peer[k]], mod_all.at[peer[k]], moda_s.at[k - 1], moda_r.at[k - 1], {"tp": peer[k]}
        ).wait_recv()
    for t in range(n_tp):
        cols = slice(t * wid, (t + 1) * wid)
        mod_b[:, cols] = mod_all[t, :, 0:wid]
        mod_a[:, cols] = (1.0 + mod_all[t, :, wid : 2 * wid]) * gain_ref[:, cols]
        mod_g[:, cols] = mod_all[t, :, 2 * wid : 3 * wid]

    def modulate(values, mod_row):
        x = values.astype(F32)
        inv = lax.rsqrt(jnp.mean(x * x, axis=-1, keepdims=True) + EPSILON)
        row = pl.ds(mod_row, 1)
        return (x * inv * mod_a[row, :] + mod_b[row, :]).astype(BF16)

    def norm_rows(src, mod_row, base, count):
        @pl.loop(0, count // CHUNK, unroll=4)
        def _(c):
            at = pl.multiple_of(c * CHUNK, CHUNK)
            hbuf[pl.ds(base + at, CHUNK), :] = modulate(src[pl.ds(at, CHUNK), :], mod_row)

    for i in (3, 4, 5):
        loads[i].wait()
    ctx_at = pl.multiple_of(sp * lc, lc)

    @pl.loop(0, lc // CHUNK, unroll=2)
    def _(c):
        at = pl.multiple_of(c * CHUNK, CHUNK)
        both = apart(ctx_v, at)
        for s in range(samples):
            hbuf[pl.ds(s * lc + at, CHUNK), :] = modulate(both[s], samples)

    made = jnp.dot(hbuf[...], wqkv[:, qw : qw + 2 * kw], preferred_element_type=F32).astype(BF16)
    for s in range(samples):
        ckv[s, pl.ds(ctx_at, lc), :] = made[s * lc : (s + 1) * lc]

    mine = ckv.at[:, pl.ds(ctx_at, lc), :]
    ctx_copies = [
        remote(mine, mine, ctx_s.at[o - 1], ctx_r.at[o - 1], {"sp": sp_peer(o)}) for o in range(1, n_sp)
    ]
    for copy in ctx_copies:
        copy.start()

    wo_direct(1, 1).wait_recv()
    wo_direct(2, 0).wait_recv()
    direct(1, 0, 0).wait_recv()
    direct(2, 0, 1).wait_recv()
    for p in range(2):
        relay(0, p).start()
    for p in range(2):
        wo_relay(p).start()
    direct(1, 1, 0).start()
    direct(2, 1, 1).start()
    direct(1, 1, 1).start()
    direct(2, 1, 0).start()

    loads[7].wait()
    lane = lax.broadcasted_iota(jnp.int32, (rows, HEAD_DIM), 1)
    low = lane % (HEAD_DIM // 2) < HEAD_DIM // 4

    def turn(u, cos, sin):
        other = jnp.where(
            low, pltpu.roll(u, HEAD_DIM - HEAD_DIM // 4, 1), pltpu.roll(u, HEAD_DIM // 4, 1)
        )
        return u * cos + other * sin

    def halo_up(s):
        return remote(
            kvbuf.at[s, pl.ds(block, WINDOW), :],
            kvbuf.at[s, pl.ds(0, WINDOW), :],
            halo_s.at[0, s],
            halo_r.at[0, s],
            {"sp": lax.min(sp + 1, n_sp - 1)},
        )

    def halo_down(s):
        return remote(
            kvbuf.at[s, pl.ds(WINDOW, WINDOW), :],
            kvbuf.at[s, pl.ds(WINDOW + block, WINDOW), :],
            halo_s.at[1, s],
            halo_r.at[1, s],
            {"sp": lax.max(sp - 1, 0)},
        )

    not_first, not_last = sp > 0, sp < n_sp - 1

    @pl.when(sp == 0)
    def _():
        kvbuf[:, 0:WINDOW, :] = jnp.zeros((samples, WINDOW, 2 * kw), BF16)

    @pl.when(sp == n_sp - 1)
    def _():
        kvbuf[:, WINDOW + block :, :] = jnp.zeros((samples, WINDOW, 2 * kw), BF16)

    def attn_copy(k, s, dest):
        return remote(attn.at[n_tp + k, s], attn.at[k, s], attn_s.at[k - 1, s], attn_r.at[k - 1, s], {"tp": dest})

    def project(blocks):
        spots = []
        for e, (k, s) in enumerate(blocks):
            norm_rows(lat_all.at[k, s], s, e * rows, rows)
            kx, ky = k % 2, k // 2
            b = 2 * (ty + ky - 2 * ty * ky) + tx + kx - 2 * tx * kx
            at = pl.multiple_of(b * rows, rows)
            spots.append((s, b, at, cos_ref[pl.ds(at, rows), :], sin_ref[pl.ds(at, rows), :]))
        for c in range(heads // 2 + 1):
            prod = jnp.dot(
                hbuf[0 : len(blocks) * rows, :],
                wqkv[:, c * 2 * HEAD_DIM : (c + 1) * 2 * HEAD_DIM],
                preferred_element_type=F32,
            )
            for e, (s, b, at, cos, sin) in enumerate(spots):
                part = prod[e * rows : (e + 1) * rows]
                first = turn(part[:, :HEAD_DIM], cos, sin).astype(BF16)
                if c < heads // 2:
                    second = turn(part[:, HEAD_DIM:], cos, sin).astype(BF16)
                    qbuf[s, b, 2 * c * rows : (2 * c + 1) * rows, :] = first
                    qbuf[s, b, (2 * c + 1) * rows : (2 * c + 2) * rows, :] = second
                else:
                    kvbuf[s, pl.ds(WINDOW + at, rows), 0:HEAD_DIM] = first
                    kvbuf[s, pl.ds(WINDOW + at, rows), HEAD_DIM:] = part[:, HEAD_DIM:].astype(BF16)

    def send_edges(s, bottom, top):
        @pl.when(not_last & top)
        def _():
            halo_up(s).start()

        @pl.when(not_first & bottom)
        def _():
            halo_down(s).start()

    at_first, at_last = tp == 0, tp == n_tp - 1
    inner = (tp > 0) & (tp < n_tp - 1)
    project([(0, s) for s in range(samples)])
    for s in range(samples):
        send_edges(s, at_first, at_last)

    scale = HEAD_DIM ** (-0.5) * LOG2E
    seq = block * n_sp
    nums = (((1,), (1,)), ((), ()))

    span = 3 * WINDOW
    pair = 2 * rows
    row_id = lax.broadcasted_iota(jnp.int32, (pair, 1), 0)

    def hand_over(k):
        wo_pair(k, None, pair_q).wait_recv()
        wo_last(k, pair_q).start()

    def out_cols(n):
        span = width // OUT_PIECES
        return pl.ds(pl.multiple_of(n * span, span), span)

    def project_own(s):
        held = pl.ds(s * rows, rows)

        @pl.loop(0, OUT_PIECES)
        def _(n):
            cols = out_cols(n)
            part = jnp.dot(attn[0, s], wo_all[0, :, cols], preferred_element_type=F32)
            acc[held, cols] = part.astype(BF16).astype(F32)

    def edges_sent(s):
        @pl.when(not_last)
        def _():
            halo_up(s).wait_send()

        @pl.when(not_first)
        def _():
            halo_down(s).wait_send()

    def early_sent():
        for copy in mod_copies + all_copies + ctx_copies:
            copy.wait_send()
        for p in range(2):
            for k in (1, 2):
                for s in range(samples):
                    direct(k, s, p).wait_send()
                wo_direct(k, p).wait_send()
            relay(0, p).wait_send()
            wo_relay(p).wait_send()
        for k in (1, 2):
            wo_pair(k, None, mine_q).wait_send()
            wo_core(k, None, mine_q).wait_send()
        edges_sent(0)

    def attend(i, s):
        k = jnp.where(i == 0, 1, jnp.where(i < n_tp - 1, n_tp - i, 0))
        kx, ky = k % 2, k // 2
        b = 2 * (ty + ky - 2 * ty * ky) + tx + kx - 2 * tx * kx
        at = pl.multiple_of(b * rows, rows)
        slot = jnp.where(k == 0, 0, n_tp + k)

        @pl.when((b == 0) & not_first)
        def _():
            halo_up(s).wait_recv()

        @pl.when((b == n_tp - 1) & not_last)
        def _():
            halo_down(s).wait_recv()

        kc = ckv[s, :, 0:HEAD_DIM]
        vc = ckv[s, :, HEAD_DIM:]
        kl = kvbuf[s, pl.ds(at, span), 0:HEAD_DIM]
        vl = kvbuf[s, pl.ds(at, span), HEAD_DIM:]
        key = lax.broadcasted_iota(jnp.int32, (pair, span), 1)
        query = lax.broadcasted_iota(jnp.int32, (pair, span), 0) % rows
        pos = key + (sp * block + b * rows - WINDOW)
        allowed = (key >= query) & (key <= query + 2 * WINDOW) & (pos >= 0) & (pos < seq)
        for c in range(heads // 2):
            q = qbuf[s, b, c * pair : (c + 1) * pair, :]
            sc = lax.dot_general(q, kc, nums, preferred_element_type=F32)
            sl = lax.dot_general(q, kl, nums, preferred_element_type=F32)
            sl = jnp.where(allowed, sl, NEGATIVE)
            sink2 = jnp.where(row_id < rows, sink_ref[0, 2 * c], sink_ref[0, 2 * c + 1]) * LOG2E
            top = jnp.maximum(
                jnp.max(sc, axis=-1, keepdims=True), jnp.max(sl, axis=-1, keepdims=True)
            )
            top = jnp.maximum(top * scale, sink2)
            ec = jnp.exp2(sc * scale - top)
            el = jnp.exp2(sl * scale - top)
            total = (
                jnp.sum(ec, axis=-1, keepdims=True)
                + jnp.sum(el, axis=-1, keepdims=True)
                + jnp.exp2(sink2 - top)
            )
            o = jnp.dot(ec.astype(BF16), vc, preferred_element_type=F32)
            o = o + jnp.dot(el.astype(BF16), vl, preferred_element_type=F32)
            o = (o / total).astype(BF16)
            attn[slot, s, :, 2 * c * HEAD_DIM : (2 * c + 1) * HEAD_DIM] = o[:rows]
            attn[slot, s, :, (2 * c + 1) * HEAD_DIM : (2 * c + 2) * HEAD_DIM] = o[rows:]

        @pl.when((s == 1) & (k > 0))
        def _():
            attn_copy(k, s, b).start()

    @pl.loop(0, samples)
    def _(s):
        direct(1, s, 1).wait_recv()
        direct(2, s, 0).wait_recv()
        project([(1, s), (2, s)])
        send_edges(s, inner, inner)

        @pl.loop(0, n_tp)
        def _(i):
            @pl.when(i == s)
            def _():
                @pl.when(s == 1)
                def _():
                    project_own(0)
                    early_sent()

                relay(s, 0).wait_recv()
                relay(s, 1).wait_recv()
                project([(3, s)])
                send_edges(s, at_last, at_first)

                @pl.when(s == 0)
                def _():
                    wo_share(1, 1)
                    wo_share(2, 0)
                    for o in range(1, n_sp):
                        got = ckv.at[:, pl.ds(pl.multiple_of(sp_peer(n_sp - o) * lc, lc), lc), :]
                        remote(got, got, ctx_s.at[o - 1], ctx_r.at[o - 1], {"sp": sp_peer(o)}).wait_recv()
                    wo_relay(0).wait_recv()
                    wo_share(3, 0)

                @pl.when(s == 1)
                def _():
                    wo_relay(1).wait_recv()
                    wo_share(3, 1)
                    hand_over(1)
                    hand_over(2)

            attend(i, s)

        @pl.when(s == 0)
        def _():
            direct(1, 1, 0).wait_recv()
            direct(2, 1, 1).wait_recv()
            for p in range(2):
                relay(1, p).start()
            for k in (3, 2, 1):
                attn_copy(k, 0, peer[k]).start()

    def arrived(k, s):
        if k > 0:
            if s == 0:
                wo_core(k, None, mine_q + 1 - 2 * dp).wait_recv()
                wo_last(k, pair_q + 1 - 2 * dp).wait_recv()
            attn_copy(k, s, peer[k]).wait_recv()

    def project_out(k, s, last):
        arrived(k, s)

        @pl.loop(0, OUT_PIECES)
        def _(n):
            cols = out_cols(n)
            part = jnp.dot(attn[k, s], wo_all[k, :, cols], preferred_element_type=F32)
            held = pl.ds(s * rows, rows)
            total = acc[held, cols] + part.astype(BF16).astype(F32)
            if not last:
                acc[held, cols] = total
            else:
                both = []
                for t in range(samples):
                    branch = total if t == s else acc[t * rows : (t + 1) * rows, cols]
                    both.append(
                        (lat_all[0, t, :, cols].astype(F32) + mod_g[t : t + 1, cols] * branch).astype(BF16)
                    )
                mixed[:, :, cols] = jnp.swapaxes(jnp.stack(both), 0, 1)

    hand_over(3)
    project_own(1)
    project_out(1, 0, False)
    project_out(2, 0, False)
    project_out(3, 0, False)
    project_out(3, 1, False)
    project_out(1, 1, False)
    project_out(2, 1, True)

    for s in range(samples):
        for k in (1, 2, 3):
            attn_copy(k, s, peer[k]).wait_send()
    for p in range(2):
        relay(1, p).wait_send()
    for k in (1, 2, 3):
        wo_last(k, pair_q).wait_send()
    wo_pair(3, None, mine_q).wait_send()
    wo_core(3, None, mine_q).wait_send()
    edges_sent(1)


def local(
    n_sp,
    n_tp,
    latent,
    context,
    condition,
    ctx_condition,
    norm_gain,
    w_shift,
    w_scale,
    w_gate,
    w_query,
    w_key,
    w_value,
    w_out,
    sink,
):
    rows, samples, width = latent.shape
    lc = context.shape[0]
    wid = w_shift.shape[1]
    depth = w_shift.shape[0]
    qw, kw = w_query.shape[1], w_key.shape[1]
    heads = qw // HEAD_DIM
    block = rows * n_tp
    assert n_tp == 4 and n_sp % 2 == 0 and qw % 64 == 0 and samples == 2 and kw == HEAD_DIM and rows == WINDOW and block % GRID_W == 0 and heads % 2 == 0
    quarter = HEAD_DIM // 4
    lane = np.arange(HEAD_DIM)
    freqs = 10000.0 ** (-(lane % quarter).astype(np.float32) / quarter)
    sign = np.where(lane % (2 * quarter) < quarter, -1.0, 1.0)

    def table(count):
        angle = np.arange(count, dtype=np.float32)[:, None] * freqs[None, :].astype(np.float32)
        return jnp.asarray(np.cos(angle), F32), jnp.asarray(np.sin(angle) * sign[None, :], F32)

    row_table = table(n_sp * block // GRID_W)
    col_table = table(GRID_W)
    hbm = pl.BlockSpec(memory_space=pltpu.HBM)
    vmem = pl.BlockSpec(memory_space=pltpu.VMEM)
    smem = pl.BlockSpec(memory_space=pltpu.SMEM)
    dma = pltpu.SemaphoreType.DMA
    mixed = pl.pallas_call(
        functools.partial(kernel, n_sp),
        out_shape=pltpu.VMEM((rows, samples, width), BF16),
        in_specs=[hbm, hbm, vmem, vmem, vmem, hbm, hbm, hbm, hbm, hbm, hbm, hbm, smem, vmem, vmem, vmem, vmem],
        out_specs=vmem,
        scratch_shapes=[
            pltpu.VMEM((rows, samples, width), BF16),
            pltpu.VMEM((n_tp, samples, rows, width), BF16),
            pltpu.VMEM((lc, samples, width), BF16),
            pltpu.VMEM((3, depth, wid), BF16),
            pltpu.VMEM((width, qw + 2 * kw), BF16),
            pltpu.VMEM((n_tp, qw, width), BF16),
            pltpu.VMEM((8, depth), F32),
            pltpu.VMEM((n_sp, 4, 3 * wid), F32),
            pltpu.VMEM((n_tp, 4, 3 * wid), F32),
            pltpu.VMEM((4, width), F32),
            pltpu.VMEM((4, width), F32),
            pltpu.VMEM((4, width), F32),
            pltpu.VMEM((samples * max(rows, lc), width), BF16),
            pltpu.VMEM((samples, n_tp, heads * rows, HEAD_DIM), BF16),
            pltpu.VMEM((samples, block + 2 * WINDOW, 2 * kw), BF16),
            pltpu.VMEM((samples, lc * n_sp, 2 * kw), BF16),
            pltpu.VMEM((2 * n_tp, samples, rows, qw), BF16),
            pltpu.VMEM((samples * rows, width), F32),
            pltpu.VMEM((block, HEAD_DIM), F32),
            pltpu.VMEM((block, HEAD_DIM), F32),
            dma((9,)),
            dma((n_sp - 1,)),
            dma((n_sp - 1,)),
            dma((n_tp - 1,)),
            dma((n_tp - 1,)),
            dma((2, samples, 2)),
            dma((2, samples, 2)),
            dma((samples, 2)),
            dma((samples, 2)),
            dma((n_sp - 1,)),
            dma((n_sp - 1,)),
            dma((2, samples)),
            dma((2, samples)),
            dma((n_tp - 1, samples)),
            dma((n_tp - 1, samples)),
            dma((2, 2)),
            dma((2, 2)),
            dma((2,)),
            dma((2,)),
            dma((n_tp - 1,)),
            dma((n_tp - 1,)),
            dma((n_tp - 1,)),
            dma((n_tp - 1,)),
            dma((n_tp - 1,)),
            dma((n_tp - 1,)),
        ],
        compiler_params=pltpu.CompilerParams(
            collective_id=0, has_side_effects=True, vmem_limit_bytes=60 * 1024 * 1024
        ),
        name="step",
    )(
        latent,
        context,
        condition,
        ctx_condition,
        norm_gain[None],
        w_shift,
        w_scale,
        w_gate,
        w_query,
        w_key,
        w_value,
        w_out,
        sink[None],
        *row_table,
        *col_table,
    )
    return mixed


def solution(mesh):
    return jax.shard_map(
        functools.partial(local, mesh.shape["sp"], mesh.shape["tp"]),
        mesh=mesh,
        in_specs=(
            P(("sp", "tp"), "dp", None),
            P("sp", "dp", None),
            P("dp", "sp"),
            P("sp"),
            P(),
            P("sp", "tp"),
            P("sp", "tp"),
            P("sp", "tp"),
            P(None, "tp"),
            P(None, "tp"),
            P(None, "tp"),
            P("tp", None),
            P("tp"),
        ),
        out_specs=P(("sp", "tp"), "dp", None),
        check_vma=False,
    )
```

```python
import functools
import math

import jax
import jax.numpy as jnp
import numpy as np
from jax import lax
from jax.experimental import pallas as pl
from jax.experimental.pallas import tpu as pltpu
from jax.sharding import PartitionSpec as P

HEAD_DIM = 128
WINDOW = 128
GRID_W = 64
EPSILON = 1e-06
NEGATIVE = -1e30
MESH = pl.DeviceIdType.MESH
F32 = jnp.float32
BF16 = jnp.bfloat16
LOG2E = math.log2(math.e)
CHUNK = 16
OUT_PIECES = 2


def kernel(
    n_sp,
    lat_hbm,
    ctx_hbm,
    cond_ref,
    cctx_ref,
    gain_ref,
    wsh_hbm,
    wsc_hbm,
    wga_hbm,
    wq_hbm,
    wk_hbm,
    wv_hbm,
    wo_hbm,
    sink_ref,
    row_cos,
    row_sin,
    col_cos,
    col_sin,
    mixed,
    lat_raw,
    lat_all,
    ctx_v,
    wmod,
    wqkv,
    wo_all,
    act_s,
    mod_p,
    mod_all,
    mod_a,
    mod_b,
    mod_g,
    hbuf,
    qbuf,
    kvbuf,
    ckv,
    attn,
    acc,
    cos_ref,
    sin_ref,
    loc_sem,
    modp_s,
    modp_r,
    moda_s,
    moda_r,
    lat_s,
    lat_r,
    relay_s,
    relay_r,
    ctx_s,
    ctx_r,
    halo_s,
    halo_r,
    attn_s,
    attn_r,
    wo_s,
    wo_r,
    wod_s,
    wod_r,
    woz_s,
    woz_r,
    woc_s,
    woc_r,
    woe_s,
    woe_r,
):
    rows, samples, width = lat_hbm.shape
    n_tp = mod_all.shape[0]
    wid = wmod.shape[2]
    qw = wq_hbm.shape[1]
    kw = wk_hbm.shape[1]
    heads = qw // HEAD_DIM
    lc = ctx_hbm.shape[0]
    block = rows * n_tp
    sp = lax.axis_index("sp")
    tp = lax.axis_index("tp")
    dp = lax.axis_index("dp")
    tx, ty = tp % 2, tp // 2
    peer = {1: 2 * ty + 1 - tx, 2: 2 * (1 - ty) + tx, 3: 3 - tp}

    def sp_peer(o):
        return lax.rem(sp + o, n_sp)

    loads = [
        pltpu.make_async_copy(wsh_hbm, wmod.at[0], loc_sem.at[0]),
        pltpu.make_async_copy(wsc_hbm, wmod.at[1], loc_sem.at[1]),
        pltpu.make_async_copy(wga_hbm, wmod.at[2], loc_sem.at[2]),
        pltpu.make_async_copy(ctx_hbm, ctx_v, loc_sem.at[3]),
        pltpu.make_async_copy(wk_hbm, wqkv.at[:, pl.ds(qw, kw)], loc_sem.at[4]),
        pltpu.make_async_copy(wv_hbm, wqkv.at[:, pl.ds(qw + kw, kw)], loc_sem.at[5]),
        pltpu.make_async_copy(lat_hbm, lat_raw, loc_sem.at[6]),
        pltpu.make_async_copy(wq_hbm, wqkv.at[:, pl.ds(0, qw)], loc_sem.at[7]),
        pltpu.make_async_copy(wo_hbm, wo_all.at[0], loc_sem.at[8]),
    ]
    for i in (8, 0, 1, 2, 6, 3, 4, 5, 7):
        loads[i].start()

    barrier = pltpu.get_barrier_semaphore()
    for o in range(1, n_sp):
        pl.semaphore_signal(barrier, inc=1, device_id={"sp": sp_peer(o)}, device_id_type=MESH)
    for k in (1, 2, 3):
        pl.semaphore_signal(barrier, inc=1, device_id={"tp": peer[k]}, device_id_type=MESH)

    pl.semaphore_signal(barrier, inc=1, device_id={"dp": 1 - dp}, device_id_type=MESH)

    def apart(src, at):
        return jnp.swapaxes(src[pl.ds(at, CHUNK)], 0, 1)

    pl.semaphore_wait(barrier, n_sp - 1 + n_tp)

    def remote(src, dst, ssem, rsem, dev):
        return pltpu.make_async_remote_copy(
            src_ref=src, dst_ref=dst, send_sem=ssem, recv_sem=rsem, device_id=dev, device_id_type=MESH
        )

    half = rows // 2

    def direct(k, s, p):
        part = pl.ds(p * half, half)
        return remote(
            lat_all.at[0, s, part], lat_all.at[k, s, part], lat_s.at[k - 1, s, p], lat_r.at[k - 1, s, p], {"tp": peer[k]}
        )

    def relay(s, p):
        part = pl.ds(p * half, half)
        return remote(
            lat_all.at[1 + p, s, part], lat_all.at[3, s, part], relay_s.at[s, p], relay_r.at[s, p], {"tp": peer[2 - p]}
        )

    zh = sp % 2
    quarter = qw // 4
    mine_q = 2 * zh + dp
    pair_q = 2 * (1 - zh) + dp

    def wo_rows(index, count=quarter, skip=0):
        return pl.ds(pl.multiple_of(index * quarter + skip, count), count)

    def wo_half(index, p):
        return wo_rows(index, quarter // 2, p * (quarter // 2))

    def wo_direct(k, p):
        part = wo_half(mine_q, p)
        return remote(wo_all.at[0, part], wo_all.at[k, part], wo_s.at[k - 1, p], wo_r.at[k - 1, p], {"tp": peer[k]})

    def wo_relay(p):
        part = wo_half(mine_q, p)
        return remote(
            wo_all.at[1 + p, part], wo_all.at[3, part], wod_s.at[p], wod_r.at[p], {"tp": peer[2 - p]}
        )

    def wo_pair(k, p, index):
        part = wo_all.at[k, wo_rows(index) if p is None else wo_half(index, p)]
        return remote(part, part, woz_s.at[k - 1], woz_r.at[k - 1], {"sp": sp + 1 - 2 * zh})

    def wo_core(k, p, index):
        part = wo_all.at[k, wo_rows(index) if p is None else wo_half(index, p)]
        return remote(part, part, woc_s.at[k - 1], woc_r.at[k - 1], {"dp": 1 - dp})

    def wo_share(k, p):
        wo_pair(k, p, mine_q).start()
        wo_core(k, p, mine_q).start()

    def wo_last(k, index):
        part = wo_all.at[k, wo_rows(index)]
        return remote(part, part, woe_s.at[k - 1], woe_r.at[k - 1], {"dp": 1 - dp})

    loads[8].wait()
    wo_direct(1, 0).start()
    wo_direct(2, 1).start()

    act_s[...] = jnp.zeros_like(act_s)
    cv = cond_ref[...].astype(F32)
    act_s[0:samples, :] = cv / (1.0 + jnp.exp(-cv))
    cc = cctx_ref[...].astype(F32).reshape(1, -1)
    act_s[samples : samples + 1, :] = cc / (1.0 + jnp.exp(-cc))
    both = act_s[...].astype(BF16)
    for m in range(3):
        loads[m].wait()
        mod_p[0, :, m * wid : (m + 1) * wid] = jnp.dot(both, wmod[m], preferred_element_type=F32)[0:4]
    mod_copies = [
        remote(mod_p.at[0], mod_p.at[o], modp_s.at[o - 1], modp_r.at[o - 1], {"sp": sp_peer(o)})
        for o in range(1, n_sp)
    ]
    for copy in mod_copies:
        copy.start()

    loads[6].wait()

    @pl.loop(0, rows // CHUNK)
    def _(c):
        at = pl.multiple_of(c * CHUNK, CHUNK)
        both = apart(lat_raw, at)
        for s in range(samples):
            lat_all[0, s, pl.ds(at, CHUNK), :] = both[s]

    grid_rows = block // GRID_W
    for by_row, by_col, table in ((row_cos, col_cos, cos_ref), (row_sin, col_sin, sin_ref)):
        left = lax.broadcasted_iota(jnp.int32, (GRID_W, HEAD_DIM), 1) < HEAD_DIM // 2
        for r in range(grid_rows):
            table[r * GRID_W : (r + 1) * GRID_W, :] = jnp.where(
                left, by_row[pl.ds(sp * grid_rows + r, 1), :], by_col[...]
            )

    for copy in mod_copies:
        copy.wait_recv()
    total = mod_p[0]
    for o in range(1, n_sp):
        total = total + mod_p[o]
    mod_all[tp] = total
    all_copies = [
        remote(mod_all.at[tp], mod_all.at[tp], moda_s.at[k - 1], moda_r.at[k - 1], {"tp": peer[k]})
        for k in (1, 2, 3)
    ]
    for copy in all_copies:
        copy.start()
    wo_direct(1, 1).start()
    wo_direct(2, 0).start()
    direct(1, 0, 0).start()
    direct(2, 0, 1).start()
    direct(1, 0, 1).start()
    direct(2, 0, 0).start()
    wo_direct(1, 0).wait_recv()
    wo_direct(2, 1).wait_recv()
    wo_share(1, 0)
    wo_share(2, 1)
    for k in (1, 2, 3):
        remote(
            mod_all.at[peer[k]], mod_all.at[peer[k]], moda_s.at[k - 1], moda_r.at[k - 1], {"tp": peer[k]}
        ).wait_recv()
    for t in range(n_tp):
        cols = slice(t * wid, (t + 1) * wid)
        mod_b[:, cols] = mod_all[t, :, 0:wid]
        mod_a[:, cols] = (1.0 + mod_all[t, :, wid : 2 * wid]) * gain_ref[:, cols]
        mod_g[:, cols] = mod_all[t, :, 2 * wid : 3 * wid]

    def modulate(values, mod_row):
        x = values.astype(F32)
        inv = lax.rsqrt(jnp.mean(x * x, axis=-1, keepdims=True) + EPSILON)
        row = pl.ds(mod_row, 1)
        return (x * inv * mod_a[row, :] + mod_b[row, :]).astype(BF16)

    def norm_rows(src, mod_row, base, count):
        @pl.loop(0, count // CHUNK, unroll=4)
        def _(c):
            at = pl.multiple_of(c * CHUNK, CHUNK)
            hbuf[pl.ds(base + at, CHUNK), :] = modulate(src[pl.ds(at, CHUNK), :], mod_row)

    for i in (3, 4, 5):
        loads[i].wait()
    ctx_at = pl.multiple_of(sp * lc, lc)

    @pl.loop(0, lc // CHUNK, unroll=2)
    def _(c):
        at = pl.multiple_of(c * CHUNK, CHUNK)
        both = apart(ctx_v, at)
        for s in range(samples):
            hbuf[pl.ds(s * lc + at, CHUNK), :] = modulate(both[s], samples)

    made = jnp.dot(hbuf[...], wqkv[:, qw : qw + 2 * kw], preferred_element_type=F32).astype(BF16)
    for s in range(samples):
        ckv[s, pl.ds(ctx_at, lc), :] = made[s * lc : (s + 1) * lc]

    mine = ckv.at[:, pl.ds(ctx_at, lc), :]
    ctx_copies = [
        remote(mine, mine, ctx_s.at[o - 1], ctx_r.at[o - 1], {"sp": sp_peer(o)}) for o in range(1, n_sp)
    ]
    for copy in ctx_copies:
        copy.start()

    wo_direct(1, 1).wait_recv()
    wo_direct(2, 0).wait_recv()
    direct(1, 0, 0).wait_recv()
    direct(2, 0, 1).wait_recv()
    for p in range(2):
        relay(0, p).start()
    for p in range(2):
        wo_relay(p).start()
    direct(1, 1, 0).start()
    direct(2, 1, 1).start()
    direct(1, 1, 1).start()
    direct(2, 1, 0).start()

    loads[7].wait()
    lane = lax.broadcasted_iota(jnp.int32, (rows, HEAD_DIM), 1)
    low = lane % (HEAD_DIM // 2) < HEAD_DIM // 4

    def turn(u, cos, sin):
        other = jnp.where(
            low, pltpu.roll(u, HEAD_DIM - HEAD_DIM // 4, 1), pltpu.roll(u, HEAD_DIM // 4, 1)
        )
        return u * cos + other * sin

    def halo_up(s):
        return remote(
            kvbuf.at[s, pl.ds(block, WINDOW), :],
            kvbuf.at[s, pl.ds(0, WINDOW), :],
            halo_s.at[0, s],
            halo_r.at[0, s],
            {"sp": lax.min(sp + 1, n_sp - 1)},
        )

    def halo_down(s):
        return remote(
            kvbuf.at[s, pl.ds(WINDOW, WINDOW), :],
            kvbuf.at[s, pl.ds(WINDOW + block, WINDOW), :],
            halo_s.at[1, s],
            halo_r.at[1, s],
            {"sp": lax.max(sp - 1, 0)},
        )

    not_first, not_last = sp > 0, sp < n_sp - 1

    @pl.when(sp == 0)
    def _():
        kvbuf[:, 0:WINDOW, :] = jnp.zeros((samples, WINDOW, 2 * kw), BF16)

    @pl.when(sp == n_sp - 1)
    def _():
        kvbuf[:, WINDOW + block :, :] = jnp.zeros((samples, WINDOW, 2 * kw), BF16)

    def attn_copy(k, s, dest):
        return remote(attn.at[n_tp + k, s], attn.at[k, s], attn_s.at[k - 1, s], attn_r.at[k - 1, s], {"tp": dest})

    def project(blocks):
        spots = []
        for e, (k, s) in enumerate(blocks):
            norm_rows(lat_all.at[k, s], s, e * rows, rows)
            kx, ky = k % 2, k // 2
            b = 2 * (ty + ky - 2 * ty * ky) + tx + kx - 2 * tx * kx
            at = pl.multiple_of(b * rows, rows)
            spots.append((s, b, at, cos_ref[pl.ds(at, rows), :], sin_ref[pl.ds(at, rows), :]))
        for c in range(heads // 2 + 1):
            prod = jnp.dot(
                hbuf[0 : len(blocks) * rows, :],
                wqkv[:, c * 2 * HEAD_DIM : (c + 1) * 2 * HEAD_DIM],
                preferred_element_type=F32,
            )
            for e, (s, b, at, cos, sin) in enumerate(spots):
                part = prod[e * rows : (e + 1) * rows]
                first = turn(part[:, :HEAD_DIM], cos, sin).astype(BF16)
                if c < heads // 2:
                    second = turn(part[:, HEAD_DIM:], cos, sin).astype(BF16)
                    qbuf[s, b, 2 * c * rows : (2 * c + 1) * rows, :] = first
                    qbuf[s, b, (2 * c + 1) * rows : (2 * c + 2) * rows, :] = second
                else:
                    kvbuf[s, pl.ds(WINDOW + at, rows), 0:HEAD_DIM] = first
                    kvbuf[s, pl.ds(WINDOW + at, rows), HEAD_DIM:] = part[:, HEAD_DIM:].astype(BF16)

    def send_edges(s, bottom, top):
        @pl.when(not_last & top)
        def _():
            halo_up(s).start()

        @pl.when(not_first & bottom)
        def _():
            halo_down(s).start()

    at_first, at_last = tp == 0, tp == n_tp - 1
    inner = (tp > 0) & (tp < n_tp - 1)
    project([(0, s) for s in range(samples)])
    for s in range(samples):
        send_edges(s, at_first, at_last)

    scale = HEAD_DIM ** (-0.5) * LOG2E
    seq = block * n_sp
    nums = (((1,), (1,)), ((), ()))

    span = 3 * WINDOW
    pair = 2 * rows
    row_id = lax.broadcasted_iota(jnp.int32, (pair, 1), 0)

    def hand_over(k):
        wo_pair(k, None, pair_q).wait_recv()
        wo_last(k, pair_q).start()

    def out_cols(n):
        span = width // OUT_PIECES
        return pl.ds(pl.multiple_of(n * span, span), span)

    def project_own(s):
        held = pl.ds(s * rows, rows)

        @pl.loop(0, OUT_PIECES)
        def _(n):
            cols = out_cols(n)
            part = jnp.dot(attn[0, s], wo_all[0, :, cols], preferred_element_type=F32)
            acc[held, cols] = part.astype(BF16).astype(F32)

    def edges_sent(s):
        @pl.when(not_last)
        def _():
            halo_up(s).wait_send()

        @pl.when(not_first)
        def _():
            halo_down(s).wait_send()

    def early_sent():
        for copy in mod_copies + all_copies + ctx_copies:
            copy.wait_send()
        for p in range(2):
            for k in (1, 2):
                for s in range(samples):
                    direct(k, s, p).wait_send()
                wo_direct(k, p).wait_send()
            relay(0, p).wait_send()
            wo_relay(p).wait_send()
        for k in (1, 2):
            wo_pair(k, None, mine_q).wait_send()
            wo_core(k, None, mine_q).wait_send()
        edges_sent(0)

    def attend(i, s):
        k = jnp.where(i == 0, 1, jnp.where(i < n_tp - 1, n_tp - i, 0))
        kx, ky = k % 2, k // 2
        b = 2 * (ty + ky - 2 * ty * ky) + tx + kx - 2 * tx * kx
        at = pl.multiple_of(b * rows, rows)
        slot = jnp.where(k == 0, 0, n_tp + k)

        @pl.when((b == 0) & not_first)
        def _():
            halo_up(s).wait_recv()

        @pl.when((b == n_tp - 1) & not_last)
        def _():
            halo_down(s).wait_recv()

        kc = ckv[s, :, 0:HEAD_DIM]
        vc = ckv[s, :, HEAD_DIM:]
        kl = kvbuf[s, pl.ds(at, span), 0:HEAD_DIM]
        vl = kvbuf[s, pl.ds(at, span), HEAD_DIM:]
        key = lax.broadcasted_iota(jnp.int32, (pair, span), 1)
        query = lax.broadcasted_iota(jnp.int32, (pair, span), 0) % rows
        pos = key + (sp * block + b * rows - WINDOW)
        allowed = (key >= query) & (key <= query + 2 * WINDOW) & (pos >= 0) & (pos < seq)
        for c in range(heads // 2):
            q = qbuf[s, b, c * pair : (c + 1) * pair, :]
            sc = lax.dot_general(q, kc, nums, preferred_element_type=F32)
            sl = lax.dot_general(q, kl, nums, preferred_element_type=F32)
            sl = jnp.where(allowed, sl, NEGATIVE)
            sink2 = jnp.where(row_id < rows, sink_ref[0, 2 * c], sink_ref[0, 2 * c + 1]) * LOG2E
            top = jnp.maximum(
                jnp.max(sc, axis=-1, keepdims=True), jnp.max(sl, axis=-1, keepdims=True)
            )
            top = jnp.maximum(top * scale, sink2)
            ec = jnp.exp2(sc * scale - top)
            el = jnp.exp2(sl * scale - top)
            total = (
                jnp.sum(ec, axis=-1, keepdims=True)
                + jnp.sum(el, axis=-1, keepdims=True)
                + jnp.exp2(sink2 - top)
            )
            o = jnp.dot(ec.astype(BF16), vc, preferred_element_type=F32)
            o = o + jnp.dot(el.astype(BF16), vl, preferred_element_type=F32)
            o = (o / total).astype(BF16)
            attn[slot, s, :, 2 * c * HEAD_DIM : (2 * c + 1) * HEAD_DIM] = o[:rows]
            attn[slot, s, :, (2 * c + 1) * HEAD_DIM : (2 * c + 2) * HEAD_DIM] = o[rows:]

        @pl.when((s == 1) & (k > 0))
        def _():
            attn_copy(k, s, b).start()

    @pl.loop(0, samples)
    def _(s):
        direct(1, s, 1).wait_recv()
        direct(2, s, 0).wait_recv()
        project([(1, s), (2, s)])
        send_edges(s, inner, inner)

        @pl.when((s == 1) & inner & (dp == 0))
        def _():
            wo_relay(1).wait_recv()
            wo_share(3, 1)

        @pl.loop(0, n_tp)
        def _(i):
            @pl.when(i == s)
            def _():
                @pl.when(s == 1)
                def _():
                    project_own(0)
                    early_sent()

                relay(s, 0).wait_recv()
                relay(s, 1).wait_recv()
                project([(3, s)])
                send_edges(s, at_last, at_first)

                @pl.when(s == 0)
                def _():
                    wo_share(1, 1)
                    wo_share(2, 0)
                    for o in range(1, n_sp):
                        got = ckv.at[:, pl.ds(pl.multiple_of(sp_peer(n_sp - o) * lc, lc), lc), :]
                        remote(got, got, ctx_s.at[o - 1], ctx_r.at[o - 1], {"sp": sp_peer(o)}).wait_recv()
                    wo_relay(0).wait_recv()
                    wo_share(3, 0)

                @pl.when(s == 1)
                def _():
                    @pl.when(at_first | at_last | (dp == 1))
                    def _():
                        wo_relay(1).wait_recv()
                        wo_share(3, 1)

                    hand_over(1)
                    hand_over(2)

            attend(i, s)

        @pl.when(s == 0)
        def _():
            direct(1, 1, 0).wait_recv()
            direct(2, 1, 1).wait_recv()
            for p in range(2):
                relay(1, p).start()
            for k in (3, 2, 1):
                attn_copy(k, 0, peer[k]).start()

    def arrived(k, s):
        if k > 0:
            if s == 0:
                wo_core(k, None, mine_q + 1 - 2 * dp).wait_recv()
                wo_last(k, pair_q + 1 - 2 * dp).wait_recv()
            attn_copy(k, s, peer[k]).wait_recv()

    def project_out(k, s, last):
        arrived(k, s)

        @pl.loop(0, OUT_PIECES)
        def _(n):
            cols = out_cols(n)
            part = jnp.dot(attn[k, s], wo_all[k, :, cols], preferred_element_type=F32)
            held = pl.ds(s * rows, rows)
            total = acc[held, cols] + part.astype(BF16).astype(F32)
            if not last:
                acc[held, cols] = total
            else:
                both = []
                for t in range(samples):
                    branch = total if t == s else acc[t * rows : (t + 1) * rows, cols]
                    both.append(
                        (lat_all[0, t, :, cols].astype(F32) + mod_g[t : t + 1, cols] * branch).astype(BF16)
                    )
                mixed[:, :, cols] = jnp.swapaxes(jnp.stack(both), 0, 1)

    hand_over(3)
    project_own(1)
    project_out(1, 0, False)
    project_out(2, 0, False)
    for core, order in enumerate((((3, 0), (3, 1), (1, 1), (2, 1)), ((1, 1), (2, 1), (3, 0), (3, 1)))):

        @pl.when(dp == core)
        def _(order=order):
            for k, s in order:
                project_out(k, s, (k, s) == order[-1])

    for s in range(samples):
        for k in (1, 2, 3):
            attn_copy(k, s, peer[k]).wait_send()
    for p in range(2):
        relay(1, p).wait_send()
    for k in (1, 2, 3):
        wo_last(k, pair_q).wait_send()
    wo_pair(3, None, mine_q).wait_send()
    wo_core(3, None, mine_q).wait_send()
    edges_sent(1)


def local(
    n_sp,
    n_tp,
    latent,
    context,
    condition,
    ctx_condition,
    norm_gain,
    w_shift,
    w_scale,
    w_gate,
    w_query,
    w_key,
    w_value,
    w_out,
    sink,
):
    rows, samples, width = latent.shape
    lc = context.shape[0]
    wid = w_shift.shape[1]
    depth = w_shift.shape[0]
    qw, kw = w_query.shape[1], w_key.shape[1]
    heads = qw // HEAD_DIM
    block = rows * n_tp
    assert n_tp == 4 and n_sp % 2 == 0 and qw % 64 == 0 and samples == 2 and kw == HEAD_DIM and rows == WINDOW and block % GRID_W == 0 and heads % 2 == 0
    quarter = HEAD_DIM // 4
    lane = np.arange(HEAD_DIM)
    freqs = 10000.0 ** (-(lane % quarter).astype(np.float32) / quarter)
    sign = np.where(lane % (2 * quarter) < quarter, -1.0, 1.0)

    def table(count):
        angle = np.arange(count, dtype=np.float32)[:, None] * freqs[None, :].astype(np.float32)
        return jnp.asarray(np.cos(angle), F32), jnp.asarray(np.sin(angle) * sign[None, :], F32)

    row_table = table(n_sp * block // GRID_W)
    col_table = table(GRID_W)
    hbm = pl.BlockSpec(memory_space=pltpu.HBM)
    vmem = pl.BlockSpec(memory_space=pltpu.VMEM)
    smem = pl.BlockSpec(memory_space=pltpu.SMEM)
    dma = pltpu.SemaphoreType.DMA
    mixed = pl.pallas_call(
        functools.partial(kernel, n_sp),
        out_shape=pltpu.VMEM((rows, samples, width), BF16),
        in_specs=[hbm, hbm, vmem, vmem, vmem, hbm, hbm, hbm, hbm, hbm, hbm, hbm, smem, vmem, vmem, vmem, vmem],
        out_specs=vmem,
        scratch_shapes=[
            pltpu.VMEM((rows, samples, width), BF16),
            pltpu.VMEM((n_tp, samples, rows, width), BF16),
            pltpu.VMEM((lc, samples, width), BF16),
            pltpu.VMEM((3, depth, wid), BF16),
            pltpu.VMEM((width, qw + 2 * kw), BF16),
            pltpu.VMEM((n_tp, qw, width), BF16),
            pltpu.VMEM((8, depth), F32),
            pltpu.VMEM((n_sp, 4, 3 * wid), F32),
            pltpu.VMEM((n_tp, 4, 3 * wid), F32),
            pltpu.VMEM((4, width), F32),
            pltpu.VMEM((4, width), F32),
            pltpu.VMEM((4, width), F32),
            pltpu.VMEM((samples * max(rows, lc), width), BF16),
            pltpu.VMEM((samples, n_tp, heads * rows, HEAD_DIM), BF16),
            pltpu.VMEM((samples, block + 2 * WINDOW, 2 * kw), BF16),
            pltpu.VMEM((samples, lc * n_sp, 2 * kw), BF16),
            pltpu.VMEM((2 * n_tp, samples, rows, qw), BF16),
            pltpu.VMEM((samples * rows, width), F32),
            pltpu.VMEM((block, HEAD_DIM), F32),
            pltpu.VMEM((block, HEAD_DIM), F32),
            dma((9,)),
            dma((n_sp - 1,)),
            dma((n_sp - 1,)),
            dma((n_tp - 1,)),
            dma((n_tp - 1,)),
            dma((2, samples, 2)),
            dma((2, samples, 2)),
            dma((samples, 2)),
            dma((samples, 2)),
            dma((n_sp - 1,)),
            dma((n_sp - 1,)),
            dma((2, samples)),
            dma((2, samples)),
            dma((n_tp - 1, samples)),
            dma((n_tp - 1, samples)),
            dma((2, 2)),
            dma((2, 2)),
            dma((2,)),
            dma((2,)),
            dma((n_tp - 1,)),
            dma((n_tp - 1,)),
            dma((n_tp - 1,)),
            dma((n_tp - 1,)),
            dma((n_tp - 1,)),
            dma((n_tp - 1,)),
        ],
        compiler_params=pltpu.CompilerParams(
            collective_id=0, has_side_effects=True, vmem_limit_bytes=60 * 1024 * 1024
        ),
        name="step",
    )(
        latent,
        context,
        condition,
        ctx_condition,
        norm_gain[None],
        w_shift,
        w_scale,
        w_gate,
        w_query,
        w_key,
        w_value,
        w_out,
        sink[None],
        *row_table,
        *col_table,
    )
    return mixed


def solution(mesh):
    return jax.shard_map(
        functools.partial(local, mesh.shape["sp"], mesh.shape["tp"]),
        mesh=mesh,
        in_specs=(
            P(("sp", "tp"), "dp", None),
            P("sp", "dp", None),
            P("dp", "sp"),
            P("sp"),
            P(),
            P("sp", "tp"),
            P("sp", "tp"),
            P("sp", "tp"),
            P(None, "tp"),
            P(None, "tp"),
            P(None, "tp"),
            P("tp", None),
            P("tp"),
        ),
        out_specs=P(("sp", "tp"), "dp", None),
        check_vma=False,
    )
```

```python
import functools
import math

import jax
import jax.numpy as jnp
import numpy as np
from jax import lax
from jax.experimental import pallas as pl
from jax.experimental.pallas import tpu as pltpu
from jax.sharding import PartitionSpec as P

HEAD_DIM = 128
WINDOW = 128
GRID_W = 64
EPSILON = 1e-06
NEGATIVE = -1e30
MESH = pl.DeviceIdType.MESH
F32 = jnp.float32
BF16 = jnp.bfloat16
LOG2E = math.log2(math.e)
CHUNK = 16
OUT_PIECES = 1


def kernel(
    n_sp,
    lat_hbm,
    ctx_hbm,
    cond_ref,
    cctx_ref,
    gain_ref,
    wsh_hbm,
    wsc_hbm,
    wga_hbm,
    wq_hbm,
    wk_hbm,
    wv_hbm,
    wo_hbm,
    sink_ref,
    row_cos,
    row_sin,
    col_cos,
    col_sin,
    mixed,
    lat_raw,
    lat_all,
    ctx_v,
    wmod,
    wqkv,
    wo_all,
    act_s,
    mod_p,
    mod_all,
    mod_a,
    mod_b,
    mod_g,
    hbuf,
    qbuf,
    kvbuf,
    ckv,
    attn,
    acc,
    cos_ref,
    sin_ref,
    loc_sem,
    modp_s,
    modp_r,
    moda_s,
    moda_r,
    lat_s,
    lat_r,
    relay_s,
    relay_r,
    ctx_s,
    ctx_r,
    halo_s,
    halo_r,
    attn_s,
    attn_r,
    wo_s,
    wo_r,
    wod_s,
    wod_r,
    woz_s,
    woz_r,
    woc_s,
    woc_r,
    woe_s,
    woe_r,
):
    rows, samples, width = lat_hbm.shape
    n_tp = mod_all.shape[0]
    wid = wmod.shape[2]
    qw = wq_hbm.shape[1]
    kw = wk_hbm.shape[1]
    heads = qw // HEAD_DIM
    lc = ctx_hbm.shape[0]
    block = rows * n_tp
    sp = lax.axis_index("sp")
    tp = lax.axis_index("tp")
    dp = lax.axis_index("dp")
    tx, ty = tp % 2, tp // 2
    peer = {1: 2 * ty + 1 - tx, 2: 2 * (1 - ty) + tx, 3: 3 - tp}

    def sp_peer(o):
        return lax.rem(sp + o, n_sp)

    loads = [
        pltpu.make_async_copy(wsh_hbm, wmod.at[0], loc_sem.at[0]),
        pltpu.make_async_copy(wsc_hbm, wmod.at[1], loc_sem.at[1]),
        pltpu.make_async_copy(wga_hbm, wmod.at[2], loc_sem.at[2]),
        pltpu.make_async_copy(ctx_hbm, ctx_v, loc_sem.at[3]),
        pltpu.make_async_copy(wk_hbm, wqkv.at[:, pl.ds(qw, kw)], loc_sem.at[4]),
        pltpu.make_async_copy(wv_hbm, wqkv.at[:, pl.ds(qw + kw, kw)], loc_sem.at[5]),
        pltpu.make_async_copy(lat_hbm, lat_raw, loc_sem.at[6]),
        pltpu.make_async_copy(wq_hbm, wqkv.at[:, pl.ds(0, qw)], loc_sem.at[7]),
        pltpu.make_async_copy(wo_hbm, wo_all.at[0], loc_sem.at[8]),
    ]
    for i in (8, 0, 1, 2, 6, 3, 4, 5, 7):
        loads[i].start()

    barrier = pltpu.get_barrier_semaphore()
    for o in range(1, n_sp):
        pl.semaphore_signal(barrier, inc=1, device_id={"sp": sp_peer(o)}, device_id_type=MESH)
    for k in (1, 2, 3):
        pl.semaphore_signal(barrier, inc=1, device_id={"tp": peer[k]}, device_id_type=MESH)

    pl.semaphore_signal(barrier, inc=1, device_id={"dp": 1 - dp}, device_id_type=MESH)

    def apart(src, at):
        return jnp.swapaxes(src[pl.ds(at, CHUNK)], 0, 1)

    pl.semaphore_wait(barrier, n_sp - 1 + n_tp)

    def remote(src, dst, ssem, rsem, dev):
        return pltpu.make_async_remote_copy(
            src_ref=src, dst_ref=dst, send_sem=ssem, recv_sem=rsem, device_id=dev, device_id_type=MESH
        )

    half = rows // 2

    def direct(k, s, p):
        part = pl.ds(p * half, half)
        return remote(
            lat_all.at[0, s, part], lat_all.at[k, s, part], lat_s.at[k - 1, s, p], lat_r.at[k - 1, s, p], {"tp": peer[k]}
        )

    def relay(s, p):
        part = pl.ds(p * half, half)
        return remote(
            lat_all.at[1 + p, s, part], lat_all.at[3, s, part], relay_s.at[s, p], relay_r.at[s, p], {"tp": peer[2 - p]}
        )

    zh = sp % 2
    quarter = qw // 4
    mine_q = 2 * zh + dp
    pair_q = 2 * (1 - zh) + dp

    def wo_rows(index, count=quarter, skip=0):
        return pl.ds(pl.multiple_of(index * quarter + skip, count), count)

    def wo_half(index, p):
        return wo_rows(index, quarter // 2, p * (quarter // 2))

    def wo_direct(k, p):
        part = wo_half(mine_q, p)
        return remote(wo_all.at[0, part], wo_all.at[k, part], wo_s.at[k - 1, p], wo_r.at[k - 1, p], {"tp": peer[k]})

    def wo_relay(p):
        part = wo_half(mine_q, p)
        return remote(
            wo_all.at[1 + p, part], wo_all.at[3, part], wod_s.at[p], wod_r.at[p], {"tp": peer[2 - p]}
        )

    def wo_pair(k, p, index):
        part = wo_all.at[k, wo_rows(index) if p is None else wo_half(index, p)]
        return remote(part, part, woz_s.at[k - 1], woz_r.at[k - 1], {"sp": sp + 1 - 2 * zh})

    def wo_core(k, p, index):
        part = wo_all.at[k, wo_rows(index) if p is None else wo_half(index, p)]
        return remote(part, part, woc_s.at[k - 1], woc_r.at[k - 1], {"dp": 1 - dp})

    def wo_share(k, p):
        wo_pair(k, p, mine_q).start()
        wo_core(k, p, mine_q).start()

    def wo_last(k, index):
        part = wo_all.at[k, wo_rows(index)]
        return remote(part, part, woe_s.at[k - 1], woe_r.at[k - 1], {"dp": 1 - dp})

    loads[8].wait()
    wo_direct(1, 0).start()
    wo_direct(2, 1).start()

    act_s[...] = jnp.zeros_like(act_s)
    cv = cond_ref[...].astype(F32)
    act_s[0:samples, :] = cv / (1.0 + jnp.exp(-cv))
    cc = cctx_ref[...].astype(F32).reshape(1, -1)
    act_s[samples : samples + 1, :] = cc / (1.0 + jnp.exp(-cc))
    both = act_s[...].astype(BF16)
    for m in range(3):
        loads[m].wait()
        mod_p[0, :, m * wid : (m + 1) * wid] = jnp.dot(both, wmod[m], preferred_element_type=F32)[0:4]
    mod_copies = [
        remote(mod_p.at[0], mod_p.at[o], modp_s.at[o - 1], modp_r.at[o - 1], {"sp": sp_peer(o)})
        for o in range(1, n_sp)
    ]
    for copy in mod_copies:
        copy.start()

    loads[6].wait()

    @pl.loop(0, rows // CHUNK)
    def _(c):
        at = pl.multiple_of(c * CHUNK, CHUNK)
        both = apart(lat_raw, at)
        for s in range(samples):
            lat_all[0, s, pl.ds(at, CHUNK), :] = both[s]

    grid_rows = block // GRID_W
    for by_row, by_col, table in ((row_cos, col_cos, cos_ref), (row_sin, col_sin, sin_ref)):
        left = lax.broadcasted_iota(jnp.int32, (GRID_W, HEAD_DIM), 1) < HEAD_DIM // 2
        for r in range(grid_rows):
            table[r * GRID_W : (r + 1) * GRID_W, :] = jnp.where(
                left, by_row[pl.ds(sp * grid_rows + r, 1), :], by_col[...]
            )

    for copy in mod_copies:
        copy.wait_recv()
    total = mod_p[0]
    for o in range(1, n_sp):
        total = total + mod_p[o]
    mod_all[tp] = total
    all_copies = [
        remote(mod_all.at[tp], mod_all.at[tp], moda_s.at[k - 1], moda_r.at[k - 1], {"tp": peer[k]})
        for k in (1, 2, 3)
    ]
    for copy in all_copies:
        copy.start()
    wo_direct(1, 1).start()
    wo_direct(2, 0).start()
    direct(1, 0, 0).start()
    direct(2, 0, 1).start()
    direct(1, 0, 1).start()
    direct(2, 0, 0).start()
    wo_direct(1, 0).wait_recv()
    wo_direct(2, 1).wait_recv()
    wo_share(1, 0)
    wo_share(2, 1)
    for k in (1, 2, 3):
        remote(
            mod_all.at[peer[k]], mod_all.at[peer[k]], moda_s.at[k - 1], moda_r.at[k - 1], {"tp": peer[k]}
        ).wait_recv()
    for t in range(n_tp):
        cols = slice(t * wid, (t + 1) * wid)
        mod_b[:, cols] = mod_all[t, :, 0:wid]
        mod_a[:, cols] = (1.0 + mod_all[t, :, wid : 2 * wid]) * gain_ref[:, cols]
        mod_g[:, cols] = mod_all[t, :, 2 * wid : 3 * wid]

    def modulate(values, mod_row):
        x = values.astype(F32)
        inv = lax.rsqrt(jnp.mean(x * x, axis=-1, keepdims=True) + EPSILON)
        row = pl.ds(mod_row, 1)
        return (x * inv * mod_a[row, :] + mod_b[row, :]).astype(BF16)

    def norm_rows(src, mod_row, base, count):
        @pl.loop(0, count // CHUNK, unroll=4)
        def _(c):
            at = pl.multiple_of(c * CHUNK, CHUNK)
            hbuf[pl.ds(base + at, CHUNK), :] = modulate(src[pl.ds(at, CHUNK), :], mod_row)

    for i in (3, 4, 5):
        loads[i].wait()
    ctx_at = pl.multiple_of(sp * lc, lc)

    @pl.loop(0, lc // CHUNK, unroll=2)
    def _(c):
        at = pl.multiple_of(c * CHUNK, CHUNK)
        both = apart(ctx_v, at)
        for s in range(samples):
            hbuf[pl.ds(s * lc + at, CHUNK), :] = modulate(both[s], samples)

    made = jnp.dot(hbuf[...], wqkv[:, qw : qw + 2 * kw], preferred_element_type=F32).astype(BF16)
    for s in range(samples):
        ckv[s, pl.ds(ctx_at, lc), :] = made[s * lc : (s + 1) * lc]

    mine = ckv.at[:, pl.ds(ctx_at, lc), :]
    ctx_copies = [
        remote(mine, mine, ctx_s.at[o - 1], ctx_r.at[o - 1], {"sp": sp_peer(o)}) for o in range(1, n_sp)
    ]
    for copy in ctx_copies:
        copy.start()

    wo_direct(1, 1).wait_recv()
    wo_direct(2, 0).wait_recv()
    direct(1, 0, 0).wait_recv()
    direct(2, 0, 1).wait_recv()
    for p in range(2):
        relay(0, p).start()
    for p in range(2):
        wo_relay(p).start()
    direct(1, 1, 0).start()
    direct(2, 1, 1).start()
    direct(1, 1, 1).start()
    direct(2, 1, 0).start()

    loads[7].wait()
    lane = lax.broadcasted_iota(jnp.int32, (rows, HEAD_DIM), 1)
    low = lane % (HEAD_DIM // 2) < HEAD_DIM // 4

    def turn(u, cos, sin):
        other = jnp.where(
            low, pltpu.roll(u, HEAD_DIM - HEAD_DIM // 4, 1), pltpu.roll(u, HEAD_DIM // 4, 1)
        )
        return u * cos + other * sin

    def halo_up(s):
        return remote(
            kvbuf.at[s, pl.ds(block, WINDOW), :],
            kvbuf.at[s, pl.ds(0, WINDOW), :],
            halo_s.at[0, s],
            halo_r.at[0, s],
            {"sp": lax.min(sp + 1, n_sp - 1)},
        )

    def halo_down(s):
        return remote(
            kvbuf.at[s, pl.ds(WINDOW, WINDOW), :],
            kvbuf.at[s, pl.ds(WINDOW + block, WINDOW), :],
            halo_s.at[1, s],
            halo_r.at[1, s],
            {"sp": lax.max(sp - 1, 0)},
        )

    not_first, not_last = sp > 0, sp < n_sp - 1

    @pl.when(sp == 0)
    def _():
        kvbuf[:, 0:WINDOW, :] = jnp.zeros((samples, WINDOW, 2 * kw), BF16)

    @pl.when(sp == n_sp - 1)
    def _():
        kvbuf[:, WINDOW + block :, :] = jnp.zeros((samples, WINDOW, 2 * kw), BF16)

    def attn_copy(k, s, dest):
        return remote(attn.at[n_tp + k, s], attn.at[k, s], attn_s.at[k - 1, s], attn_r.at[k - 1, s], {"tp": dest})

    def project(blocks):
        spots = []
        for e, (k, s) in enumerate(blocks):
            norm_rows(lat_all.at[k, s], s, e * rows, rows)
            kx, ky = k % 2, k // 2
            b = 2 * (ty + ky - 2 * ty * ky) + tx + kx - 2 * tx * kx
            at = pl.multiple_of(b * rows, rows)
            spots.append((s, b, at, cos_ref[pl.ds(at, rows), :], sin_ref[pl.ds(at, rows), :]))
        for c in range(heads // 2 + 1):
            prod = jnp.dot(
                hbuf[0 : len(blocks) * rows, :],
                wqkv[:, c * 2 * HEAD_DIM : (c + 1) * 2 * HEAD_DIM],
                preferred_element_type=F32,
            )
            for e, (s, b, at, cos, sin) in enumerate(spots):
                part = prod[e * rows : (e + 1) * rows]
                first = turn(part[:, :HEAD_DIM], cos, sin).astype(BF16)
                if c < heads // 2:
                    second = turn(part[:, HEAD_DIM:], cos, sin).astype(BF16)
                    qbuf[s, b, 2 * c * rows : (2 * c + 1) * rows, :] = first
                    qbuf[s, b, (2 * c + 1) * rows : (2 * c + 2) * rows, :] = second
                else:
                    kvbuf[s, pl.ds(WINDOW + at, rows), 0:HEAD_DIM] = first
                    kvbuf[s, pl.ds(WINDOW + at, rows), HEAD_DIM:] = part[:, HEAD_DIM:].astype(BF16)

    def send_edges(s, bottom, top):
        @pl.when(not_last & top)
        def _():
            halo_up(s).start()

        @pl.when(not_first & bottom)
        def _():
            halo_down(s).start()

    at_first, at_last = tp == 0, tp == n_tp - 1
    inner = (tp > 0) & (tp < n_tp - 1)
    project([(0, s) for s in range(samples)])
    for s in range(samples):
        send_edges(s, at_first, at_last)

    scale = HEAD_DIM ** (-0.5) * LOG2E
    seq = block * n_sp
    nums = (((1,), (1,)), ((), ()))

    span = 3 * WINDOW
    pair = 2 * rows
    row_id = lax.broadcasted_iota(jnp.int32, (pair, 1), 0)

    def hand_over(k):
        wo_pair(k, None, pair_q).wait_recv()
        wo_last(k, pair_q).start()

    def out_cols(n):
        span = width // OUT_PIECES
        return pl.ds(pl.multiple_of(n * span, span), span)

    def project_own(s):
        held = pl.ds(s * rows, rows)

        @pl.loop(0, OUT_PIECES)
        def _(n):
            cols = out_cols(n)
            part = jnp.dot(attn[0, s], wo_all[0, :, cols], preferred_element_type=F32)
            acc[held, cols] = part.astype(BF16).astype(F32)

    def edges_sent(s):
        @pl.when(not_last)
        def _():
            halo_up(s).wait_send()

        @pl.when(not_first)
        def _():
            halo_down(s).wait_send()

    def early_sent():
        for copy in mod_copies + all_copies + ctx_copies:
            copy.wait_send()
        for p in range(2):
            for k in (1, 2):
                for s in range(samples):
                    direct(k, s, p).wait_send()
                wo_direct(k, p).wait_send()
            relay(0, p).wait_send()
            wo_relay(p).wait_send()
        for k in (1, 2):
            wo_pair(k, None, mine_q).wait_send()
            wo_core(k, None, mine_q).wait_send()
        edges_sent(0)

    def attend(i, s):
        k = jnp.where(i == 0, 1, jnp.where(i < n_tp - 1, n_tp - i, 0))
        kx, ky = k % 2, k // 2
        b = 2 * (ty + ky - 2 * ty * ky) + tx + kx - 2 * tx * kx
        at = pl.multiple_of(b * rows, rows)
        slot = jnp.where(k == 0, 0, n_tp + k)

        @pl.when((b == 0) & not_first)
        def _():
            halo_up(s).wait_recv()

        @pl.when((b == n_tp - 1) & not_last)
        def _():
            halo_down(s).wait_recv()

        kc = ckv[s, :, 0:HEAD_DIM]
        vc = ckv[s, :, HEAD_DIM:]
        kl = kvbuf[s, pl.ds(at, span), 0:HEAD_DIM]
        vl = kvbuf[s, pl.ds(at, span), HEAD_DIM:]
        key = lax.broadcasted_iota(jnp.int32, (pair, span), 1)
        query = lax.broadcasted_iota(jnp.int32, (pair, span), 0) % rows
        pos = key + (sp * block + b * rows - WINDOW)
        allowed = (key >= query) & (key <= query + 2 * WINDOW) & (pos >= 0) & (pos < seq)
        for c in range(heads // 2):
            q = qbuf[s, b, c * pair : (c + 1) * pair, :]
            sc = lax.dot_general(q, kc, nums, preferred_element_type=F32)
            sl = lax.dot_general(q, kl, nums, preferred_element_type=F32)
            sl = jnp.where(allowed, sl, NEGATIVE)
            sink2 = jnp.where(row_id < rows, sink_ref[0, 2 * c], sink_ref[0, 2 * c + 1]) * LOG2E
            top = jnp.maximum(
                jnp.max(sc, axis=-1, keepdims=True), jnp.max(sl, axis=-1, keepdims=True)
            )
            top = jnp.maximum(top * scale, sink2)
            ec = jnp.exp2(sc * scale - top)
            el = jnp.exp2(sl * scale - top)
            total = (
                jnp.sum(ec, axis=-1, keepdims=True)
                + jnp.sum(el, axis=-1, keepdims=True)
                + jnp.exp2(sink2 - top)
            )
            o = jnp.dot(ec.astype(BF16), vc, preferred_element_type=F32)
            o = o + jnp.dot(el.astype(BF16), vl, preferred_element_type=F32)
            o = (o / total).astype(BF16)
            attn[slot, s, :, 2 * c * HEAD_DIM : (2 * c + 1) * HEAD_DIM] = o[:rows]
            attn[slot, s, :, (2 * c + 1) * HEAD_DIM : (2 * c + 2) * HEAD_DIM] = o[rows:]

        @pl.when((s == 1) & (k > 0))
        def _():
            attn_copy(k, s, b).start()

    @pl.loop(0, samples)
    def _(s):
        direct(1, s, 1).wait_recv()
        direct(2, s, 0).wait_recv()
        project([(1, s), (2, s)])
        send_edges(s, inner, inner)

        @pl.when((s == 1) & inner & (dp == 0))
        def _():
            wo_relay(1).wait_recv()
            wo_share(3, 1)

        @pl.loop(0, n_tp)
        def _(i):
            @pl.when(i == s)
            def _():
                @pl.when(s == 1)
                def _():
                    project_own(0)
                    early_sent()

                relay(s, 0).wait_recv()
                relay(s, 1).wait_recv()
                project([(3, s)])
                send_edges(s, at_last, at_first)

                @pl.when(s == 0)
                def _():
                    wo_share(1, 1)
                    wo_share(2, 0)
                    for o in range(1, n_sp):
                        got = ckv.at[:, pl.ds(pl.multiple_of(sp_peer(n_sp - o) * lc, lc), lc), :]
                        remote(got, got, ctx_s.at[o - 1], ctx_r.at[o - 1], {"sp": sp_peer(o)}).wait_recv()
                    wo_relay(0).wait_recv()
                    wo_share(3, 0)

                @pl.when(s == 1)
                def _():
                    @pl.when(at_first | at_last | (dp == 1))
                    def _():
                        wo_relay(1).wait_recv()
                        wo_share(3, 1)

                    hand_over(1)
                    hand_over(2)

            @pl.when((s == 1) & (i == n_tp - 1) & (dp == 1))
            def _():
                hand_over(3)

            attend(i, s)

        @pl.when(s == 0)
        def _():
            direct(1, 1, 0).wait_recv()
            direct(2, 1, 1).wait_recv()
            for p in range(2):
                relay(1, p).start()
            for k in (3, 2, 1):
                attn_copy(k, 0, peer[k]).start()

    def arrived(k, s):
        if k > 0:
            if s == 0:
                wo_core(k, None, mine_q + 1 - 2 * dp).wait_recv()
                wo_last(k, pair_q + 1 - 2 * dp).wait_recv()
            attn_copy(k, s, peer[k]).wait_recv()

    def project_out(k, s, last):
        arrived(k, s)

        @pl.loop(0, OUT_PIECES)
        def _(n):
            cols = out_cols(n)
            part = jnp.dot(attn[k, s], wo_all[k, :, cols], preferred_element_type=F32)
            held = pl.ds(s * rows, rows)
            total = acc[held, cols] + part.astype(BF16).astype(F32)
            if not last:
                acc[held, cols] = total
            else:
                both = []
                for t in range(samples):
                    branch = total if t == s else acc[t * rows : (t + 1) * rows, cols]
                    both.append(
                        (lat_all[0, t, :, cols].astype(F32) + mod_g[t : t + 1, cols] * branch).astype(BF16)
                    )
                mixed[:, :, cols] = jnp.swapaxes(jnp.stack(both), 0, 1)

    @pl.when(dp == 0)
    def _():
        hand_over(3)

    project_own(1)
    project_out(1, 0, False)
    project_out(2, 0, False)
    for core, order in enumerate((((3, 0), (3, 1), (1, 1), (2, 1)), ((1, 1), (2, 1), (3, 0), (3, 1)))):

        @pl.when(dp == core)
        def _(order=order):
            for k, s in order:
                project_out(k, s, (k, s) == order[-1])

    for s in range(samples):
        for k in (1, 2, 3):
            attn_copy(k, s, peer[k]).wait_send()
    for p in range(2):
        relay(1, p).wait_send()
    for k in (1, 2, 3):
        wo_last(k, pair_q).wait_send()
    wo_pair(3, None, mine_q).wait_send()
    wo_core(3, None, mine_q).wait_send()
    edges_sent(1)


def local(
    n_sp,
    n_tp,
    latent,
    context,
    condition,
    ctx_condition,
    norm_gain,
    w_shift,
    w_scale,
    w_gate,
    w_query,
    w_key,
    w_value,
    w_out,
    sink,
):
    rows, samples, width = latent.shape
    lc = context.shape[0]
    wid = w_shift.shape[1]
    depth = w_shift.shape[0]
    qw, kw = w_query.shape[1], w_key.shape[1]
    heads = qw // HEAD_DIM
    block = rows * n_tp
    assert n_tp == 4 and n_sp % 2 == 0 and qw % 64 == 0 and samples == 2 and kw == HEAD_DIM and rows == WINDOW and block % GRID_W == 0 and heads % 2 == 0
    quarter = HEAD_DIM // 4
    lane = np.arange(HEAD_DIM)
    freqs = 10000.0 ** (-(lane % quarter).astype(np.float32) / quarter)
    sign = np.where(lane % (2 * quarter) < quarter, -1.0, 1.0)

    def table(count):
        angle = np.arange(count, dtype=np.float32)[:, None] * freqs[None, :].astype(np.float32)
        return jnp.asarray(np.cos(angle), F32), jnp.asarray(np.sin(angle) * sign[None, :], F32)

    row_table = table(n_sp * block // GRID_W)
    col_table = table(GRID_W)
    hbm = pl.BlockSpec(memory_space=pltpu.HBM)
    vmem = pl.BlockSpec(memory_space=pltpu.VMEM)
    smem = pl.BlockSpec(memory_space=pltpu.SMEM)
    dma = pltpu.SemaphoreType.DMA
    mixed = pl.pallas_call(
        functools.partial(kernel, n_sp),
        out_shape=pltpu.VMEM((rows, samples, width), BF16),
        in_specs=[hbm, hbm, vmem, vmem, vmem, hbm, hbm, hbm, hbm, hbm, hbm, hbm, smem, vmem, vmem, vmem, vmem],
        out_specs=vmem,
        scratch_shapes=[
            pltpu.VMEM((rows, samples, width), BF16),
            pltpu.VMEM((n_tp, samples, rows, width), BF16),
            pltpu.VMEM((lc, samples, width), BF16),
            pltpu.VMEM((3, depth, wid), BF16),
            pltpu.VMEM((width, qw + 2 * kw), BF16),
            pltpu.VMEM((n_tp, qw, width), BF16),
            pltpu.VMEM((8, depth), F32),
            pltpu.VMEM((n_sp, 4, 3 * wid), F32),
            pltpu.VMEM((n_tp, 4, 3 * wid), F32),
            pltpu.VMEM((4, width), F32),
            pltpu.VMEM((4, width), F32),
            pltpu.VMEM((4, width), F32),
            pltpu.VMEM((samples * max(rows, lc), width), BF16),
            pltpu.VMEM((samples, n_tp, heads * rows, HEAD_DIM), BF16),
            pltpu.VMEM((samples, block + 2 * WINDOW, 2 * kw), BF16),
            pltpu.VMEM((samples, lc * n_sp, 2 * kw), BF16),
            pltpu.VMEM((2 * n_tp, samples, rows, qw), BF16),
            pltpu.VMEM((samples * rows, width), F32),
            pltpu.VMEM((block, HEAD_DIM), F32),
            pltpu.VMEM((block, HEAD_DIM), F32),
            dma((9,)),
            dma((n_sp - 1,)),
            dma((n_sp - 1,)),
            dma((n_tp - 1,)),
            dma((n_tp - 1,)),
            dma((2, samples, 2)),
            dma((2, samples, 2)),
            dma((samples, 2)),
            dma((samples, 2)),
            dma((n_sp - 1,)),
            dma((n_sp - 1,)),
            dma((2, samples)),
            dma((2, samples)),
            dma((n_tp - 1, samples)),
            dma((n_tp - 1, samples)),
            dma((2, 2)),
            dma((2, 2)),
            dma((2,)),
            dma((2,)),
            dma((n_tp - 1,)),
            dma((n_tp - 1,)),
            dma((n_tp - 1,)),
            dma((n_tp - 1,)),
            dma((n_tp - 1,)),
            dma((n_tp - 1,)),
        ],
        compiler_params=pltpu.CompilerParams(
            collective_id=0, has_side_effects=True, vmem_limit_bytes=60 * 1024 * 1024
        ),
        name="step",
    )(
        latent,
        context,
        condition,
        ctx_condition,
        norm_gain[None],
        w_shift,
        w_scale,
        w_gate,
        w_query,
        w_key,
        w_value,
        w_out,
        sink[None],
        *row_table,
        *col_table,
    )
    return mixed


def solution(mesh):
    return jax.shard_map(
        functools.partial(local, mesh.shape["sp"], mesh.shape["tp"]),
        mesh=mesh,
        in_specs=(
            P(("sp", "tp"), "dp", None),
            P("sp", "dp", None),
            P("dp", "sp"),
            P("sp"),
            P(),
            P("sp", "tp"),
            P("sp", "tp"),
            P("sp", "tp"),
            P(None, "tp"),
            P(None, "tp"),
            P(None, "tp"),
            P("tp", None),
            P("tp"),
        ),
        out_specs=P(("sp", "tp"), "dp", None),
        check_vma=False,
    )
```

```python
import functools
import math

import jax
import jax.numpy as jnp
import numpy as np
from jax import lax
from jax.experimental import pallas as pl
from jax.experimental.pallas import tpu as pltpu
from jax.sharding import PartitionSpec as P

HEAD_DIM = 128
WINDOW = 128
GRID_W = 64
EPSILON = 1e-06
NEGATIVE = -1e30
MESH = pl.DeviceIdType.MESH
F32 = jnp.float32
BF16 = jnp.bfloat16
LOG2E = math.log2(math.e)
CHUNK = 16
OUT_PIECES = 1


def kernel(
    n_sp,
    lat_hbm,
    ctx_hbm,
    cond_ref,
    cctx_ref,
    gain_ref,
    wsh_hbm,
    wsc_hbm,
    wga_hbm,
    wq_hbm,
    wk_hbm,
    wv_hbm,
    wo_hbm,
    sink_ref,
    row_cos,
    row_sin,
    col_cos,
    col_sin,
    mixed,
    lat_raw,
    lat_all,
    ctx_v,
    wmod,
    wqkv,
    wo_all,
    act_s,
    mod_p,
    mod_all,
    mod_a,
    mod_b,
    mod_g,
    hbuf,
    qbuf,
    kvbuf,
    ckv,
    attn,
    acc,
    cos_ref,
    sin_ref,
    loc_sem,
    modp_s,
    modp_r,
    moda_s,
    moda_r,
    lat_s,
    lat_r,
    relay_s,
    relay_r,
    ctx_s,
    ctx_r,
    halo_s,
    halo_r,
    attn_s,
    attn_r,
    wo_s,
    wo_r,
    wod_s,
    wod_r,
    woz_s,
    woz_r,
    woc_s,
    woc_r,
    woe_s,
    woe_r,
):
    rows, samples, width = lat_hbm.shape
    n_tp = mod_all.shape[0]
    wid = wmod.shape[2]
    qw = wq_hbm.shape[1]
    kw = wk_hbm.shape[1]
    heads = qw // HEAD_DIM
    lc = ctx_hbm.shape[0]
    block = rows * n_tp
    sp = lax.axis_index("sp")
    tp = lax.axis_index("tp")
    dp = lax.axis_index("dp")
    tx, ty = tp % 2, tp // 2
    peer = {1: 2 * ty + 1 - tx, 2: 2 * (1 - ty) + tx, 3: 3 - tp}

    def sp_peer(o):
        return lax.rem(sp + o, n_sp)

    loads = [
        pltpu.make_async_copy(wsh_hbm, wmod.at[0], loc_sem.at[0]),
        pltpu.make_async_copy(wsc_hbm, wmod.at[1], loc_sem.at[1]),
        pltpu.make_async_copy(wga_hbm, wmod.at[2], loc_sem.at[2]),
        pltpu.make_async_copy(ctx_hbm, ctx_v, loc_sem.at[3]),
        pltpu.make_async_copy(wk_hbm, wqkv.at[:, pl.ds(qw, kw)], loc_sem.at[4]),
        pltpu.make_async_copy(wv_hbm, wqkv.at[:, pl.ds(qw + kw, kw)], loc_sem.at[5]),
        pltpu.make_async_copy(lat_hbm, lat_raw, loc_sem.at[6]),
        pltpu.make_async_copy(wq_hbm, wqkv.at[:, pl.ds(0, qw)], loc_sem.at[7]),
        pltpu.make_async_copy(wo_hbm, wo_all.at[0], loc_sem.at[8]),
    ]
    for i in (8, 0, 1, 2, 6, 3, 4, 5, 7):
        loads[i].start()

    barrier = pltpu.get_barrier_semaphore()
    for o in range(1, n_sp):
        pl.semaphore_signal(barrier, inc=1, device_id={"sp": sp_peer(o)}, device_id_type=MESH)
    for k in (1, 2, 3):
        pl.semaphore_signal(barrier, inc=1, device_id={"tp": peer[k]}, device_id_type=MESH)

    pl.semaphore_signal(barrier, inc=1, device_id={"dp": 1 - dp}, device_id_type=MESH)

    def apart(src, at):
        return jnp.swapaxes(src[pl.ds(at, CHUNK)], 0, 1)

    pl.semaphore_wait(barrier, n_sp - 1 + n_tp)

    def remote(src, dst, ssem, rsem, dev):
        return pltpu.make_async_remote_copy(
            src_ref=src, dst_ref=dst, send_sem=ssem, recv_sem=rsem, device_id=dev, device_id_type=MESH
        )

    half = rows // 2

    def direct(k, s, p):
        part = pl.ds(p * half, half)
        return remote(
            lat_all.at[0, s, part], lat_all.at[k, s, part], lat_s.at[k - 1], lat_r.at[k - 1, s, p], {"tp": peer[k]}
        )

    def relay(s, p):
        part = pl.ds(p * half, half)
        return remote(
            lat_all.at[1 + p, s, part], lat_all.at[3, s, part], relay_s.at[s, p], relay_r.at[s, p], {"tp": peer[2 - p]}
        )

    zh = sp % 2
    quarter = qw // 4
    mine_q = 2 * zh + dp
    pair_q = 2 * (1 - zh) + dp

    def wo_rows(index, count=quarter, skip=0):
        return pl.ds(pl.multiple_of(index * quarter + skip, count), count)

    def wo_half(index, p):
        return wo_rows(index, quarter // 2, p * (quarter // 2))

    def wo_direct(k, p):
        part = wo_half(mine_q, p)
        return remote(wo_all.at[0, part], wo_all.at[k, part], wo_s.at[k - 1], wo_r.at[k - 1, p], {"tp": peer[k]})

    def wo_relay(p):
        part = wo_half(mine_q, p)
        return remote(
            wo_all.at[1 + p, part], wo_all.at[3, part], wod_s.at[p], wod_r.at[p], {"tp": peer[2 - p]}
        )

    def wo_pair(k, p, index):
        part = wo_all.at[k, wo_rows(index) if p is None else wo_half(index, p)]
        return remote(part, part, woz_s.at[k - 1], woz_r.at[k - 1], {"sp": sp + 1 - 2 * zh})

    def wo_core(k, p, index):
        part = wo_all.at[k, wo_rows(index) if p is None else wo_half(index, p)]
        return remote(part, part, woc_s.at[k - 1], woc_r.at[k - 1], {"dp": 1 - dp})

    def wo_share(k, p):
        wo_pair(k, p, mine_q).start()
        wo_core(k, p, mine_q).start()

    def wo_last(k, index):
        part = wo_all.at[k, wo_rows(index)]
        return remote(part, part, woe_s.at[k - 1], woe_r.at[k - 1], {"dp": 1 - dp})

    loads[8].wait()
    wo_direct(1, 0).start()
    wo_direct(2, 1).start()

    act_s[...] = jnp.zeros_like(act_s)
    cv = cond_ref[...].astype(F32)
    act_s[0:samples, :] = cv / (1.0 + jnp.exp(-cv))
    cc = cctx_ref[...].astype(F32).reshape(1, -1)
    act_s[samples : samples + 1, :] = cc / (1.0 + jnp.exp(-cc))
    both = act_s[...].astype(BF16)
    for m in range(3):
        loads[m].wait()
        mod_p[0, :, m * wid : (m + 1) * wid] = jnp.dot(both, wmod[m], preferred_element_type=F32)[0:4]
    mod_copies = [
        remote(mod_p.at[0], mod_p.at[o], modp_s.at[o - 1], modp_r.at[o - 1], {"sp": sp_peer(o)})
        for o in range(1, n_sp)
    ]
    for copy in mod_copies:
        copy.start()

    loads[6].wait()

    @pl.loop(0, rows // CHUNK)
    def _(c):
        at = pl.multiple_of(c * CHUNK, CHUNK)
        both = apart(lat_raw, at)
        for s in range(samples):
            lat_all[0, s, pl.ds(at, CHUNK), :] = both[s]

    grid_rows = block // GRID_W
    for by_row, by_col, table in ((row_cos, col_cos, cos_ref), (row_sin, col_sin, sin_ref)):
        left = lax.broadcasted_iota(jnp.int32, (GRID_W, HEAD_DIM), 1) < HEAD_DIM // 2
        for r in range(grid_rows):
            table[r * GRID_W : (r + 1) * GRID_W, :] = jnp.where(
                left, by_row[pl.ds(sp * grid_rows + r, 1), :], by_col[...]
            )

    for copy in mod_copies:
        copy.wait_recv()
    total = mod_p[0]
    for o in range(1, n_sp):
        total = total + mod_p[o]
    mod_all[tp] = total
    all_copies = [
        remote(mod_all.at[tp], mod_all.at[tp], moda_s.at[k - 1], moda_r.at[k - 1], {"tp": peer[k]})
        for k in (1, 2, 3)
    ]
    for copy in all_copies:
        copy.start()
    wo_direct(1, 1).start()
    wo_direct(2, 0).start()
    direct(1, 0, 0).start()
    direct(2, 0, 1).start()
    direct(1, 0, 1).start()
    direct(2, 0, 0).start()
    wo_direct(1, 0).wait_recv()
    wo_direct(2, 1).wait_recv()
    wo_share(1, 0)
    wo_share(2, 1)
    for k in (1, 2, 3):
        remote(
            mod_all.at[peer[k]], mod_all.at[peer[k]], moda_s.at[k - 1], moda_r.at[k - 1], {"tp": peer[k]}
        ).wait_recv()
    for t in range(n_tp):
        cols = slice(t * wid, (t + 1) * wid)
        mod_b[:, cols] = mod_all[t, :, 0:wid]
        mod_a[:, cols] = (1.0 + mod_all[t, :, wid : 2 * wid]) * gain_ref[:, cols]
        mod_g[:, cols] = mod_all[t, :, 2 * wid : 3 * wid]

    def modulate(values, mod_row):
        x = values.astype(F32)
        inv = lax.rsqrt(jnp.mean(x * x, axis=-1, keepdims=True) + EPSILON)
        row = pl.ds(mod_row, 1)
        return (x * inv * mod_a[row, :] + mod_b[row, :]).astype(BF16)

    def norm_rows(src, mod_row, base, count):
        @pl.loop(0, count // CHUNK, unroll=4)
        def _(c):
            at = pl.multiple_of(c * CHUNK, CHUNK)
            hbuf[pl.ds(base + at, CHUNK), :] = modulate(src[pl.ds(at, CHUNK), :], mod_row)

    for i in (3, 4, 5):
        loads[i].wait()
    ctx_at = pl.multiple_of(sp * lc, lc)

    @pl.loop(0, lc // CHUNK, unroll=2)
    def _(c):
        at = pl.multiple_of(c * CHUNK, CHUNK)
        both = apart(ctx_v, at)
        for s in range(samples):
            hbuf[pl.ds(s * lc + at, CHUNK), :] = modulate(both[s], samples)

    made = jnp.dot(hbuf[...], wqkv[:, qw : qw + 2 * kw], preferred_element_type=F32).astype(BF16)
    for s in range(samples):
        ckv[s, pl.ds(ctx_at, lc), :] = made[s * lc : (s + 1) * lc]

    mine = ckv.at[:, pl.ds(ctx_at, lc), :]
    ctx_copies = [
        remote(mine, mine, ctx_s.at[o - 1], ctx_r.at[o - 1], {"sp": sp_peer(o)}) for o in range(1, n_sp)
    ]
    for copy in ctx_copies:
        copy.start()

    wo_direct(1, 1).wait_recv()
    wo_direct(2, 0).wait_recv()
    direct(1, 0, 0).wait_recv()
    direct(2, 0, 1).wait_recv()
    for p in range(2):
        relay(0, p).start()
    for p in range(2):
        wo_relay(p).start()
    direct(1, 1, 0).start()
    direct(2, 1, 1).start()
    direct(1, 1, 1).start()
    direct(2, 1, 0).start()

    loads[7].wait()
    lane = lax.broadcasted_iota(jnp.int32, (rows, HEAD_DIM), 1)
    low = lane % (HEAD_DIM // 2) < HEAD_DIM // 4

    def turn(u, cos, sin):
        other = jnp.where(
            low, pltpu.roll(u, HEAD_DIM - HEAD_DIM // 4, 1), pltpu.roll(u, HEAD_DIM // 4, 1)
        )
        return u * cos + other * sin

    def halo_up(s):
        return remote(
            kvbuf.at[s, pl.ds(block, WINDOW), :],
            kvbuf.at[s, pl.ds(0, WINDOW), :],
            halo_s.at[0, s],
            halo_r.at[0, s],
            {"sp": lax.min(sp + 1, n_sp - 1)},
        )

    def halo_down(s):
        return remote(
            kvbuf.at[s, pl.ds(WINDOW, WINDOW), :],
            kvbuf.at[s, pl.ds(WINDOW + block, WINDOW), :],
            halo_s.at[1, s],
            halo_r.at[1, s],
            {"sp": lax.max(sp - 1, 0)},
        )

    not_first, not_last = sp > 0, sp < n_sp - 1

    @pl.when(sp == 0)
    def _():
        kvbuf[:, 0:WINDOW, :] = jnp.zeros((samples, WINDOW, 2 * kw), BF16)

    @pl.when(sp == n_sp - 1)
    def _():
        kvbuf[:, WINDOW + block :, :] = jnp.zeros((samples, WINDOW, 2 * kw), BF16)

    def attn_copy(k, s, dest):
        return remote(attn.at[n_tp + k, s], attn.at[k, s], attn_s.at[k - 1], attn_r.at[k - 1, s], {"tp": dest})

    def project(blocks):
        spots = []
        for e, (k, s) in enumerate(blocks):
            norm_rows(lat_all.at[k, s], s, e * rows, rows)
            kx, ky = k % 2, k // 2
            b = 2 * (ty + ky - 2 * ty * ky) + tx + kx - 2 * tx * kx
            at = pl.multiple_of(b * rows, rows)
            spots.append((s, b, at, cos_ref[pl.ds(at, rows), :], sin_ref[pl.ds(at, rows), :]))
        for c in range(heads // 2 + 1):
            prod = jnp.dot(
                hbuf[0 : len(blocks) * rows, :],
                wqkv[:, c * 2 * HEAD_DIM : (c + 1) * 2 * HEAD_DIM],
                preferred_element_type=F32,
            )
            for e, (s, b, at, cos, sin) in enumerate(spots):
                part = prod[e * rows : (e + 1) * rows]
                first = turn(part[:, :HEAD_DIM], cos, sin).astype(BF16)
                if c < heads // 2:
                    second = turn(part[:, HEAD_DIM:], cos, sin).astype(BF16)
                    qbuf[s, b, 2 * c * rows : (2 * c + 1) * rows, :] = first
                    qbuf[s, b, (2 * c + 1) * rows : (2 * c + 2) * rows, :] = second
                else:
                    kvbuf[s, pl.ds(WINDOW + at, rows), 0:HEAD_DIM] = first
                    kvbuf[s, pl.ds(WINDOW + at, rows), HEAD_DIM:] = part[:, HEAD_DIM:].astype(BF16)

    def send_edges(s, bottom, top):
        @pl.when(not_last & top)
        def _():
            halo_up(s).start()

        @pl.when(not_first & bottom)
        def _():
            halo_down(s).start()

    at_first, at_last = tp == 0, tp == n_tp - 1
    inner = (tp > 0) & (tp < n_tp - 1)
    project([(0, s) for s in range(samples)])
    for s in range(samples):
        send_edges(s, at_first, at_last)

    scale = HEAD_DIM ** (-0.5) * LOG2E
    seq = block * n_sp
    nums = (((1,), (1,)), ((), ()))

    span = 3 * WINDOW
    pair = 2 * rows
    row_id = lax.broadcasted_iota(jnp.int32, (pair, 1), 0)

    def hand_over(k):
        wo_pair(k, None, pair_q).wait_recv()
        wo_last(k, pair_q).start()

    def out_cols(n):
        span = width // OUT_PIECES
        return pl.ds(pl.multiple_of(n * span, span), span)

    def project_own(s):
        held = pl.ds(s * rows, rows)

        @pl.loop(0, OUT_PIECES)
        def _(n):
            cols = out_cols(n)
            part = jnp.dot(attn[0, s], wo_all[0, :, cols], preferred_element_type=F32)
            acc[held, cols] = part.astype(BF16).astype(F32)

    def edges_sent(s):
        @pl.when(not_last)
        def _():
            halo_up(s).wait_send()

        @pl.when(not_first)
        def _():
            halo_down(s).wait_send()

    def early_sent():
        for copy in mod_copies + all_copies + ctx_copies:
            copy.wait_send()
        for p in range(2):
            relay(0, p).wait_send()
            wo_relay(p).wait_send()
        for k in (1, 2):
            remote(
                lat_all.at[0], lat_all.at[k], lat_s.at[k - 1], lat_r.at[k - 1, 0, 0], {"tp": peer[k]}
            ).wait_send()
            part = wo_rows(mine_q)
            remote(
                wo_all.at[0, part], wo_all.at[k, part], wo_s.at[k - 1], wo_r.at[k - 1, 0], {"tp": peer[k]}
            ).wait_send()
            wo_pair(k, None, mine_q).wait_send()
            wo_core(k, None, mine_q).wait_send()
        edges_sent(0)

    def attend(i, s):
        k = jnp.where(i == 0, 1, jnp.where(i < n_tp - 1, n_tp - i, 0))
        kx, ky = k % 2, k // 2
        b = 2 * (ty + ky - 2 * ty * ky) + tx + kx - 2 * tx * kx
        at = pl.multiple_of(b * rows, rows)
        slot = jnp.where(k == 0, 0, n_tp + k)

        @pl.when((b == 0) & not_first)
        def _():
            halo_up(s).wait_recv()

        @pl.when((b == n_tp - 1) & not_last)
        def _():
            halo_down(s).wait_recv()

        kc = ckv[s, :, 0:HEAD_DIM]
        vc = ckv[s, :, HEAD_DIM:]
        kl = kvbuf[s, pl.ds(at, span), 0:HEAD_DIM]
        vl = kvbuf[s, pl.ds(at, span), HEAD_DIM:]
        key = lax.broadcasted_iota(jnp.int32, (pair, span), 1)
        query = lax.broadcasted_iota(jnp.int32, (pair, span), 0) % rows
        pos = key + (sp * block + b * rows - WINDOW)
        allowed = (key >= query) & (key <= query + 2 * WINDOW) & (pos >= 0) & (pos < seq)
        for c in range(heads // 2):
            q = qbuf[s, b, c * pair : (c + 1) * pair, :]
            sc = lax.dot_general(q, kc, nums, preferred_element_type=F32)
            sl = lax.dot_general(q, kl, nums, preferred_element_type=F32)
            sl = jnp.where(allowed, sl, NEGATIVE)
            sink2 = jnp.where(row_id < rows, sink_ref[0, 2 * c], sink_ref[0, 2 * c + 1]) * LOG2E
            top = jnp.maximum(
                jnp.max(sc, axis=-1, keepdims=True), jnp.max(sl, axis=-1, keepdims=True)
            )
            top = jnp.maximum(top * scale, sink2)
            ec = jnp.exp2(sc * scale - top)
            el = jnp.exp2(sl * scale - top)
            total = (
                jnp.sum(ec, axis=-1, keepdims=True)
                + jnp.sum(el, axis=-1, keepdims=True)
                + jnp.exp2(sink2 - top)
            )
            o = jnp.dot(ec.astype(BF16), vc, preferred_element_type=F32)
            o = o + jnp.dot(el.astype(BF16), vl, preferred_element_type=F32)
            o = (o / total).astype(BF16)
            attn[slot, s, :, 2 * c * HEAD_DIM : (2 * c + 1) * HEAD_DIM] = o[:rows]
            attn[slot, s, :, (2 * c + 1) * HEAD_DIM : (2 * c + 2) * HEAD_DIM] = o[rows:]

        @pl.when((s == 1) & (k > 0))
        def _():
            attn_copy(k, s, b).start()

    @pl.loop(0, samples)
    def _(s):
        direct(1, s, 1).wait_recv()
        direct(2, s, 0).wait_recv()
        project([(1, s), (2, s)])
        send_edges(s, inner, inner)

        @pl.when((s == 1) & inner & (dp == 0))
        def _():
            wo_relay(1).wait_recv()
            wo_share(3, 1)

        @pl.loop(0, n_tp)
        def _(i):
            @pl.when(i == s)
            def _():
                @pl.when(s == 1)
                def _():
                    project_own(0)
                    early_sent()

                relay(s, 0).wait_recv()
                relay(s, 1).wait_recv()
                project([(3, s)])
                send_edges(s, at_last, at_first)

                @pl.when(s == 0)
                def _():
                    wo_share(1, 1)
                    wo_share(2, 0)
                    for o in range(1, n_sp):
                        got = ckv.at[:, pl.ds(pl.multiple_of(sp_peer(n_sp - o) * lc, lc), lc), :]
                        remote(got, got, ctx_s.at[o - 1], ctx_r.at[o - 1], {"sp": sp_peer(o)}).wait_recv()
                    wo_relay(0).wait_recv()
                    wo_share(3, 0)

                @pl.when(s == 1)
                def _():
                    @pl.when(at_first | at_last | (dp == 1))
                    def _():
                        wo_relay(1).wait_recv()
                        wo_share(3, 1)

                    hand_over(1)
                    hand_over(2)

            @pl.when((s == 1) & (i == n_tp - 1) & (dp == 1))
            def _():
                hand_over(3)

            attend(i, s)

        @pl.when(s == 0)
        def _():
            direct(1, 1, 0).wait_recv()
            direct(2, 1, 1).wait_recv()
            for p in range(2):
                relay(1, p).start()
            for k in (3, 2, 1):
                attn_copy(k, 0, peer[k]).start()

    def arrived(k, s):
        if k > 0:
            if s == 0:
                wo_core(k, None, mine_q + 1 - 2 * dp).wait_recv()
                wo_last(k, pair_q + 1 - 2 * dp).wait_recv()
            attn_copy(k, s, peer[k]).wait_recv()

    def project_out(k, s, last):
        arrived(k, s)

        @pl.loop(0, OUT_PIECES)
        def _(n):
            cols = out_cols(n)
            part = jnp.dot(attn[k, s], wo_all[k, :, cols], preferred_element_type=F32)
            held = pl.ds(s * rows, rows)
            total = acc[held, cols] + part.astype(BF16).astype(F32)
            if not last:
                acc[held, cols] = total
            else:
                both = []
                for t in range(samples):
                    branch = total if t == s else acc[t * rows : (t + 1) * rows, cols]
                    both.append(
                        (lat_all[0, t, :, cols].astype(F32) + mod_g[t : t + 1, cols] * branch).astype(BF16)
                    )
                mixed[:, :, cols] = jnp.swapaxes(jnp.stack(both), 0, 1)

    @pl.when(dp == 0)
    def _():
        hand_over(3)

    project_own(1)
    project_out(1, 0, False)
    project_out(2, 0, False)
    for core, order in enumerate((((3, 0), (3, 1), (1, 1), (2, 1)), ((1, 1), (2, 1), (3, 0), (3, 1)))):

        @pl.when(dp == core)
        def _(order=order):
            for k, s in order:
                project_out(k, s, (k, s) == order[-1])

    for k in (1, 2, 3):
        remote(
            attn.at[n_tp + k], attn.at[k], attn_s.at[k - 1], attn_r.at[k - 1, 0], {"tp": peer[k]}
        ).wait_send()
    for p in range(2):
        relay(1, p).wait_send()
    for k in (1, 2, 3):
        wo_last(k, pair_q).wait_send()
    wo_pair(3, None, mine_q).wait_send()
    wo_core(3, None, mine_q).wait_send()
    edges_sent(1)


def local(
    n_sp,
    n_tp,
    latent,
    context,
    condition,
    ctx_condition,
    norm_gain,
    w_shift,
    w_scale,
    w_gate,
    w_query,
    w_key,
    w_value,
    w_out,
    sink,
):
    rows, samples, width = latent.shape
    lc = context.shape[0]
    wid = w_shift.shape[1]
    depth = w_shift.shape[0]
    qw, kw = w_query.shape[1], w_key.shape[1]
    heads = qw // HEAD_DIM
    block = rows * n_tp
    assert n_tp == 4 and n_sp % 2 == 0 and qw % 64 == 0 and samples == 2 and kw == HEAD_DIM and rows == WINDOW and block % GRID_W == 0 and heads % 2 == 0
    quarter = HEAD_DIM // 4
    lane = np.arange(HEAD_DIM)
    freqs = 10000.0 ** (-(lane % quarter).astype(np.float32) / quarter)
    sign = np.where(lane % (2 * quarter) < quarter, -1.0, 1.0)

    def table(count):
        angle = np.arange(count, dtype=np.float32)[:, None] * freqs[None, :].astype(np.float32)
        return jnp.asarray(np.cos(angle), F32), jnp.asarray(np.sin(angle) * sign[None, :], F32)

    row_table = table(n_sp * block // GRID_W)
    col_table = table(GRID_W)
    hbm = pl.BlockSpec(memory_space=pltpu.HBM)
    vmem = pl.BlockSpec(memory_space=pltpu.VMEM)
    smem = pl.BlockSpec(memory_space=pltpu.SMEM)
    dma = pltpu.SemaphoreType.DMA
    mixed = pl.pallas_call(
        functools.partial(kernel, n_sp),
        out_shape=pltpu.VMEM((rows, samples, width), BF16),
        in_specs=[hbm, hbm, vmem, vmem, vmem, hbm, hbm, hbm, hbm, hbm, hbm, hbm, smem, vmem, vmem, vmem, vmem],
        out_specs=vmem,
        scratch_shapes=[
            pltpu.VMEM((rows, samples, width), BF16),
            pltpu.VMEM((n_tp, samples, rows, width), BF16),
            pltpu.VMEM((lc, samples, width), BF16),
            pltpu.VMEM((3, depth, wid), BF16),
            pltpu.VMEM((width, qw + 2 * kw), BF16),
            pltpu.VMEM((n_tp, qw, width), BF16),
            pltpu.VMEM((8, depth), F32),
            pltpu.VMEM((n_sp, 4, 3 * wid), F32),
            pltpu.VMEM((n_tp, 4, 3 * wid), F32),
            pltpu.VMEM((4, width), F32),
            pltpu.VMEM((4, width), F32),
            pltpu.VMEM((4, width), F32),
            pltpu.VMEM((samples * max(rows, lc), width), BF16),
            pltpu.VMEM((samples, n_tp, heads * rows, HEAD_DIM), BF16),
            pltpu.VMEM((samples, block + 2 * WINDOW, 2 * kw), BF16),
            pltpu.VMEM((samples, lc * n_sp, 2 * kw), BF16),
            pltpu.VMEM((2 * n_tp, samples, rows, qw), BF16),
            pltpu.VMEM((samples * rows, width), F32),
            pltpu.VMEM((block, HEAD_DIM), F32),
            pltpu.VMEM((block, HEAD_DIM), F32),
            dma((9,)),
            dma((n_sp - 1,)),
            dma((n_sp - 1,)),
            dma((n_tp - 1,)),
            dma((n_tp - 1,)),
            dma((2,)),
            dma((2, samples, 2)),
            dma((samples, 2)),
            dma((samples, 2)),
            dma((n_sp - 1,)),
            dma((n_sp - 1,)),
            dma((2, samples)),
            dma((2, samples)),
            dma((n_tp - 1,)),
            dma((n_tp - 1, samples)),
            dma((2,)),
            dma((2, 2)),
            dma((2,)),
            dma((2,)),
            dma((n_tp - 1,)),
            dma((n_tp - 1,)),
            dma((n_tp - 1,)),
            dma((n_tp - 1,)),
            dma((n_tp - 1,)),
            dma((n_tp - 1,)),
        ],
        compiler_params=pltpu.CompilerParams(
            collective_id=0, has_side_effects=True, vmem_limit_bytes=60 * 1024 * 1024
        ),
        name="step",
    )(
        latent,
        context,
        condition,
        ctx_condition,
        norm_gain[None],
        w_shift,
        w_scale,
        w_gate,
        w_query,
        w_key,
        w_value,
        w_out,
        sink[None],
        *row_table,
        *col_table,
    )
    return mixed


def solution(mesh):
    return jax.shard_map(
        functools.partial(local, mesh.shape["sp"], mesh.shape["tp"]),
        mesh=mesh,
        in_specs=(
            P(("sp", "tp"), "dp", None),
            P("sp", "dp", None),
            P("dp", "sp"),
            P("sp"),
            P(),
            P("sp", "tp"),
            P("sp", "tp"),
            P("sp", "tp"),
            P(None, "tp"),
            P(None, "tp"),
            P(None, "tp"),
            P("tp", None),
            P("tp"),
        ),
        out_specs=P(("sp", "tp"), "dp", None),
        check_vma=False,
    )
```
